512 devices in a mesh: sp: 64 (over z, y), dp: 8 (over x, core).
Axes of the slice: x: 4, y: 8, z: 8, core: 2. Of those that a mesh axis runs over, the one named last changes fastest.
Arguments:
- gated: bfloat16 [8, 8192, 3072], P('dp', 'sp'), may hold values from -6 to 6
- values_in: bfloat16 [8, 8192, 3072], P('dp', 'sp'), may hold values from -6 to 6
- upstream: bfloat16 [8, 8192, 3072], P('dp', 'sp'), may hold values from -6 to 6
- gain: float32 [3072], replicated, may hold values from 0.1 to 1.9
- shift: float32 [3072], replicated, may hold values from -3 to 3
- mix_w: bfloat16 [512, 4, 512], P('dp'), may hold values from -0.375 to 0.375
- mix_bias: float32 [4, 512], replicated, may hold values from 0.1 to 1.9
Outputs:
- grad_u: bfloat16 [8, 8192, 3072], P('dp', 'sp')
- grad_v: bfloat16 [8, 8192, 3072], P('dp', 'sp')
- grad_mix: float32 [512, 4, 512], P('dp')
- grad_bias: float32 [4, 512], replicated
- grad_gain: float32 [3072], replicated
- grad_shift: float32 [3072], replicated
The draws below stay inside these ranges and needn't reach their ends.
All inputs are finite; a program needn't handle non-finite values.
Results may differ from the reference program's by a relative error of at most 0.014.
Values may be sent and summed in bfloat16 or wider, within the bound.
No kernel may reach another device: no remote copies, remote signals or barrier semaphores. Data moves between devices by JAX's collectives and lax.ppermute only.
A program may use at most 64 MiB of HBM per device.

```python
import jax
import jax.numpy as jnp
from jax import lax

GROUPS = 4
GROUP_DIM = 768
SPAN = 512
SEG = 64
HALF = 3072
LENGTH = 8192
BATCH = 8


def level_of(own_key, extent, shards, smallest, top_value):
    def one(dim, parts):
        steps = jax.random.uniform(jax.random.fold_in(jax.random.fold_in(own_key, 6), dim), (parts,), jnp.float32, smallest / len(shards), top_value / len(shards))
        return jnp.repeat(jnp.exp(steps), extent[dim] // parts).reshape((-1,) + (1,) * (len(extent) - dim - 1))

    loudness = one(*shards[0])
    for cut in shards[1:]:
        loudness = loudness * one(*cut)
    return loudness


def noise(rng, dims, deviation, most, split=(), kind=jnp.bfloat16):
    loudness = level_of(rng, dims, split, -0.22, 0.18) if split else 1.0
    drawn = jax.random.normal(rng, dims, jnp.float32) * deviation * loudness
    return jnp.minimum(jnp.maximum(drawn, -most), most).astype(kind)


def setup_inputs(seed: int = 0) -> dict:
    streams_of = jax.random.split(jax.random.key(seed), 8)
    gated = noise(streams_of[0], (BATCH, LENGTH, HALF), 1.0, 6.0, ((0, 8), (1, 64)))
    values_in = noise(streams_of[1], (BATCH, LENGTH, HALF), 1.0, 6.0, ((0, 8), (1, 64)))
    upstream = noise(streams_of[2], (BATCH, LENGTH, HALF), 1.0, 6.0, ((0, 8), (1, 64)))
    gain = jnp.clip(1.0 + 0.18 * jax.random.normal(streams_of[3], (HALF,), jnp.float32), 0.1, 1.9)
    shift = noise(streams_of[4], (HALF,), 0.5, 3.0, (), jnp.float32)
    mix_w = noise(streams_of[5], (SPAN, GROUPS, SPAN), (SPAN // 2) ** -0.5, 0.375, ((0, 8),))
    mix_bias = jnp.clip(1.0 + 0.18 * jax.random.normal(streams_of[6], (GROUPS, SPAN), jnp.float32), 0.1, 1.9)
    return {"gated": gated, "values_in": values_in, "upstream": upstream, "gain": gain, "shift": shift, "mix_w": mix_w, "mix_bias": mix_bias}


EPS = 1e-05

def span_mask():
    places = jnp.arange(SPAN)
    return (places[:, None] // SEG >= places[None, :] // SEG).astype(jnp.float32)

def reference(gated, values_in, upstream, gain, shift, mix_w, mix_bias):
    allowed = span_mask()
    masked_w = mix_w.astype(jnp.float32) * allowed[:, None, :]
    blocks = LENGTH // SPAN

    def one_sequence(carry, inputs):
        gated_row, values_row, upstream_row = inputs
        raw_values = values_row.astype(jnp.float32)
        centred = raw_values - lax.optimization_barrier(jnp.mean(raw_values, axis=-1, keepdims=True))
        inv_std = lax.rsqrt(lax.optimization_barrier(jnp.mean(centred * centred, axis=-1, keepdims=True)) + EPS)
        unit_v = centred * inv_std
        normed = (unit_v * gain + shift).astype(jnp.bfloat16)
        mix_grad = (upstream_row.astype(jnp.float32) * gated_row.astype(jnp.float32)).astype(jnp.bfloat16)
        norm_blocks = normed.reshape(blocks, SPAN, GROUPS, GROUP_DIM).astype(jnp.float32)
        grad_blocks = mix_grad.reshape(blocks, SPAN, GROUPS, GROUP_DIM).astype(jnp.float32)
        mixed_f = jnp.einsum('tgs,nsgc->ntgc', masked_w, norm_blocks) + mix_bias.T[None, :, :, None]
        mixed = lax.optimization_barrier(mixed_f.astype(jnp.bfloat16)).reshape(LENGTH, HALF)
        grad_u = (upstream_row.astype(jnp.float32) * mixed.astype(jnp.float32)).astype(jnp.bfloat16)
        back_f = jnp.einsum('tgs,ntgc->nsgc', masked_w, grad_blocks)
        grad_normed = lax.optimization_barrier(back_f.astype(jnp.bfloat16)).reshape(LENGTH, HALF).astype(jnp.float32)
        scaled = grad_normed * gain
        grad_v = inv_std * (scaled - lax.optimization_barrier(jnp.mean(scaled, axis=-1, keepdims=True)) - unit_v * lax.optimization_barrier(jnp.mean(scaled * unit_v, axis=-1, keepdims=True)))
        mix_term = jnp.einsum('ntgc,nsgc->tgs', grad_blocks, norm_blocks) * allowed[:, None, :]
        bias_term = lax.optimization_barrier(jnp.sum(grad_blocks, axis=(0, 3))).T
        carry = (carry[0] + mix_term, carry[1] + bias_term, carry[2] + lax.optimization_barrier(jnp.sum(grad_normed * unit_v, axis=0)), carry[3] + lax.optimization_barrier(jnp.sum(grad_normed, axis=0)))
        return (carry, (grad_u, grad_v.astype(jnp.bfloat16)))
    initial = (jnp.zeros((SPAN, GROUPS, SPAN), jnp.float32), jnp.zeros((GROUPS, SPAN), jnp.float32), jnp.zeros((HALF,), jnp.float32), jnp.zeros((HALF,), jnp.float32))
    totals, outputs = lax.scan(one_sequence, initial, (gated, values_in, upstream))
    return (outputs[0], outputs[1], totals[0], totals[1], totals[2], totals[3])
```

```python
import functools

import jax
import jax.numpy as jnp
from jax import lax
from jax.experimental import pallas as pl
from jax.experimental.pallas import tpu as pltpu
from jax.sharding import Mesh
from jax.sharding import PartitionSpec as P

SEG = 64
ROWS = 128
GROUPS = 4
WIDTH = 768
HALF = GROUPS * WIDTH
QUAD = 4
DP = ("dp_0", "dp_1")
SP = ("sp_0", "sp_1")
Y = "sp_1"
Z = "sp_0"
EPS = 1e-05

NEAR = [(0, 1), (3, 2), (4, 5), (7, 6)]
FAR = [(0, 2), (3, 1), (4, 6), (7, 5)]
SWAP = [(1, 2), (2, 1), (5, 6), (6, 5)]
OUT = [(1, 0), (2, 3), (5, 4), (6, 7)]


VMEM = pl.BlockSpec(memory_space=pltpu.VMEM)
SMEM = pl.BlockSpec(memory_space=pltpu.SMEM)
F32 = jnp.float32
BF16 = jnp.bfloat16


def call(kernel, name, out_shape, inputs, scalars=1):
    return pl.pallas_call(
        kernel,
        out_shape=out_shape,
        in_specs=[SMEM] * scalars + [VMEM] * (len(inputs) - scalars),
        out_specs=jax.tree.map(lambda _: VMEM, out_shape),
        name=name,
    )(*inputs)


def shape(dims, dtype):
    return jax.ShapeDtypeStruct(dims, dtype)


def nt(a, b):
    return lax.dot_general(a, b, (((1,), (1,)), ((), ())), preferred_element_type=F32)


def tn(a, b):
    return lax.dot_general(a, b, (((0,), (0,)), ((), ())), preferred_element_type=F32)


def nn(a, b):
    return jnp.dot(a, b, preferred_element_type=F32)


def pre_kernel(place, values, gated, upstream, gain, shift, *outs):
    us, vs, stats, bias = outs[:4], outs[4:8], outs[8], outs[9]
    low = place[0] < 2
    step = 16

    def block(i, carry):
        rows = pl.ds(pl.multiple_of(i * step, step), step)
        raw = values[0, rows, :].astype(F32)
        mean = jnp.sum(raw, axis=1, keepdims=True) * (1.0 / HALF)
        centred = raw - mean
        var = jnp.sum(centred * centred, axis=1, keepdims=True) * (1.0 / HALF)
        inv = lax.rsqrt(var + EPS)
        stats[0, rows, :] = jnp.broadcast_to(mean, (step, 128))
        stats[1, rows, :] = jnp.broadcast_to(inv, (step, 128))
        for g in range(GROUPS):
            cols = slice(g * WIDTH, (g + 1) * WIDTH)
            unit = (values[0, rows, cols].astype(F32) - mean) * inv
            normed = (unit * gain[:, cols] + shift[:, cols]).astype(BF16)
            grad = (upstream[0, rows, cols].astype(F32) * gated[0, rows, cols].astype(F32)).astype(BF16)
            us[g][rows, :] = jnp.where(low, grad, normed)
            vs[g][rows, :] = jnp.where(low, normed, grad)
        return carry

    lax.fori_loop(0, ROWS // step, block, 0)
    bias[...] = jnp.zeros_like(bias)
    ones = jnp.ones((8, WIDTH), BF16)
    for g in range(GROUPS):
        grad = jnp.where(low, us[g][...], vs[g][...])
        bias[pl.ds(g * QUAD + place[0], 1), :] = nt(ones, grad)[:1]


def weight_kernel(place, rows_in, out):
    p = place[0]
    low = p < 2
    r = lax.broadcasted_iota(jnp.int32, (ROWS, ROWS), 0) // SEG
    c = lax.broadcasted_iota(jnp.int32, (ROWS, ROWS), 1) // SEG

    def piece(t, g, s):
        top = rows_in[2 * t, g, :, pl.ds(pl.multiple_of(s * ROWS, ROWS), ROWS)]
        low_half = rows_in[2 * t + 1, g, :, pl.ds(pl.multiple_of(s * ROWS, ROWS), ROWS)]
        return jnp.concatenate([top, low_half], axis=0)

    @pl.when(low)
    def _():
        for g in range(GROUPS):
            for i in range(2):
                for j in range(3):
                    got = piece(p + j, g, jnp.maximum(p - i, 0)).astype(F32)
                    if i == 0 and j == 0:
                        got = jnp.where(r >= c, got, 0.0)
                    out[g, i * ROWS : (i + 1) * ROWS, j * ROWS : (j + 1) * ROWS] = got.T.astype(BF16)

    @pl.when(jnp.logical_not(low))
    def _():
        for g in range(GROUPS):
            for i in range(2):
                for j in range(3):
                    got = piece(jnp.minimum(p + i, 3), g, p - j)
                    if i == 0 and j == 0:
                        got = jnp.where(r >= c, got.astype(F32), 0.0).astype(BF16)
                    out[g, i * ROWS : (i + 1) * ROWS, j * ROWS : (j + 1) * ROWS] = got


def product_kernel(g, u, v, near, far, swap, weights, part, out_u, out_v):
    own, other = weights[g, :ROWS, :], weights[g, ROWS:, :]
    long_side = jnp.concatenate([u[...], swap[...], far[...]], axis=0)
    part[...] = nn(other, long_side).astype(BF16)
    out_u[...] = nn(own, long_side)
    short_side = jnp.concatenate([v[...], near[...]], axis=0)
    both = jnp.concatenate([own[:, :ROWS], other[:, :ROWS]], axis=0)
    out_v[...] = tn(both, short_side)


def mix_grad_kernel(n, place, *refs):
    ins, out = refs[: 5 * n], refs[5 * n]
    p = place[0]
    r = lax.broadcasted_iota(jnp.int32, (ROWS, ROWS), 0) // SEG
    c = lax.broadcasted_iota(jnp.int32, (ROWS, ROWS), 1) // SEG
    out[...] = jnp.zeros_like(out)

    def put(target, slot, k, got):
        got = got.astype(BF16)
        lanes = slice(k * ROWS, (k + 1) * ROWS)
        out[2 * target, slot, :, lanes] = got[:SEG]
        out[2 * target + 1, slot, :, lanes] = got[SEG:]

    for k in range(n):
        u, v, near, far, swap = ins[5 * k : 5 * k + 5]

        @pl.when(p == 0)
        def _():
            put(0, 0, k, jnp.where(r >= c, nt(u[...], v[...]), 0.0))

        @pl.when(p == 1)
        def _():
            put(1, 0, k, nt(u[...], near[...]))
            put(1, 1, k, jnp.where(r >= c, nt(u[...], v[...]), 0.0))
            put(2, 0, k, nt(swap[...], near[...]))
            put(3, 0, k, nt(far[...], near[...]))

        @pl.when(p == 2)
        def _():
            put(2, 0, k, jnp.where(r >= c, nt(v[...], u[...]), 0.0))
            put(2, 1, k, nt(v[...], swap[...]))
            put(3, 0, k, nt(near[...], u[...]))
            put(3, 1, k, nt(near[...], swap[...]))

        @pl.when(p == 3)
        def _():
            put(3, 0, k, jnp.where(r >= c, nt(v[...], u[...]), 0.0))


def deal_kernel(n, *refs):
    got, out = refs
    total = got[0].astype(F32)
    for d in range(1, 8):
        total = total + got[d].astype(F32)
    for z in range(8):
        out[z] = total[:, z * 8 : (z + 1) * 8, :].astype(BF16)


def add_kernel(got, out):
    total = got[0].astype(F32)
    for z in range(1, 8):
        total = total + got[z].astype(F32)
    out[...] = total.astype(BF16)


def place_kernel(got, out):
    def at(place, slot):
        return got[place, slot].astype(F32) + got[place + QUAD, slot].astype(F32)

    columns = (at(0, 0) + at(1, 0), at(1, 1) + at(2, 1), at(2, 0), at(3, 0))
    for s in range(4):
        for g in range(GROUPS):
            out[:, g * 512 + s * ROWS : g * 512 + (s + 1) * ROWS] = columns[s][
                :, g * ROWS : (g + 1) * ROWS
            ].astype(BF16)


def sums_kernel(place, values, stats, *refs):
    outs_u, outs_v, got, out = refs[:4], refs[4:8], refs[8:12], refs[12]
    low = place[0] < 2
    for g in range(GROUPS):
        cols = slice(g * WIDTH, (g + 1) * WIDTH)
        back = jnp.where(low, outs_u[g][...] + got[g][...].astype(F32), outs_v[g][...])
        back = back.astype(BF16).astype(F32)
        mean = stats[0, :, :1]
        inv = stats[1, :, :1]
        unit = (values[0, :, cols].astype(F32) - mean) * inv
        out[0:1, cols] = jnp.sum(back * unit, axis=0, keepdims=True)
        out[1:2, cols] = jnp.sum(back, axis=0, keepdims=True)


def post_kernel(place, values, upstream, stats, gain, bias_row, *refs):
    outs_u, outs_v, got, grad_u, grad_v = refs[:4], refs[4:8], refs[8:12], refs[12], refs[13]
    low = place[0] < 2
    step = 16

    def block(i, carry):
        rows = pl.ds(pl.multiple_of(i * step, step), step)
        mean = stats[0, rows, :1]
        inv = stats[1, rows, :1]
        first = jnp.zeros((step, 1), F32)
        second = jnp.zeros((step, 1), F32)
        for g in range(GROUPS):
            cols = slice(g * WIDTH, (g + 1) * WIDTH)
            long_side = outs_u[g][rows, :] + got[g][rows, :].astype(F32)
            short_side = outs_v[g][rows, :]
            mixed = jnp.where(low, short_side, long_side) + bias_row[rows, g : g + 1]
            mixed = mixed.astype(BF16).astype(F32)
            grad_u[0, rows, cols] = (upstream[0, rows, cols].astype(F32) * mixed).astype(BF16)
            back = jnp.where(low, long_side, short_side).astype(BF16).astype(F32)
            scaled = back * gain[:, cols]
            unit = (values[0, rows, cols].astype(F32) - mean) * inv
            first = first + jnp.sum(scaled, axis=1, keepdims=True)
            second = second + jnp.sum(scaled * unit, axis=1, keepdims=True)
        first = first * (1.0 / HALF)
        second = second * (1.0 / HALF)
        for g in range(GROUPS):
            cols = slice(g * WIDTH, (g + 1) * WIDTH)
            long_side = outs_u[g][rows, :] + got[g][rows, :].astype(F32)
            back = jnp.where(low, long_side, outs_v[g][rows, :]).astype(BF16).astype(F32)
            scaled = back * gain[:, cols]
            unit = (values[0, rows, cols].astype(F32) - mean) * inv
            grad_v[0, rows, cols] = (inv * (scaled - first - unit * second)).astype(BF16)
        return carry

    lax.fori_loop(0, ROWS // step, block, 0)


def exchanged(x, axis):
    return lax.all_to_all(x, axis, split_axis=0, concat_axis=0, tiled=True)


def per_device(gated, values_in, upstream, gain, shift, mix_w, mix_bias):
    y_index = lax.axis_index(Y)
    place = (y_index % QUAD).astype(jnp.int32).reshape(1)
    gain_row, shift_row = gain.reshape(1, HALF), shift.reshape(1, HALF)

    part_shape = [shape((ROWS, WIDTH), BF16)] * GROUPS
    full_shape = [shape((ROWS, WIDTH), F32)] * GROUPS

    pre = call(
        pre_kernel,
        "pre",
        part_shape * 2 + [shape((2, ROWS, 128), F32), shape((16, 128), F32)],
        (place, values_in, gated, upstream, gain_row, shift_row),
    )
    us, vs, stats, bias_term = pre[:4], pre[4:8], pre[8], pre[9]

    near, far, swap = [], [], []
    for g in range(GROUPS):
        near.append(lax.ppermute(vs[g], Y, NEAR))
        far.append(lax.ppermute(vs[g], Y, FAR))
        swap.append(lax.ppermute(vs[g], Y, SWAP))

    own_rows = jnp.swapaxes(mix_w, 0, 1)
    all_rows = exchanged(jnp.broadcast_to(own_rows, (8, *own_rows.shape)), DP)
    weights = call(weight_kernel, "weights", shape((GROUPS, 2 * ROWS, 3 * ROWS), BF16), (place, all_rows))

    outs_u, outs_v, got = [], [], []
    for g in range(GROUPS):
        part, out_u, out_v = call(
            functools.partial(product_kernel, g),
            "product",
            [part_shape[0], full_shape[0], full_shape[0]],
            (us[g], vs[g], near[g], far[g], swap[g], weights),
            0,
        )
        got.append(lax.ppermute(part, Y, OUT))
        outs_u.append(out_u)
        outs_v.append(out_v)

    operands = []
    for g in range(GROUPS):
        operands += [us[g], vs[g], near[g], far[g], swap[g]]
    terms = call(
        functools.partial(mix_grad_kernel, GROUPS),
        "mix_grad",
        shape((8, 2, SEG, GROUPS * ROWS), BF16),
        (place, *operands),
    )
    dealt = call(
        functools.partial(deal_kernel, GROUPS),
        "deal",
        shape((8, 2, 8, GROUPS * ROWS), BF16),
        (exchanged(terms, DP),),
        0,
    )
    added = call(add_kernel, "add", shape((2, 8, GROUPS * ROWS), BF16), (exchanged(dealt, Z),), 0)
    placed = call(
        place_kernel,
        "place",
        shape((8, GROUPS * 512), BF16),
        (lax.all_gather(added, Y, axis=0),),
        0,
    )
    grad_mix = lax.all_gather(placed, Z, axis=0, tiled=True).astype(F32).reshape(SEG, GROUPS, 512)

    sums = call(
        sums_kernel, "sums", shape((2, HALF), F32), (place, values_in, stats, *outs_u, *outs_v, *got)
    )
    small = jnp.concatenate([bias_term, sums.reshape(48, 128)], axis=0)
    for axis in (DP, Z, Y):
        small = jnp.sum(lax.all_gather(small, axis, axis=0), axis=0)

    bias_row = lax.dynamic_slice_in_dim(mix_bias, place[0] * ROWS, ROWS, 1).T
    grad_u, grad_v = call(
        post_kernel,
        "post",
        [shape((1, ROWS, HALF), BF16)] * 2,
        (place, values_in, upstream, stats, gain_row, bias_row, *outs_u, *outs_v, *got),
    )
    return (
        grad_u,
        grad_v,
        grad_mix,
        small[:16].reshape(GROUPS, 512),
        small[16:40].reshape(HALF),
        small[40:].reshape(HALF),
    )


def solution(mesh):
    torus = Mesh(mesh.devices.reshape(8, 8, 4, 2), ("sp_0", "sp_1", "dp_0", "dp_1"))
    return jax.shard_map(
        per_device,
        mesh=torus,
        in_specs=(
            P(DP, SP, None),
            P(DP, SP, None),
            P(DP, SP, None),
            P(),
            P(),
            P(DP, None, None),
            P(),
        ),
        out_specs=(P(DP, SP, None), P(DP, SP, None), P(DP, None, None), P(), P(), P()),
        check_vma=False,
    )
```

```python
import functools

import jax
import jax.numpy as jnp
from jax import lax
from jax.experimental import pallas as pl
from jax.experimental.pallas import tpu as pltpu
from jax.sharding import Mesh
from jax.sharding import PartitionSpec as P


SEG = 64
ROWS = 128
GROUPS = 4
WIDTH = 768
HALF = GROUPS * WIDTH
QUAD = 4
DP = ("dp_0", "dp_1")
SP = ("sp_0", "sp_1")
Y = "sp_1"
Z = "sp_0"
X = "dp_0"
CORE = "dp_1"
EPS = 1e-05

NEAR = [(0, 1), (3, 2), (4, 5), (7, 6)]
FAR = [(0, 2), (3, 1), (4, 6), (7, 5)]
SWAP = [(1, 2), (2, 1), (5, 6), (6, 5)]
OUT = [(1, 0), (2, 3), (5, 4), (6, 7)]
PARTNER = [(0, 1), (1, 0)]
CHIPS = [[(i, (i + k) % 4) for i in range(4)] for k in range(4)]
SETS = ((0, 1, 2), (3,))


VMEM = pl.BlockSpec(memory_space=pltpu.VMEM)
SMEM = pl.BlockSpec(memory_space=pltpu.SMEM)
F32 = jnp.float32
BF16 = jnp.bfloat16


def call(kernel, out_shape, inputs, scalars=1, scratch=(), vmem=16):
    return pl.pallas_call(
        kernel,
        out_shape=out_shape,
        in_specs=[SMEM] * scalars + [VMEM] * (len(inputs) - scalars),
        out_specs=jax.tree.map(lambda _: VMEM, out_shape),
        scratch_shapes=list(scratch),
        compiler_params=pltpu.CompilerParams(vmem_limit_bytes=vmem << 20),
    )(*inputs)


def shape(dims, dtype):
    return jax.ShapeDtypeStruct(dims, dtype)


def nt(a, b):
    return lax.dot_general(a, b, (((1,), (1,)), ((), ())), preferred_element_type=F32)


def tn(a, b):
    return lax.dot_general(a, b, (((0,), (0,)), ((), ())), preferred_element_type=F32)


def nn(a, b):
    return jnp.dot(a, b, preferred_element_type=F32)


def pre_kernel(place, values, gated, upstream, gain, shift, *outs):
    us, vs, stats, bias = outs[:4], outs[4:8], outs[8], outs[9]
    low = place[0] < 2
    step = 16

    def block(i, carry):
        rows = pl.ds(pl.multiple_of(i * step, step), step)
        raw = values[0, rows, :].astype(F32)
        mean = jnp.sum(raw, axis=1, keepdims=True) * (1.0 / HALF)
        centred = raw - mean
        var = jnp.sum(centred * centred, axis=1, keepdims=True) * (1.0 / HALF)
        inv = lax.rsqrt(var + EPS)
        stats[0, rows, :] = jnp.broadcast_to(mean, (step, 128))
        stats[1, rows, :] = jnp.broadcast_to(inv, (step, 128))
        for g in range(GROUPS):
            cols = slice(g * WIDTH, (g + 1) * WIDTH)
            unit = (values[0, rows, cols].astype(F32) - mean) * inv
            normed = (unit * gain[:, cols] + shift[:, cols]).astype(BF16)
            grad = (upstream[0, rows, cols].astype(F32) * gated[0, rows, cols].astype(F32)).astype(BF16)
            us[g][rows, :] = jnp.where(low, grad, normed)
            vs[g][rows, :] = jnp.where(low, normed, grad)
        return carry

    lax.fori_loop(0, ROWS // step, block, 0)
    bias[...] = jnp.zeros_like(bias)
    ones = jnp.ones((8, WIDTH), BF16)
    for g in range(GROUPS):
        grad = jnp.where(low, us[g][...], vs[g][...])
        bias[pl.ds(g * QUAD + place[0], 1), :] = nt(ones, grad)[:1]


def weight_kernel(place, *refs):
    mine, theirs, out, held = refs[:4], refs[4:8], refs[8], refs[9]
    p, x, core = place[0], place[1], place[2]
    low = p < 2
    for k in range(4):
        b = (x + 4 - k) % 4
        held[b, core] = mine[k][...]
        held[b, 1 - core] = theirs[k][...]
    start = jnp.where(p == 3, 1, 0)
    r = lax.broadcasted_iota(jnp.int32, (ROWS, ROWS), 0) // SEG
    c = lax.broadcasted_iota(jnp.int32, (ROWS, ROWS), 1) // SEG

    def piece(t, g, s):
        cols = pl.ds(pl.multiple_of((s - start) * ROWS, ROWS), ROWS)
        return jnp.concatenate([held[t, 0, g, :, cols], held[t, 1, g, :, cols]], axis=0)

    @pl.when(low)
    def _():
        for g in range(GROUPS):
            for i in range(2):
                for j in range(3):
                    got = piece(p + j, g, jnp.maximum(p - i, 0)).astype(F32)
                    if i == 0 and j == 0:
                        got = jnp.where(r >= c, got, 0.0)
                    out[g, i * ROWS : (i + 1) * ROWS, j * ROWS : (j + 1) * ROWS] = got.T.astype(BF16)

    @pl.when(jnp.logical_not(low))
    def _():
        for g in range(GROUPS):
            for i in range(2):
                for j in range(3):
                    got = piece(jnp.minimum(p + i, 3), g, p - j)
                    if i == 0 and j == 0:
                        got = jnp.where(r >= c, got.astype(F32), 0.0).astype(BF16)
                    out[g, i * ROWS : (i + 1) * ROWS, j * ROWS : (j + 1) * ROWS] = got


def product_kernel(g, u, v, near, far, swap, weights, part, out_u, out_v):
    own, other = weights[g, :ROWS, :], weights[g, ROWS:, :]
    long_side = jnp.concatenate([u[...], swap[...], far[...]], axis=0)
    part[...] = nn(other, long_side).astype(BF16)
    out_u[...] = nn(own, long_side)
    short_side = jnp.concatenate([v[...], near[...]], axis=0)
    both = jnp.concatenate([own[:, :ROWS], other[:, :ROWS]], axis=0)
    out_v[...] = tn(both, short_side)


def mix_grad_kernel(n, place, *refs):
    ins, keep, send = refs[: 5 * n], refs[5 * n], refs[5 * n + 1]
    p, core = place[0], place[2]
    first = core == 0
    r = lax.broadcasted_iota(jnp.int32, (ROWS, ROWS), 0) // SEG
    c = lax.broadcasted_iota(jnp.int32, (ROWS, ROWS), 1) // SEG
    keep[...] = jnp.zeros_like(keep)
    send[...] = jnp.zeros_like(send)

    def put(target, slot, k, got):
        lanes = slice(k * ROWS, (k + 1) * ROWS)
        keep[target, slot, :, lanes] = jnp.where(first, got[:SEG], got[SEG:])
        send[target, slot, :, lanes] = jnp.where(first, got[SEG:], got[:SEG]).astype(BF16)

    for k in range(n):
        u, v, near, far, swap = ins[5 * k : 5 * k + 5]

        @pl.when(p == 0)
        def _():
            put(0, 0, k, jnp.where(r >= c, nt(u[...], v[...]), 0.0))

        @pl.when(p == 1)
        def _():
            put(1, 0, k, nt(u[...], near[...]))
            put(1, 1, k, jnp.where(r >= c, nt(u[...], v[...]), 0.0))
            put(2, 0, k, nt(swap[...], near[...]))
            put(3, 0, k, nt(far[...], near[...]))

        @pl.when(p == 2)
        def _():
            put(2, 0, k, jnp.where(r >= c, nt(v[...], u[...]), 0.0))
            put(2, 1, k, nt(v[...], swap[...]))
            put(3, 0, k, nt(near[...], u[...]))
            put(3, 1, k, nt(near[...], swap[...]))

        @pl.when(p == 3)
        def _():
            put(3, 0, k, jnp.where(r >= c, nt(v[...], u[...]), 0.0))


def core_sum_kernel(place, keep, got, mine, *sends):
    x = place[1]
    mine[...] = keep[x] + got[x].astype(F32)
    for k in range(1, 4):
        b = (x + k) % 4
        sends[k - 1][...] = (keep[b] + got[b].astype(F32)).astype(BF16)


def split(x):
    high = x.astype(BF16)
    return high, (x - high.astype(F32)).astype(BF16)


def deal_kernel(*refs):
    small, out = refs[8:12], refs[12]
    extra = small[0][...] + small[1][...] + small[2][...] + small[3][...]
    high, low = split(extra)
    for z in range(8):
        out[z, :, 1024:1152] = high[z * 8 : (z + 1) * 8]
        out[z, :, 1152:1280] = low[z * 8 : (z + 1) * 8]
    lane = 0
    for i, groups in enumerate(SETS):
        parts = refs[4 * i : 4 * i + 4]
        width = len(groups) * ROWS
        for slot in range(2):
            total = parts[0][slot]
            for k in range(1, 4):
                total = total + parts[k][slot].astype(F32)
            total = total.astype(BF16)
            for z in range(8):
                out[z, :, slot * 512 + lane : slot * 512 + lane + width] = total[z * 8 : (z + 1) * 8]
        lane += width


def add_kernel(got, out):
    total = got[0].astype(F32)
    for z in range(1, 8):
        total = total + got[z].astype(F32)
    extra = total[:, 1024:1152] + total[:, 1152:1280]
    high, low = split(extra)
    total = total[:, :1024].astype(BF16)
    for y in range(8):
        out[y, :, :1024] = total
        out[y, :, 1024:1152] = high
        out[y, :, 1152:1280] = low


def place_kernel(got, out):
    def at(place, slot):
        lanes = slice(slot * 512, (slot + 1) * 512)
        return got[place, :, lanes].astype(F32) + got[place + QUAD, :, lanes].astype(F32)

    columns = (at(0, 0) + at(1, 0), at(1, 1) + at(2, 1), at(2, 0), at(3, 0))
    columns = [c.astype(BF16) for c in columns]
    extra = jnp.zeros((8, 128), F32)
    for y in range(8):
        extra = extra + got[y, :, 1024:1152].astype(F32) + got[y, :, 1152:1280].astype(F32)
    high, low = split(extra)
    for z in range(8):
        for s in range(4):
            for g in range(GROUPS):
                out[z, :, g * 512 + s * ROWS : g * 512 + (s + 1) * ROWS] = columns[s][
                    :, g * ROWS : (g + 1) * ROWS
                ]
        out[z, :, 2048:2176] = high
        out[z, :, 2176:2304] = low


def final_kernel(got, grad_mix, small):
    for z in range(8):
        rows = slice(z * 8, (z + 1) * 8)
        for g in range(GROUPS):
            grad_mix[rows, g, :] = got[z, :, g * 512 : (g + 1) * 512].astype(F32)
        small[rows, :] = got[z, :, 2048:2176].astype(F32) + got[z, :, 2176:2304].astype(F32)


def sums_kernel(place, values, stats, bias, *refs):
    outs_u, outs_v, got, out = refs[:4], refs[4:8], refs[8:12], refs[12]
    low = place[0] < 2
    out[:16] = bias[...]
    mean = stats[0, :, :1]
    inv = stats[1, :, :1]
    for g in range(GROUPS):
        for i in range(WIDTH // 128):
            own = slice(i * 128, (i + 1) * 128)
            cols = slice(g * WIDTH + i * 128, g * WIDTH + (i + 1) * 128)
            back = jnp.where(low, outs_u[g][:, own] + got[g][:, own].astype(F32), outs_v[g][:, own])
            back = back.astype(BF16).astype(F32)
            unit = (values[0, :, cols].astype(F32) - mean) * inv
            row = 16 + g * 6 + i
            out[row : row + 1] = jnp.sum(back * unit, axis=0, keepdims=True)
            out[row + 24 : row + 25] = jnp.sum(back, axis=0, keepdims=True)


def post_kernel(place, values, upstream, stats, gain, bias_row, *refs):
    outs_u, outs_v, got, grad_u, grad_v = refs[:4], refs[4:8], refs[8:12], refs[12], refs[13]
    low = place[0] < 2
    step = 16

    def block(i, carry):
        rows = pl.ds(pl.multiple_of(i * step, step), step)
        mean = stats[0, rows, :1]
        inv = stats[1, rows, :1]
        first = jnp.zeros((step, 1), F32)
        second = jnp.zeros((step, 1), F32)
        for g in range(GROUPS):
            cols = slice(g * WIDTH, (g + 1) * WIDTH)
            long_side = outs_u[g][rows, :] + got[g][rows, :].astype(F32)
            short_side = outs_v[g][rows, :]
            mixed = jnp.where(low, short_side, long_side) + bias_row[rows, g : g + 1]
            mixed = mixed.astype(BF16).astype(F32)
            grad_u[0, rows, cols] = (upstream[0, rows, cols].astype(F32) * mixed).astype(BF16)
            back = jnp.where(low, long_side, short_side).astype(BF16).astype(F32)
            scaled = back * gain[:, cols]
            unit = (values[0, rows, cols].astype(F32) - mean) * inv
            first = first + jnp.sum(scaled, axis=1, keepdims=True)
            second = second + jnp.sum(scaled * unit, axis=1, keepdims=True)
        first = first * (1.0 / HALF)
        second = second * (1.0 / HALF)
        for g in range(GROUPS):
            cols = slice(g * WIDTH, (g + 1) * WIDTH)
            long_side = outs_u[g][rows, :] + got[g][rows, :].astype(F32)
            back = jnp.where(low, long_side, outs_v[g][rows, :]).astype(BF16).astype(F32)
            scaled = back * gain[:, cols]
            unit = (values[0, rows, cols].astype(F32) - mean) * inv
            grad_v[0, rows, cols] = (inv * (scaled - first - unit * second)).astype(BF16)
        return carry

    lax.fori_loop(0, ROWS // step, block, 0)


def exchanged(x, axis):
    return lax.all_to_all(x, axis, split_axis=0, concat_axis=0, tiled=True)


def compute(gated, values_in, upstream, gain, shift, mix_w, mix_bias):
    spot = lax.axis_index(Y) % QUAD
    place = jnp.stack([spot, lax.axis_index(X), lax.axis_index(CORE)]).astype(jnp.int32)
    gain_row, shift_row = gain.reshape(1, HALF), shift.reshape(1, HALF)

    half = shape((ROWS, WIDTH), BF16)
    full = shape((ROWS, WIDTH), F32)

    first = jnp.where(spot == 3, ROWS, 0)
    own_rows = lax.dynamic_slice_in_dim(jnp.swapaxes(mix_w, 0, 1), first, 3 * ROWS, 2)
    mine = [own_rows] + [lax.ppermute(own_rows, X, CHIPS[k]) for k in range(1, 4)]
    theirs = [lax.ppermute(rows, CORE, PARTNER) for rows in mine]

    pre = call(
        pre_kernel,
        [half] * 8 + [shape((2, ROWS, 128), F32), shape((16, 128), F32)],
        (place, values_in, gated, upstream, gain_row, shift_row),
    )
    us, vs, stats, bias_term = pre[:4], pre[4:8], pre[8], pre[9]

    near, far, swap = [], [], []
    for g in range(GROUPS):
        near.append(lax.ppermute(vs[g], Y, NEAR))
        far.append(lax.ppermute(vs[g], Y, FAR))
        swap.append(lax.ppermute(vs[g], Y, SWAP))

    weights = call(
        weight_kernel,
        shape((GROUPS, 2 * ROWS, 3 * ROWS), BF16),
        (place, *mine, *theirs),
        scratch=[pltpu.VMEM((4, 2, GROUPS, SEG, 3 * ROWS), BF16)],
    )

    outs_u, outs_v, got = [], [], []
    for g in range(GROUPS):
        part, out_u, out_v = call(
            functools.partial(product_kernel, g),
            [half, full, full],
            (us[g], vs[g], near[g], far[g], swap[g], weights),
            0,
        )
        got.append(lax.ppermute(part, Y, OUT))
        outs_u.append(out_u)
        outs_v.append(out_v)

    terms = []
    for groups in SETS:
        operands = []
        for g in groups:
            operands += [us[g], vs[g], near[g], far[g], swap[g]]
        width = len(groups) * ROWS
        keep, send = call(
            functools.partial(mix_grad_kernel, len(groups)),
            [shape((4, 2, SEG, width), F32), shape((4, 2, SEG, width), BF16)],
            (place, *operands),
        )
        sums = call(
            core_sum_kernel,
            [shape((2, SEG, width), F32)] + [shape((2, SEG, width), BF16)] * 3,
            (place, keep, lax.ppermute(send, CORE, PARTNER)),
        )
        terms += [sums[0]] + [lax.ppermute(sums[k], X, CHIPS[k]) for k in range(1, 4)]

    small = call(
        sums_kernel,
        shape((64, 128), F32),
        (place, values_in, stats, bias_term, *outs_u, *outs_v, *got),
    )
    small = small + lax.ppermute(small, CORE, PARTNER)
    smalls = [small] + [lax.ppermute(small, X, CHIPS[k]) for k in range(1, 4)]

    dealt = call(deal_kernel, shape((8, 8, 1280), BF16), (*terms, *smalls), 0)
    added = call(add_kernel, shape((8, 8, 1280), BF16), (exchanged(dealt, Z),), 0)
    placed = call(place_kernel, shape((8, 8, 2304), BF16), (exchanged(added, Y),), 0)
    grad_mix, small = call(
        final_kernel,
        [shape((SEG, GROUPS, 512), F32), shape((64, 128), F32)],
        (exchanged(placed, Z),),
        0,
    )

    bias_row = lax.dynamic_slice_in_dim(mix_bias, spot * ROWS, ROWS, 1).T
    grad_u, grad_v = call(
        post_kernel,
        [shape((1, ROWS, HALF), BF16)] * 2,
        (place, values_in, upstream, stats, gain_row, bias_row, *outs_u, *outs_v, *got),
    )
    return (
        grad_u,
        grad_v,
        grad_mix,
        small[:16].reshape(GROUPS, 512),
        small[16:40].reshape(HALF),
        small[40:].reshape(HALF),
    )


def solution(mesh):
    torus = Mesh(mesh.devices.reshape(8, 8, 4, 2), ("sp_0", "sp_1", "dp_0", "dp_1"))
    return jax.shard_map(
        compute,
        mesh=torus,
        in_specs=(
            P(DP, SP, None),
            P(DP, SP, None),
            P(DP, SP, None),
            P(),
            P(),
            P(DP, None, None),
            P(),
        ),
        out_specs=(P(DP, SP, None), P(DP, SP, None), P(DP, None, None), P(), P(), P()),
        check_vma=False,
    )
```

```python
import functools

import jax
import jax.numpy as jnp
from jax import lax
from jax.experimental import pallas as pl
from jax.experimental.pallas import tpu as pltpu
from jax.sharding import Mesh
from jax.sharding import PartitionSpec as P


SEG = 64
ROWS = 128
GROUPS = 4
WIDTH = 768
HALF = GROUPS * WIDTH
QUAD = 4
DP = ("dp_0", "dp_1")
SP = ("sp_0", "sp_1")
Y = "sp_1"
Z = "sp_0"
X = "dp_0"
CORE = "dp_1"
EPS = 1e-05

NEAR = [(0, 1), (3, 2), (4, 5), (7, 6)]
FAR = [(0, 2), (3, 1), (4, 6), (7, 5)]
SWAP = [(1, 2), (2, 1), (5, 6), (6, 5)]
OUT = [(1, 0), (2, 3), (5, 4), (6, 7)]
PARTNER = [(0, 1), (1, 0)]

CHUNKS = (3, 1)
PLACES = [(i, k * WIDTH) for i, n in enumerate(CHUNKS) for k in range(n)]


VMEM = pl.BlockSpec(memory_space=pltpu.VMEM)
SMEM = pl.BlockSpec(memory_space=pltpu.SMEM)
F32 = jnp.float32
BF16 = jnp.bfloat16


def call(kernel, out_shape, inputs, scalars=1, scratch=(), vmem=16):
    return pl.pallas_call(
        kernel,
        out_shape=out_shape,
        in_specs=[SMEM] * scalars + [VMEM] * (len(inputs) - scalars),
        out_specs=jax.tree.map(lambda _: VMEM, out_shape),
        scratch_shapes=list(scratch),
        compiler_params=pltpu.CompilerParams(vmem_limit_bytes=vmem << 20),
    )(*inputs)


def shape(dims, dtype):
    return jax.ShapeDtypeStruct(dims, dtype)


def nt(a, b):
    return lax.dot_general(a, b, (((1,), (1,)), ((), ())), preferred_element_type=F32)


def tn(a, b):
    return lax.dot_general(a, b, (((0,), (0,)), ((), ())), preferred_element_type=F32)


def nn(a, b):
    return jnp.dot(a, b, preferred_element_type=F32)


def lanes_of(g, width=WIDTH):
    chunk, start = PLACES[g]
    start = start // WIDTH * width
    return chunk, slice(start, start + width)


def pre_kernel(place, values, gated, upstream, gain, shift, mix_bias, *outs):
    n = len(CHUNKS)
    us, vs, stats, bias = outs[:n], outs[n : 2 * n], outs[2 * n], outs[2 * n + 1]
    p = place[0]
    low = p < 2
    step = 16

    def block(i, carry):
        rows = pl.ds(pl.multiple_of(i * step, step), step)
        raw = values[0, rows, :].astype(F32)
        mean = jnp.sum(raw, axis=1, keepdims=True) * (1.0 / HALF)
        centred = raw - mean
        var = jnp.sum(centred * centred, axis=1, keepdims=True) * (1.0 / HALF)
        inv = lax.rsqrt(var + EPS)
        stats[0, rows, :] = jnp.broadcast_to(mean, (step, 128))
        stats[1, rows, :] = jnp.broadcast_to(inv, (step, 128))
        for g in range(GROUPS):
            cols = slice(g * WIDTH, (g + 1) * WIDTH)
            unit = (values[0, rows, cols].astype(F32) - mean) * inv
            normed = (unit * gain[:, cols] + shift[:, cols]).astype(BF16)
            grad = (upstream[0, rows, cols].astype(F32) * gated[0, rows, cols].astype(F32)).astype(BF16)
            i, lanes = lanes_of(g)
            us[i][rows, lanes] = jnp.where(low, grad, normed)
            vs[i][rows, lanes] = jnp.where(low, normed, grad)
        return carry

    lax.fori_loop(0, ROWS // step, block, 0)
    own_bias = mix_bias[:, pl.ds(pl.multiple_of(p * ROWS, ROWS), ROWS)]
    stats[2] = jnp.concatenate([own_bias, jnp.zeros((ROWS - GROUPS, ROWS), F32)], axis=0).T
    bias[...] = jnp.zeros_like(bias)
    ones = jnp.ones((8, WIDTH), BF16)
    for g in range(GROUPS):
        i, lanes = lanes_of(g)
        grad = jnp.where(low, us[i][:, lanes], vs[i][:, lanes])
        bias[pl.ds(g * QUAD + p, 1), :] = nt(ones, grad)[:1]


def weight_kernel(place, held, out):
    p = place[0]
    low = p < 2
    start = jnp.where(p == 3, 1, 0)
    r = lax.broadcasted_iota(jnp.int32, (ROWS, ROWS), 0) // SEG
    c = lax.broadcasted_iota(jnp.int32, (ROWS, ROWS), 1) // SEG

    def piece(t, g, s):
        cols = pl.ds(pl.multiple_of((s - start) * ROWS, ROWS), ROWS)
        return jnp.concatenate([held[2 * t, g, :, cols], held[2 * t + 1, g, :, cols]], axis=0)

    @pl.when(low)
    def _():
        for g in range(GROUPS):
            for i in range(2):
                for j in range(3):
                    got = piece(p + j, g, jnp.maximum(p - i, 0)).astype(F32)
                    if i == 0 and j == 0:
                        got = jnp.where(r >= c, got, 0.0)
                    out[g, i * ROWS : (i + 1) * ROWS, j * ROWS : (j + 1) * ROWS] = got.T.astype(BF16)

    @pl.when(jnp.logical_not(low))
    def _():
        for g in range(GROUPS):
            for i in range(2):
                for j in range(3):
                    got = piece(jnp.minimum(p + i, 3), g, p - j)
                    if i == 0 and j == 0:
                        got = jnp.where(r >= c, got.astype(F32), 0.0).astype(BF16)
                    out[g, i * ROWS : (i + 1) * ROWS, j * ROWS : (j + 1) * ROWS] = got


def product_kernel(chunk, u, v, near, far, swap, weights, part, out_u, out_v):
    for g in range(GROUPS):
        i, lanes = lanes_of(g)
        if i != chunk:
            continue
        own, other = weights[g, :ROWS, :], weights[g, ROWS:, :]
        long_side = jnp.concatenate([u[:, lanes], swap[:, lanes], far[:, lanes]], axis=0)
        part[:, lanes] = nn(other, long_side).astype(BF16)
        out_u[:, lanes] = nn(own, long_side)
        short_side = jnp.concatenate([v[:, lanes], near[:, lanes]], axis=0)
        both = jnp.concatenate([own[:, :ROWS], other[:, :ROWS]], axis=0)
        out_v[:, lanes] = tn(both, short_side)


def mix_grad_kernel(n, place, u, v, near, far, swap, keep, send):
    p, core = place[0], place[2]
    first = core == 0
    r = lax.broadcasted_iota(jnp.int32, (ROWS, ROWS), 0) // SEG
    c = lax.broadcasted_iota(jnp.int32, (ROWS, ROWS), 1) // SEG
    keep[...] = jnp.zeros_like(keep)
    send[...] = jnp.zeros_like(send)

    def put(target, slot, k, got):
        lanes = slice((slot * n + k) * ROWS, (slot * n + k + 1) * ROWS)
        keep[target, :, lanes] = jnp.where(first, got[:SEG], got[SEG:])
        send[target, :, lanes] = jnp.where(first, got[SEG:], got[:SEG]).astype(BF16)

    for k in range(n):
        at = slice(k * WIDTH, (k + 1) * WIDTH)

        @pl.when(p == 0)
        def _():
            put(0, 0, k, jnp.where(r >= c, nt(u[:, at], v[:, at]), 0.0))

        @pl.when(p == 1)
        def _():
            put(1, 0, k, nt(u[:, at], near[:, at]))
            put(1, 1, k, jnp.where(r >= c, nt(u[:, at], v[:, at]), 0.0))
            put(2, 0, k, nt(swap[:, at], near[:, at]))
            put(3, 0, k, nt(far[:, at], near[:, at]))

        @pl.when(p == 2)
        def _():
            put(2, 0, k, jnp.where(r >= c, nt(v[:, at], u[:, at]), 0.0))
            put(2, 1, k, nt(v[:, at], swap[:, at]))
            put(3, 0, k, nt(near[:, at], u[:, at]))
            put(3, 1, k, nt(near[:, at], swap[:, at]))

        @pl.when(p == 3)
        def _():
            put(3, 0, k, jnp.where(r >= c, nt(v[:, at], u[:, at]), 0.0))


def split(x):
    high = x.astype(BF16)
    return high, (x - high.astype(F32)).astype(BF16)


def sums_kernel(place, values, stats, bias, last, *refs):
    n = len(CHUNKS)
    outs_u, outs_v, got, small, send = refs[:n], refs[n : 2 * n], refs[2 * n : 3 * n], refs[3 * n], refs[3 * n + 1]
    low = place[0] < 2
    small[:16] = bias[...]
    mean = stats[0, :, :1]
    inv = stats[1, :, :1]
    for g in range(GROUPS):
        i, lanes = lanes_of(g)
        for k in range(WIDTH // 128):
            own = slice(lanes.start + k * 128, lanes.start + (k + 1) * 128)
            cols = slice(g * WIDTH + k * 128, g * WIDTH + (k + 1) * 128)
            back = jnp.where(low, outs_u[i][:, own] + got[i][:, own].astype(F32), outs_v[i][:, own])
            back = back.astype(BF16).astype(F32)
            unit = (values[0, :, cols].astype(F32) - mean) * inv
            row = 16 + g * 6 + k
            small[row : row + 1] = jnp.sum(back * unit, axis=0, keepdims=True)
            small[row + 24 : row + 25] = jnp.sum(back, axis=0, keepdims=True)
    send[:4] = last[...]
    high, low_part = split(small[...])
    send[4, :, :128] = high
    send[4, :, 128:] = low_part


def chip_kernel(keep0, keep1, small, got0, got1, out):
    extra = small[...] + (got1[4, :, :128].astype(F32) + got1[4, :, 128:].astype(F32))
    high, low = split(extra)
    for b in range(4):
        for i, (keep, got) in enumerate(((keep0, got0), (keep1, got1))):
            total = (keep[b] + got[b].astype(F32)).astype(BF16)
            width = CHUNKS[i] * ROWS
            lane = sum(CHUNKS[:i]) * ROWS
            for slot in range(2):
                out[b, :, slot * 512 + lane : slot * 512 + lane + width] = total[
                    :, slot * width : (slot + 1) * width
                ]
        out[b, :, 1024:1152] = high
        out[b, :, 1152:1280] = low


def total_of(got):
    total = got[0].astype(F32)
    for k in range(1, got.shape[0]):
        total = total + got[k].astype(F32)
    high, low = split(total[:, 1024:1152] + total[:, 1152:1280])
    return total[:, :1024].astype(BF16), high, low


def deal_kernel(got, out):
    total, high, low = total_of(got)
    for z in range(8):
        rows = slice(z * 8, (z + 1) * 8)
        out[z, :, :1024] = total[rows]
        out[z, :, 1024:1152] = high[rows]
        out[z, :, 1152:1280] = low[rows]


def add_kernel(got, out):
    total, high, low = total_of(got)
    for y in range(8):
        out[y, :, :1024] = total
        out[y, :, 1024:1152] = high
        out[y, :, 1152:1280] = low


def place_kernel(got, out):
    def at(place, slot):
        lanes = slice(slot * 512, (slot + 1) * 512)
        return got[place, :, lanes].astype(F32) + got[place + QUAD, :, lanes].astype(F32)

    columns = (at(0, 0) + at(1, 0), at(1, 1) + at(2, 1), at(2, 0), at(3, 0))
    columns = [c.astype(BF16) for c in columns]
    extra = jnp.zeros((8, 128), F32)
    for y in range(8):
        extra = extra + got[y, :, 1024:1152].astype(F32) + got[y, :, 1152:1280].astype(F32)
    high, low = split(extra)
    for z in range(8):
        for s in range(4):
            for g in range(GROUPS):
                out[z, :, g * 512 + s * ROWS : g * 512 + (s + 1) * ROWS] = columns[s][
                    :, g * ROWS : (g + 1) * ROWS
                ]
        out[z, :, 2048:2176] = high
        out[z, :, 2176:2304] = low


def final_kernel(got, grad_mix, grad_bias, grad_gain, grad_shift):
    for z in range(8):
        rows = slice(z * 8, (z + 1) * 8)
        for g in range(GROUPS):
            grad_mix[rows, g, :] = got[z, :, g * 512 : (g + 1) * 512].astype(F32)
        small = got[z, :, 2048:2176].astype(F32) + got[z, :, 2176:2304].astype(F32)
        if z < 2:
            for i in range(8):
                g, p = 2 * z + i // QUAD, i % QUAD
                grad_bias[g : g + 1, p * ROWS : (p + 1) * ROWS] = small[i : i + 1]
        elif z < 5:
            grad_gain[(z - 2) * 8 : (z - 1) * 8] = small
        else:
            grad_shift[(z - 5) * 8 : (z - 4) * 8] = small


def post_kernel(place, values, upstream, stats, gain, *refs):
    n = len(CHUNKS)
    outs_u, outs_v, got, grad_u, grad_v = refs[:n], refs[n : 2 * n], refs[2 * n : 3 * n], refs[3 * n], refs[3 * n + 1]
    low = place[0] < 2
    step = 16

    def block(i, carry):
        rows = pl.ds(pl.multiple_of(i * step, step), step)
        mean = stats[0, rows, :1]
        inv = stats[1, rows, :1]
        first = jnp.zeros((step, 1), F32)
        second = jnp.zeros((step, 1), F32)
        for g in range(GROUPS):
            cols = slice(g * WIDTH, (g + 1) * WIDTH)
            c, lanes = lanes_of(g)
            long_side = outs_u[c][rows, lanes] + got[c][rows, lanes].astype(F32)
            short_side = outs_v[c][rows, lanes]
            mixed = jnp.where(low, short_side, long_side) + stats[2, rows, g : g + 1]
            mixed = mixed.astype(BF16).astype(F32)
            grad_u[0, rows, cols] = (upstream[0, rows, cols].astype(F32) * mixed).astype(BF16)
            back = jnp.where(low, long_side, short_side).astype(BF16).astype(F32)
            scaled = back * gain[:, cols]
            unit = (values[0, rows, cols].astype(F32) - mean) * inv
            first = first + jnp.sum(scaled, axis=1, keepdims=True)
            second = second + jnp.sum(scaled * unit, axis=1, keepdims=True)
        first = first * (1.0 / HALF)
        second = second * (1.0 / HALF)
        for g in range(GROUPS):
            cols = slice(g * WIDTH, (g + 1) * WIDTH)
            c, lanes = lanes_of(g)
            long_side = outs_u[c][rows, lanes] + got[c][rows, lanes].astype(F32)
            back = jnp.where(low, long_side, outs_v[c][rows, lanes]).astype(BF16).astype(F32)
            scaled = back * gain[:, cols]
            unit = (values[0, rows, cols].astype(F32) - mean) * inv
            grad_v[0, rows, cols] = (inv * (scaled - first - unit * second)).astype(BF16)
        return carry

    lax.fori_loop(0, ROWS // step, block, 0)


def exchanged(x, axis):
    return lax.all_to_all(x, axis, split_axis=0, concat_axis=0, tiled=True)


def compute(gated, values_in, upstream, gain, shift, mix_w, mix_bias):
    spot = lax.axis_index(Y) % QUAD
    place = jnp.stack([spot, lax.axis_index(X), lax.axis_index(CORE)]).astype(jnp.int32)
    gain_row, shift_row = gain.reshape(1, HALF), shift.reshape(1, HALF)
    n = len(CHUNKS)
    halves = [shape((ROWS, k * WIDTH), BF16) for k in CHUNKS]
    fulls = [shape((ROWS, k * WIDTH), F32) for k in CHUNKS]

    pre = call(
        pre_kernel,
        halves * 2 + [shape((3, ROWS, 128), F32), shape((16, 128), F32)],
        (place, values_in, gated, upstream, gain_row, shift_row, mix_bias),
    )
    us, vs, stats, bias_term = pre[:n], pre[n : 2 * n], pre[2 * n], pre[2 * n + 1]

    near, far, swap = [], [], []
    for i in range(n):
        near.append(lax.ppermute(vs[i], Y, NEAR))
        far.append(lax.ppermute(vs[i], Y, FAR))
        swap.append(lax.ppermute(vs[i], Y, SWAP))

    first = jnp.where(spot == 3, ROWS, 0)
    own_rows = lax.dynamic_slice_in_dim(jnp.swapaxes(mix_w, 0, 1), first, 3 * ROWS, 2)
    all_rows = exchanged(jnp.broadcast_to(own_rows, (8, *own_rows.shape)), DP)
    weights = call(weight_kernel, shape((GROUPS, 2 * ROWS, 3 * ROWS), BF16), (place, all_rows))

    outs_u, outs_v, got, keeps, sends = [], [], [], [], []
    for i in range(n):
        operands = (us[i], vs[i], near[i], far[i], swap[i])
        part, out_u, out_v = call(
            functools.partial(product_kernel, i),
            [halves[i], fulls[i], fulls[i]],
            (*operands, weights),
            0,
        )
        got.append(lax.ppermute(part, Y, OUT))
        outs_u.append(out_u)
        outs_v.append(out_v)
        dims = (4, SEG, 2 * CHUNKS[i] * ROWS)
        keep, send = call(
            functools.partial(mix_grad_kernel, CHUNKS[i]),
            [shape(dims, F32), shape(dims, BF16)],
            (place, *operands),
        )
        keeps.append(keep)
        sends.append(send)

    small, last = call(
        sums_kernel,
        [shape((64, 128), F32), shape((5, SEG, 2 * ROWS), BF16)],
        (place, values_in, stats, bias_term, sends[1], *outs_u, *outs_v, *got),
    )
    folded = [lax.ppermute(sends[0], CORE, PARTNER), lax.ppermute(last, CORE, PARTNER)]
    chip = call(chip_kernel, shape((4, SEG, 1280), BF16), (*keeps, small, *folded), 0)
    dealt = call(deal_kernel, shape((8, 8, 1280), BF16), (exchanged(chip, X),), 0)
    added = call(add_kernel, shape((8, 8, 1280), BF16), (exchanged(dealt, Z),), 0)
    placed = call(place_kernel, shape((8, 8, 2304), BF16), (exchanged(added, Y),), 0)
    grad_mix, grad_bias, grad_gain, grad_shift = call(
        final_kernel,
        [shape((SEG, GROUPS, 512), F32), shape((GROUPS, 512), F32)] + [shape((24, 128), F32)] * 2,
        (exchanged(placed, Z),),
        0,
    )

    grad_u, grad_v = call(
        post_kernel,
        [shape((1, ROWS, HALF), BF16)] * 2,
        (place, values_in, upstream, stats, gain_row, *outs_u, *outs_v, *got),
    )
    return (grad_u, grad_v, grad_mix, grad_bias, grad_gain.reshape(HALF), grad_shift.reshape(HALF))


def solution(mesh):
    torus = Mesh(mesh.devices.reshape(8, 8, 4, 2), ("sp_0", "sp_1", "dp_0", "dp_1"))
    return jax.shard_map(
        compute,
        mesh=torus,
        in_specs=(
            P(DP, SP, None),
            P(DP, SP, None),
            P(DP, SP, None),
            P(),
            P(),
            P(DP, None, None),
            P(),
        ),
        out_specs=(P(DP, SP, None), P(DP, SP, None), P(DP, None, None), P(), P(), P()),
        check_vma=False,
    )
```

```python
import functools

import jax
import jax.numpy as jnp
from jax import lax
from jax.experimental import pallas as pl
from jax.experimental.pallas import tpu as pltpu
from jax.sharding import Mesh
from jax.sharding import PartitionSpec as P


SEG = 64
ROWS = 128
GROUPS = 4
WIDTH = 768
HALF = GROUPS * WIDTH
QUAD = 4
DP = ("dp_0", "dp_1")
SP = ("sp_0", "sp_1")
Y = "sp_1"
Z = "sp_0"
X = "dp_0"
CORE = "dp_1"
EPS = 1e-05

NEAR = [(0, 1), (3, 2), (4, 5), (7, 6)]
FAR = [(0, 2), (3, 1), (4, 6), (7, 5)]
SWAP = [(1, 2), (2, 1), (5, 6), (6, 5)]
OUT = [(1, 0), (2, 3), (5, 4), (6, 7)]
PARTNER = [(0, 1), (1, 0)]
CHIPS = [[(i, (i + k) % 4) for i in range(4)] for k in range(4)]

CHUNKS = (3, 1)
PLACES = [(i, k * WIDTH) for i, n in enumerate(CHUNKS) for k in range(n)]


VMEM = pl.BlockSpec(memory_space=pltpu.VMEM)
SMEM = pl.BlockSpec(memory_space=pltpu.SMEM)
HBM = pl.BlockSpec(memory_space=pltpu.HBM)
F32 = jnp.float32
BF16 = jnp.bfloat16


def far_memory(x):
    return pltpu.with_memory_space_constraint(x, pltpu.HBM)


def call(kernel, out_shape, inputs, scalars=1, scratch=(), vmem=16, remote=()):
    return pl.pallas_call(
        kernel,
        out_shape=out_shape,
        in_specs=[SMEM] * scalars + [HBM if i in remote else VMEM for i in range(scalars, len(inputs))],
        out_specs=jax.tree.map(lambda _: VMEM, out_shape),
        scratch_shapes=list(scratch),
        compiler_params=pltpu.CompilerParams(vmem_limit_bytes=vmem << 20),
    )(*inputs)


def shape(dims, dtype):
    return jax.ShapeDtypeStruct(dims, dtype)


def nt(a, b):
    return lax.dot_general(a, b, (((1,), (1,)), ((), ())), preferred_element_type=F32)


def tn(a, b):
    return lax.dot_general(a, b, (((0,), (0,)), ((), ())), preferred_element_type=F32)


def nn(a, b):
    return jnp.dot(a, b, preferred_element_type=F32)


def lanes_of(g, width=WIDTH):
    chunk, start = PLACES[g]
    start = start // WIDTH * width
    return chunk, slice(start, start + width)


def pre_kernel(place, values_in, gated_in, upstream_in, gain_in, shift_in, bias_in, *outs):
    n = len(CHUNKS)
    us, vs, stats, bias = outs[:n], outs[n : 2 * n], outs[2 * n], outs[2 * n + 1]
    values, gated, upstream, gain, shift, mix_bias, sems, few = outs[2 * n + 2 :]
    p = place[0]
    low = p < 2
    step = 16
    part = ROWS // 4
    pairs = ((values_in, values), (gated_in, gated), (upstream_in, upstream))

    def copy(k, i):
        rows = slice(i * part, (i + 1) * part)
        return pltpu.make_async_copy(pairs[k][0].at[0, rows], pairs[k][1].at[0, rows], sems.at[k, i])

    singles = [
        pltpu.make_async_copy(source, target, few.at[k])
        for k, (source, target) in enumerate(((gain_in, gain), (shift_in, shift), (bias_in, mix_bias)))
    ]
    copy(0, 0).start()
    for single in singles:
        single.start()
    copy(1, 0).start()
    copy(2, 0).start()
    for i in range(1, 4):
        for k in range(3):
            copy(k, i).start()
    for single in singles:
        single.wait()

    def block(i, carry):
        rows = pl.ds(pl.multiple_of(i * step, step), step)
        raw = values[0, rows, :].astype(F32)
        mean = jnp.sum(raw, axis=1, keepdims=True) * (1.0 / HALF)
        centred = raw - mean
        var = jnp.sum(centred * centred, axis=1, keepdims=True) * (1.0 / HALF)
        inv = lax.rsqrt(var + EPS)
        stats[0, rows, :] = jnp.broadcast_to(mean, (step, 128))
        stats[1, rows, :] = jnp.broadcast_to(inv, (step, 128))
        for g in range(GROUPS):
            cols = slice(g * WIDTH, (g + 1) * WIDTH)
            unit = (values[0, rows, cols].astype(F32) - mean) * inv
            normed = (unit * gain[:, cols] + shift[:, cols]).astype(BF16)
            grad = (upstream[0, rows, cols].astype(F32) * gated[0, rows, cols].astype(F32)).astype(BF16)
            i, lanes = lanes_of(g)
            us[i][rows, lanes] = jnp.where(low, grad, normed)
            vs[i][rows, lanes] = jnp.where(low, normed, grad)
        return carry

    for i in range(4):
        for k in range(3):
            copy(k, i).wait()
        lax.fori_loop(i * part // step, (i + 1) * part // step, block, 0)
    own_bias = mix_bias[:, pl.ds(pl.multiple_of(p * ROWS, ROWS), ROWS)]
    stats[2] = jnp.concatenate([own_bias, jnp.zeros((ROWS - GROUPS, ROWS), F32)], axis=0).T
    bias[...] = jnp.zeros_like(bias)
    ones = jnp.ones((8, WIDTH), BF16)
    for g in range(GROUPS):
        i, lanes = lanes_of(g)
        grad = jnp.where(low, us[i][:, lanes], vs[i][:, lanes])
        bias[pl.ds(g * QUAD + p, 1), :] = nt(ones, grad)[:1]


def slab_kernel(place, rows, out):
    p = place[0]

    @pl.when(p < 3)
    def _():
        for g in range(GROUPS):
            out[g] = rows[:, g, : 3 * ROWS]

    @pl.when(p == 3)
    def _():
        for g in range(GROUPS):
            out[g] = rows[:, g, ROWS:]


def join_kernel(place, *refs):
    for k in range(4):
        refs[4][(place[1] + 4 - k) % 4] = refs[k][...]


def weight_kernel(place, mine, theirs, out):
    p, core = place[0], place[2]
    low = p < 2
    first = core == 0
    start = jnp.where(p == 3, 1, 0)
    r = lax.broadcasted_iota(jnp.int32, (ROWS, ROWS), 0) // SEG
    c = lax.broadcasted_iota(jnp.int32, (ROWS, ROWS), 1) // SEG

    def piece(t, g, s):
        cols = pl.ds(pl.multiple_of((s - start) * ROWS, ROWS), ROWS)
        ours, others = mine[t, g, :, cols], theirs[t, g, :, cols]
        return jnp.concatenate([jnp.where(first, ours, others), jnp.where(first, others, ours)], axis=0)

    @pl.when(low)
    def _():
        for g in range(GROUPS):
            for i in range(2):
                for j in range(3):
                    got = piece(p + j, g, jnp.maximum(p - i, 0)).astype(F32)
                    if i == 0 and j == 0:
                        got = jnp.where(r >= c, got, 0.0)
                    out[g, i * ROWS : (i + 1) * ROWS, j * ROWS : (j + 1) * ROWS] = got.T.astype(BF16)

    @pl.when(jnp.logical_not(low))
    def _():
        for g in range(GROUPS):
            for i in range(2):
                for j in range(3):
                    got = piece(jnp.minimum(p + i, 3), g, p - j)
                    if i == 0 and j == 0:
                        got = jnp.where(r >= c, got.astype(F32), 0.0).astype(BF16)
                    out[g, i * ROWS : (i + 1) * ROWS, j * ROWS : (j + 1) * ROWS] = got


def product_kernel(chunk, u, v, near, far, swap, weights, part, out_u, out_v):
    for g in range(GROUPS):
        i, lanes = lanes_of(g)
        if i != chunk:
            continue
        own, other = weights[g, :ROWS, :], weights[g, ROWS:, :]
        long_side = jnp.concatenate([u[:, lanes], swap[:, lanes], far[:, lanes]], axis=0)
        part[:, lanes] = nn(other, long_side).astype(BF16)
        out_u[:, lanes] = nn(own, long_side)
        short_side = jnp.concatenate([v[:, lanes], near[:, lanes]], axis=0)
        both = jnp.concatenate([own[:, :ROWS], other[:, :ROWS]], axis=0)
        out_v[:, lanes] = tn(both, short_side)


def mix_grad_kernel(n, place, u, v, near, far, swap, keep, send):
    p, core = place[0], place[2]
    first = core == 0
    r = lax.broadcasted_iota(jnp.int32, (ROWS, ROWS), 0) // SEG
    c = lax.broadcasted_iota(jnp.int32, (ROWS, ROWS), 1) // SEG
    keep[...] = jnp.zeros_like(keep)
    send[...] = jnp.zeros_like(send)

    def put(target, slot, k, got):
        lanes = slice((slot * n + k) * ROWS, (slot * n + k + 1) * ROWS)
        keep[target, :, lanes] = jnp.where(first, got[:SEG], got[SEG:])
        send[target, :, lanes] = jnp.where(first, got[SEG:], got[:SEG]).astype(BF16)

    for k in range(n):
        at = slice(k * WIDTH, (k + 1) * WIDTH)

        @pl.when(p == 0)
        def _():
            put(0, 0, k, jnp.where(r >= c, nt(u[:, at], v[:, at]), 0.0))

        @pl.when(p == 1)
        def _():
            put(1, 0, k, nt(u[:, at], near[:, at]))
            put(1, 1, k, jnp.where(r >= c, nt(u[:, at], v[:, at]), 0.0))
            put(2, 0, k, nt(swap[:, at], near[:, at]))
            put(3, 0, k, nt(far[:, at], near[:, at]))

        @pl.when(p == 2)
        def _():
            put(2, 0, k, jnp.where(r >= c, nt(v[:, at], u[:, at]), 0.0))
            put(2, 1, k, nt(v[:, at], swap[:, at]))
            put(3, 0, k, nt(near[:, at], u[:, at]))
            put(3, 1, k, nt(near[:, at], swap[:, at]))

        @pl.when(p == 3)
        def _():
            put(3, 0, k, jnp.where(r >= c, nt(v[:, at], u[:, at]), 0.0))


def split(x):
    high = x.astype(BF16)
    return high, (x - high.astype(F32)).astype(BF16)


def sums_kernel(chunk, place, values, stats, before, out_u, out_v, got, small):
    low = place[0] < 2
    small[...] = before[...]
    mean = stats[0, :, :1]
    inv = stats[1, :, :1]
    for g in range(GROUPS):
        i, lanes = lanes_of(g)
        if i != chunk:
            continue
        for k in range(WIDTH // 128):
            own = slice(lanes.start + k * 128, lanes.start + (k + 1) * 128)
            cols = slice(g * WIDTH + k * 128, g * WIDTH + (k + 1) * 128)
            back = jnp.where(low, out_u[:, own] + got[:, own].astype(F32), out_v[:, own])
            back = back.astype(BF16).astype(F32)
            unit = (values[0, :, cols].astype(F32) - mean) * inv
            row = 16 + g * 6 + k
            small[row : row + 1] = jnp.sum(back * unit, axis=0, keepdims=True)
            small[row + 24 : row + 25] = jnp.sum(back, axis=0, keepdims=True)


def last_sums_kernel(place, values, stats, before, out_u, out_v, got, last, small, send):
    sums_kernel(1, place, values, stats, before, out_u, out_v, got, small)
    send[:4] = last[...]
    high, low = split(small[...])
    send[4, :, :128] = high
    send[4, :, 128:] = low


def chip_kernel(place, keep, got, *outs):
    for k in range(4):
        b = (place[1] + k) % 4
        outs[k][...] = (keep[b] + got[b].astype(F32)).astype(BF16)


def last_chip_kernel(keep, small, got, out):
    extra = small[...] + (got[4, :, :128].astype(F32) + got[4, :, 128:].astype(F32))
    high, low = split(extra)
    for b in range(4):
        out[b, :, :256] = (keep[b] + got[b].astype(F32)).astype(BF16)
        out[b, :, 256:384] = high
        out[b, :, 384:512] = low


def deal_kernel(own, one, two, three, got1, out):
    got0 = (own, one, two, three)

    def total_of(parts, lanes):
        total = parts[0][:, lanes].astype(F32)
        for k in range(1, 4):
            total = total + parts[k][:, lanes].astype(F32)
        return total

    got1 = [got1.at[k] for k in range(4)]

    def put(lane, block):
        for z in range(8):
            out[z, :, lane : lane + block.shape[1]] = block[z * 8 : (z + 1) * 8]

    for slot in range(2):
        put(slot * 512, total_of(got0, slice(slot * 384, (slot + 1) * 384)).astype(BF16))
        put(slot * 512 + 384, total_of(got1, slice(slot * 128, (slot + 1) * 128)).astype(BF16))
    high, low = split(total_of(got1, slice(256, 384)) + total_of(got1, slice(384, 512)))
    put(1024, high)
    put(1152, low)


def add_kernel(got, out):
    total = got[0].astype(F32)
    for z in range(1, 8):
        total = total + got[z].astype(F32)
    high, low = split(total[:, 1024:1152] + total[:, 1152:1280])
    total = total[:, :1024].astype(BF16)
    for y in range(8):
        out[y, :, :1024] = total
        out[y, :, 1024:1152] = high
        out[y, :, 1152:1280] = low


def place_kernel(got, out):
    def at(place, slot):
        lanes = slice(slot * 512, (slot + 1) * 512)
        return got[place, :, lanes].astype(F32) + got[place + QUAD, :, lanes].astype(F32)

    columns = (at(0, 0) + at(1, 0), at(1, 1) + at(2, 1), at(2, 0), at(3, 0))
    columns = [c.astype(BF16) for c in columns]
    extra = jnp.zeros((8, 128), F32)
    for y in range(8):
        extra = extra + got[y, :, 1024:1152].astype(F32) + got[y, :, 1152:1280].astype(F32)
    high, low = split(extra)
    for z in range(8):
        for s in range(4):
            for g in range(GROUPS):
                out[z, :, g * 512 + s * ROWS : g * 512 + (s + 1) * ROWS] = columns[s][
                    :, g * ROWS : (g + 1) * ROWS
                ]
        out[z, :, 2048:2176] = high
        out[z, :, 2176:2304] = low


def final_kernel(got, grad_mix, grad_bias, grad_gain, grad_shift):
    for z in range(8):
        rows = slice(z * 8, (z + 1) * 8)
        for g in range(GROUPS):
            grad_mix[rows, g, :] = got[z, :, g * 512 : (g + 1) * 512].astype(F32)
        small = got[z, :, 2048:2176].astype(F32) + got[z, :, 2176:2304].astype(F32)
        if z < 2:
            for i in range(8):
                g, p = 2 * z + i // QUAD, i % QUAD
                grad_bias[g : g + 1, p * ROWS : (p + 1) * ROWS] = small[i : i + 1]
        elif z < 5:
            grad_gain[(z - 2) * 8 : (z - 1) * 8] = small
        else:
            grad_shift[(z - 5) * 8 : (z - 4) * 8] = small


def post_kernel(place, values, upstream, stats, gain, *refs):
    n = len(CHUNKS)
    outs_u, outs_v, got, grad_u, grad_v = refs[:n], refs[n : 2 * n], refs[2 * n : 3 * n], refs[3 * n], refs[3 * n + 1]
    low = place[0] < 2
    step = 16

    def block(i, carry):
        rows = pl.ds(pl.multiple_of(i * step, step), step)
        mean = stats[0, rows, :1]
        inv = stats[1, rows, :1]
        first = jnp.zeros((step, 1), F32)
        second = jnp.zeros((step, 1), F32)
        for g in range(GROUPS):
            cols = slice(g * WIDTH, (g + 1) * WIDTH)
            c, lanes = lanes_of(g)
            long_side = outs_u[c][rows, lanes] + got[c][rows, lanes].astype(F32)
            short_side = outs_v[c][rows, lanes]
            mixed = jnp.where(low, short_side, long_side) + stats[2, rows, g : g + 1]
            mixed = mixed.astype(BF16).astype(F32)
            grad_u[0, rows, cols] = (upstream[0, rows, cols].astype(F32) * mixed).astype(BF16)
            back = jnp.where(low, long_side, short_side).astype(BF16).astype(F32)
            scaled = back * gain[:, cols]
            unit = (values[0, rows, cols].astype(F32) - mean) * inv
            first = first + jnp.sum(scaled, axis=1, keepdims=True)
            second = second + jnp.sum(scaled * unit, axis=1, keepdims=True)
        first = first * (1.0 / HALF)
        second = second * (1.0 / HALF)
        for g in range(GROUPS):
            cols = slice(g * WIDTH, (g + 1) * WIDTH)
            c, lanes = lanes_of(g)
            long_side = outs_u[c][rows, lanes] + got[c][rows, lanes].astype(F32)
            back = jnp.where(low, long_side, outs_v[c][rows, lanes]).astype(BF16).astype(F32)
            scaled = back * gain[:, cols]
            unit = (values[0, rows, cols].astype(F32) - mean) * inv
            grad_v[0, rows, cols] = (inv * (scaled - first - unit * second)).astype(BF16)
        return carry

    lax.fori_loop(0, ROWS // step, block, 0)


def exchanged(x, axis):
    return lax.all_to_all(x, axis, split_axis=0, concat_axis=0, tiled=True)


def compute(gated, values_in, upstream, gain, shift, mix_w, mix_bias):
    spot = lax.axis_index(Y) % QUAD
    place = jnp.stack([spot, lax.axis_index(X), lax.axis_index(CORE)]).astype(jnp.int32)
    gain_row, shift_row = gain.reshape(1, HALF), shift.reshape(1, HALF)
    n = len(CHUNKS)
    halves = [shape((ROWS, k * WIDTH), BF16) for k in CHUNKS]
    fulls = [shape((ROWS, k * WIDTH), F32) for k in CHUNKS]

    pre = call(
        pre_kernel,
        halves * 2 + [shape((3, ROWS, 128), F32), shape((64, 128), F32)],
        (place, *map(far_memory, (values_in, gated, upstream, gain_row, shift_row, mix_bias))),
        scratch=[pltpu.VMEM((1, ROWS, HALF), BF16)] * 3
        + [pltpu.VMEM((1, HALF), F32)] * 2
        + [pltpu.VMEM((GROUPS, 512), F32), pltpu.SemaphoreType.DMA((3, 4)), pltpu.SemaphoreType.DMA((3,))],
        remote=range(1, 7),
    )
    us, vs, stats, bias_term = pre[:n], pre[n : 2 * n], pre[2 * n], pre[2 * n + 1]

    near, far, swap = [], [], []
    for i in range(n):
        near.append(lax.ppermute(vs[i], Y, NEAR))
        far.append(lax.ppermute(vs[i], Y, FAR))
        swap.append(lax.ppermute(vs[i], Y, SWAP))

    slab = call(slab_kernel, shape((GROUPS, SEG, 3 * ROWS), BF16), (place, mix_w))
    slabs = [slab] + [lax.ppermute(slab, X, CHIPS[k]) for k in range(1, 4)]
    mine = call(join_kernel, shape((4, GROUPS, SEG, 3 * ROWS), BF16), (place, *slabs))
    theirs = lax.ppermute(mine, CORE, PARTNER)
    weights = call(weight_kernel, shape((GROUPS, 2 * ROWS, 3 * ROWS), BF16), (place, mine, theirs))

    outs_u, outs_v, got, keeps, sends = [], [], [], [], []
    for i in range(n):
        operands = (us[i], vs[i], near[i], far[i], swap[i])
        part, out_u, out_v = call(
            functools.partial(product_kernel, i),
            [halves[i], fulls[i], fulls[i]],
            (*operands, weights),
            0,
        )
        got.append(lax.ppermute(part, Y, OUT))
        outs_u.append(out_u)
        outs_v.append(out_v)
        dims = (4, SEG, 2 * CHUNKS[i] * ROWS)
        keep, send = call(
            functools.partial(mix_grad_kernel, CHUNKS[i]),
            [shape(dims, F32), shape(dims, BF16)],
            (place, *operands),
        )
        keeps.append(keep)
        sends.append(send)

    folded = lax.ppermute(sends[0], CORE, PARTNER)
    chip = call(chip_kernel, [shape((SEG, 768), BF16)] * 4, (place, keeps[0], folded))
    chip = [chip[0]] + [lax.ppermute(chip[k], X, CHIPS[k]) for k in range(1, 4)]
    sums = call(
        functools.partial(sums_kernel, 0),
        shape((64, 128), F32),
        (place, values_in, stats, bias_term, outs_u[0], outs_v[0], got[0]),
    )
    small, last = call(
        last_sums_kernel,
        [shape((64, 128), F32), shape((5, SEG, 2 * ROWS), BF16)],
        (place, values_in, stats, sums, outs_u[1], outs_v[1], got[1], sends[1]),
    )
    last = call(
        last_chip_kernel,
        shape((4, SEG, 512), BF16),
        (keeps[1], small, lax.ppermute(last, CORE, PARTNER)),
        0,
    )
    dealt = call(deal_kernel, shape((8, 8, 1280), BF16), (*chip, exchanged(last, X)), 0)
    added = call(add_kernel, shape((8, 8, 1280), BF16), (exchanged(dealt, Z),), 0)
    placed = call(place_kernel, shape((8, 8, 2304), BF16), (exchanged(added, Y),), 0)
    grad_mix, grad_bias, grad_gain, grad_shift = call(
        final_kernel,
        [shape((SEG, GROUPS, 512), F32), shape((GROUPS, 512), F32)] + [shape((24, 128), F32)] * 2,
        (exchanged(placed, Z),),
        0,
    )

    grad_u, grad_v = call(
        post_kernel,
        [shape((1, ROWS, HALF), BF16)] * 2,
        (place, values_in, upstream, stats, gain_row, *outs_u, *outs_v, *got),
    )
    return (grad_u, grad_v, grad_mix, grad_bias, grad_gain.reshape(HALF), grad_shift.reshape(HALF))


def solution(mesh):
    torus = Mesh(mesh.devices.reshape(8, 8, 4, 2), ("sp_0", "sp_1", "dp_0", "dp_1"))
    return jax.shard_map(
        compute,
        mesh=torus,
        in_specs=(
            P(DP, SP, None),
            P(DP, SP, None),
            P(DP, SP, None),
            P(),
            P(),
            P(DP, None, None),
            P(),
        ),
        out_specs=(P(DP, SP, None), P(DP, SP, None), P(DP, None, None), P(), P(), P()),
        check_vma=False,
    )
```

```python
import functools

import jax
import jax.numpy as jnp
from jax import lax
from jax.experimental import pallas as pl
from jax.experimental.pallas import tpu as pltpu
from jax.sharding import Mesh
from jax.sharding import PartitionSpec as P


SEG = 64
ROWS = 128
GROUPS = 4
WIDTH = 768
HALF = GROUPS * WIDTH
QUAD = 4
DP = ("dp_0", "dp_1")
SP = ("sp_0", "sp_1")
Y = "sp_1"
Z = "sp_0"
X = "dp_0"
CORE = "dp_1"
EPS = 1e-05

NEAR = [(0, 1), (3, 2), (4, 5), (7, 6)]
FAR = [(0, 2), (3, 1), (4, 6), (7, 5)]
SWAP = [(1, 2), (2, 1), (5, 6), (6, 5)]
OUT = [(1, 0), (2, 3), (5, 4), (6, 7)]
PARTNER = [(0, 1), (1, 0)]
ACROSS = [(0, 3), (3, 0), (1, 2), (2, 1)]
WITHIN = [(0, 1), (1, 0), (2, 3), (3, 2)]

CHUNKS = (3, 1)
PLACES = [(i, k * WIDTH) for i, n in enumerate(CHUNKS) for k in range(n)]


VMEM = pl.BlockSpec(memory_space=pltpu.VMEM)
SMEM = pl.BlockSpec(memory_space=pltpu.SMEM)
HBM = pl.BlockSpec(memory_space=pltpu.HBM)
F32 = jnp.float32
BF16 = jnp.bfloat16


def far_memory(x):
    return pltpu.with_memory_space_constraint(x, pltpu.HBM)


def call(kernel, out_shape, inputs, scalars=1, scratch=(), vmem=16, remote=()):
    return pl.pallas_call(
        kernel,
        out_shape=out_shape,
        in_specs=[SMEM] * scalars + [HBM if i in remote else VMEM for i in range(scalars, len(inputs))],
        out_specs=jax.tree.map(lambda _: VMEM, out_shape),
        scratch_shapes=list(scratch),
        compiler_params=pltpu.CompilerParams(vmem_limit_bytes=vmem << 20),
    )(*inputs)


def shape(dims, dtype):
    return jax.ShapeDtypeStruct(dims, dtype)


def nt(a, b):
    return lax.dot_general(a, b, (((1,), (1,)), ((), ())), preferred_element_type=F32)


def tn(a, b):
    return lax.dot_general(a, b, (((0,), (0,)), ((), ())), preferred_element_type=F32)


def nn(a, b):
    return jnp.dot(a, b, preferred_element_type=F32)


def lanes_of(g, width=WIDTH):
    chunk, start = PLACES[g]
    start = start // WIDTH * width
    return chunk, slice(start, start + width)


def pre_kernel(place, values_in, gated_in, upstream_in, gain_in, shift_in, *outs):
    n = len(CHUNKS)
    us, vs, stats = outs[:n], outs[n : 2 * n], outs[2 * n]
    values, gated, upstream, gain, shift, sems, few = outs[2 * n + 1 :]
    low = place[0] < 2
    step = 16
    part = ROWS // 4
    pairs = ((values_in, values), (gated_in, gated), (upstream_in, upstream))

    def copy(k, i):
        rows = slice(i * part, (i + 1) * part)
        return pltpu.make_async_copy(pairs[k][0].at[0, rows], pairs[k][1].at[0, rows], sems.at[k, i])

    singles = [
        pltpu.make_async_copy(source, target, few.at[k])
        for k, (source, target) in enumerate(((gain_in, gain), (shift_in, shift)))
    ]
    copy(0, 0).start()
    for single in singles:
        single.start()
    copy(1, 0).start()
    copy(2, 0).start()
    for i in range(1, 4):
        for k in range(3):
            copy(k, i).start()
    for single in singles:
        single.wait()

    def block(i, carry):
        rows = pl.ds(pl.multiple_of(i * step, step), step)
        raw = values[0, rows, :].astype(F32)
        mean = jnp.sum(raw, axis=1, keepdims=True) * (1.0 / HALF)
        centred = raw - mean
        var = jnp.sum(centred * centred, axis=1, keepdims=True) * (1.0 / HALF)
        inv = lax.rsqrt(var + EPS)
        stats[0, rows, :] = jnp.broadcast_to(mean, (step, 128))
        stats[1, rows, :] = jnp.broadcast_to(inv, (step, 128))
        for g in range(GROUPS):
            cols = slice(g * WIDTH, (g + 1) * WIDTH)
            unit = (values[0, rows, cols].astype(F32) - mean) * inv
            normed = (unit * gain[:, cols] + shift[:, cols]).astype(BF16)
            grad = (upstream[0, rows, cols].astype(F32) * gated[0, rows, cols].astype(F32)).astype(BF16)
            i, lanes = lanes_of(g)
            us[i][rows, lanes] = jnp.where(low, grad, normed)
            vs[i][rows, lanes] = jnp.where(low, normed, grad)
        return carry

    for i in range(4):
        for k in range(3):
            copy(k, i).wait()
        lax.fori_loop(i * part // step, (i + 1) * part // step, block, 0, unroll=True)


def side_kernel(place, u, v, u1, v1, mix_bias, columns, bias):
    p = place[0]
    low = p < 2
    own_bias = mix_bias[:, pl.ds(pl.multiple_of(p * ROWS, ROWS), ROWS)]
    columns[...] = jnp.concatenate([own_bias, jnp.zeros((ROWS - GROUPS, ROWS), F32)], axis=0).T
    bias[...] = jnp.zeros_like(bias)
    ones = jnp.ones((8, WIDTH), BF16)
    us, vs = (u, u1), (v, v1)
    for g in range(GROUPS):
        i, lanes = lanes_of(g)
        grad = jnp.where(low, us[i][:, lanes], vs[i][:, lanes])
        bias[pl.ds(g * QUAD + p, 1), :] = nt(ones, grad)[:1]


def slab_kernel(place, rows, out):
    p = place[0]

    def fill(start):
        for g in range(GROUPS):
            got = rows[:, g, start : start + 3 * ROWS]
            for x in range(4):
                out[x, g] = got

    @pl.when(p < 3)
    def _():
        fill(0)

    @pl.when(p == 3)
    def _():
        fill(ROWS)


def weight_kernel(place, mine, theirs, out):
    p, core = place[0], place[2]
    low = p < 2
    first = core == 0
    start = jnp.where(p == 3, 1, 0)
    r = lax.broadcasted_iota(jnp.int32, (ROWS, ROWS), 0) // SEG
    c = lax.broadcasted_iota(jnp.int32, (ROWS, ROWS), 1) // SEG

    def piece(t, g, s):
        cols = pl.ds(pl.multiple_of((s - start) * ROWS, ROWS), ROWS)
        ours, others = mine[t, g, :, cols], theirs[t, g, :, cols]
        return jnp.concatenate([jnp.where(first, ours, others), jnp.where(first, others, ours)], axis=0)

    @pl.when(low)
    def _():
        for g in range(GROUPS):
            for i in range(2):
                for j in range(3):
                    got = piece(p + j, g, jnp.maximum(p - i, 0)).astype(F32)
                    if i == 0 and j == 0:
                        got = jnp.where(r >= c, got, 0.0)
                    out[g, i * ROWS : (i + 1) * ROWS, j * ROWS : (j + 1) * ROWS] = got.T.astype(BF16)

    @pl.when(jnp.logical_not(low))
    def _():
        for g in range(GROUPS):
            for i in range(2):
                for j in range(3):
                    got = piece(jnp.minimum(p + i, 3), g, p - j)
                    if i == 0 and j == 0:
                        got = jnp.where(r >= c, got.astype(F32), 0.0).astype(BF16)
                    out[g, i * ROWS : (i + 1) * ROWS, j * ROWS : (j + 1) * ROWS] = got


def product_kernel(chunk, u, v, near, far, swap, weights, part, out_u, out_v):
    for g in range(GROUPS):
        i, lanes = lanes_of(g)
        if i != chunk:
            continue
        own, other = weights[g, :ROWS, :], weights[g, ROWS:, :]
        long_side = jnp.concatenate([u[:, lanes], swap[:, lanes], far[:, lanes]], axis=0)
        part[:, lanes] = nn(other, long_side).astype(BF16)
        out_u[:, lanes] = nn(own, long_side)
        short_side = jnp.concatenate([v[:, lanes], near[:, lanes]], axis=0)
        both = jnp.concatenate([own[:, :ROWS], other[:, :ROWS]], axis=0)
        out_v[:, lanes] = tn(both, short_side)


def mix_grad_kernel(n, place, u, v, near, far, swap, keep, send):
    p, core = place[0], place[2]
    first = core == 0
    r = lax.broadcasted_iota(jnp.int32, (ROWS, ROWS), 0) // SEG
    c = lax.broadcasted_iota(jnp.int32, (ROWS, ROWS), 1) // SEG
    keep[...] = jnp.zeros_like(keep)
    send[...] = jnp.zeros_like(send)

    def put(target, slot, k, got):
        lanes = slice((slot * n + k) * ROWS, (slot * n + k + 1) * ROWS)
        keep[target, :, lanes] = jnp.where(first, got[:SEG], got[SEG:])
        send[target, :, lanes] = jnp.where(first, got[SEG:], got[:SEG]).astype(BF16)

    for k in range(n):
        at = slice(k * WIDTH, (k + 1) * WIDTH)

        @pl.when(p == 0)
        def _():
            put(0, 0, k, jnp.where(r >= c, nt(u[:, at], v[:, at]), 0.0))

        @pl.when(p == 1)
        def _():
            put(1, 0, k, nt(u[:, at], near[:, at]))
            put(1, 1, k, jnp.where(r >= c, nt(u[:, at], v[:, at]), 0.0))
            put(2, 0, k, nt(swap[:, at], near[:, at]))
            put(3, 0, k, nt(far[:, at], near[:, at]))

        @pl.when(p == 2)
        def _():
            put(2, 0, k, jnp.where(r >= c, nt(v[:, at], u[:, at]), 0.0))
            put(2, 1, k, nt(v[:, at], swap[:, at]))
            put(3, 0, k, nt(near[:, at], u[:, at]))
            put(3, 1, k, nt(near[:, at], swap[:, at]))

        @pl.when(p == 3)
        def _():
            put(3, 0, k, jnp.where(r >= c, nt(v[:, at], u[:, at]), 0.0))


def split(x):
    high = x.astype(BF16)
    return high, (x - high.astype(F32)).astype(BF16)


def sums_kernel(chunk, place, values, stats, before, out_u, out_v, got, small):
    low = place[0] < 2
    small[...] = before[...]
    mean = stats[0, :, :1]
    inv = stats[1, :, :1]
    for g in range(GROUPS):
        i, lanes = lanes_of(g)
        if i != chunk:
            continue
        for k in range(WIDTH // 128):
            own = slice(lanes.start + k * 128, lanes.start + (k + 1) * 128)
            cols = slice(g * WIDTH + k * 128, g * WIDTH + (k + 1) * 128)
            back = jnp.where(low, out_u[:, own] + got[:, own].astype(F32), out_v[:, own])
            back = back.astype(BF16).astype(F32)
            unit = (values[0, :, cols].astype(F32) - mean) * inv
            row = 16 + g * 6 + k
            small[row : row + 1] = jnp.sum(back * unit, axis=0, keepdims=True)
            small[row + 24 : row + 25] = jnp.sum(back, axis=0, keepdims=True)


def last_sums_kernel(place, values, stats, before, out_u, out_v, got, last, small, send):
    sums_kernel(1, place, values, stats, before, out_u, out_v, got, small)
    send[:4] = last[...]
    high, low = split(small[...])
    send[4, :, :128] = high
    send[4, :, 128:] = low


def chip_kernel(place, keep, got, own, send):
    near = place[1] // 2 * 2
    for k in range(2):
        own[k] = keep[near + k] + got[near + k].astype(F32)
        other = 2 - near + k
        send[k] = (keep[other] + got[other].astype(F32)).astype(BF16)


def chip_pair_kernel(place, keep, got, own, send):
    b = place[1] % 2
    own[...] = keep[b] + got[b].astype(F32)
    send[...] = (keep[1 - b] + got[1 - b].astype(F32)).astype(BF16)


def last_chip_kernel(keep, small, got, out):
    extra = small[...] + (got[4, :, :128].astype(F32) + got[4, :, 128:].astype(F32))
    high, low = split(extra)
    for b in range(4):
        out[b, :, :256] = (keep[b] + got[b].astype(F32)).astype(BF16)
        out[b, :, 256:384] = high
        out[b, :, 384:512] = low


def deal_kernel(own, other, got1, out):
    def total_of(parts, lanes):
        total = parts[0][:, lanes].astype(F32)
        for part in parts[1:]:
            total = total + part[:, lanes].astype(F32)
        return total

    got0 = (own, other)
    got1 = [got1.at[k] for k in range(4)]

    def put(lane, block):
        for z in range(8):
            out[z, :, lane : lane + block.shape[1]] = block[z * 8 : (z + 1) * 8]

    for slot in range(2):
        put(slot * 512, total_of(got0, slice(slot * 384, (slot + 1) * 384)).astype(BF16))
        put(slot * 512 + 384, total_of(got1, slice(slot * 128, (slot + 1) * 128)).astype(BF16))
    high, low = split(total_of(got1, slice(256, 384)) + total_of(got1, slice(384, 512)))
    put(1024, high)
    put(1152, low)


def add_kernel(got, out):
    total = got[0].astype(F32)
    for z in range(1, 8):
        total = total + got[z].astype(F32)
    high, low = split(total[:, 1024:1152] + total[:, 1152:1280])
    total = total[:, :1024].astype(BF16)
    for y in range(8):
        out[y, :, :1024] = total
        out[y, :, 1024:1152] = high
        out[y, :, 1152:1280] = low


def place_kernel(got, out):
    def at(place, slot):
        lanes = slice(slot * 512, (slot + 1) * 512)
        return got[place, :, lanes].astype(F32) + got[place + QUAD, :, lanes].astype(F32)

    columns = (at(0, 0) + at(1, 0), at(1, 1) + at(2, 1), at(2, 0), at(3, 0))
    columns = [c.astype(BF16) for c in columns]
    extra = jnp.zeros((8, 128), F32)
    for y in range(8):
        extra = extra + got[y, :, 1024:1152].astype(F32) + got[y, :, 1152:1280].astype(F32)
    high, low = split(extra)
    for z in range(8):
        for s in range(4):
            for g in range(GROUPS):
                out[z, :, g * 512 + s * ROWS : g * 512 + (s + 1) * ROWS] = columns[s][
                    :, g * ROWS : (g + 1) * ROWS
                ]
        out[z, :, 2048:2176] = high
        out[z, :, 2176:2304] = low


def final_kernel(got, grad_mix, grad_bias, grad_gain, grad_shift):
    for z in range(8):
        rows = slice(z * 8, (z + 1) * 8)
        for g in range(GROUPS):
            grad_mix[rows, g, :] = got[z, :, g * 512 : (g + 1) * 512].astype(F32)
        small = got[z, :, 2048:2176].astype(F32) + got[z, :, 2176:2304].astype(F32)
        if z < 2:
            for i in range(8):
                g, p = 2 * z + i // QUAD, i % QUAD
                grad_bias[g : g + 1, p * ROWS : (p + 1) * ROWS] = small[i : i + 1]
        elif z < 5:
            grad_gain[(z - 2) * 8 : (z - 1) * 8] = small
        else:
            grad_shift[(z - 5) * 8 : (z - 4) * 8] = small


def post_kernel(place, values, upstream, stats, columns, gain, *refs):
    n = len(CHUNKS)
    outs_u, outs_v, got, grad_u, grad_v = refs[:n], refs[n : 2 * n], refs[2 * n : 3 * n], refs[3 * n], refs[3 * n + 1]
    low = place[0] < 2
    step = 16

    def block(i, carry):
        rows = pl.ds(pl.multiple_of(i * step, step), step)
        mean = stats[0, rows, :1]
        inv = stats[1, rows, :1]
        first = jnp.zeros((step, 1), F32)
        second = jnp.zeros((step, 1), F32)
        for g in range(GROUPS):
            cols = slice(g * WIDTH, (g + 1) * WIDTH)
            c, lanes = lanes_of(g)
            long_side = outs_u[c][rows, lanes] + got[c][rows, lanes].astype(F32)
            short_side = outs_v[c][rows, lanes]
            mixed = jnp.where(low, short_side, long_side) + columns[rows, g : g + 1]
            mixed = mixed.astype(BF16).astype(F32)
            grad_u[0, rows, cols] = (upstream[0, rows, cols].astype(F32) * mixed).astype(BF16)
            back = jnp.where(low, long_side, short_side).astype(BF16).astype(F32)
            scaled = back * gain[:, cols]
            unit = (values[0, rows, cols].astype(F32) - mean) * inv
            first = first + jnp.sum(scaled, axis=1, keepdims=True)
            second = second + jnp.sum(scaled * unit, axis=1, keepdims=True)
        first = first * (1.0 / HALF)
        second = second * (1.0 / HALF)
        for g in range(GROUPS):
            cols = slice(g * WIDTH, (g + 1) * WIDTH)
            c, lanes = lanes_of(g)
            long_side = outs_u[c][rows, lanes] + got[c][rows, lanes].astype(F32)
            back = jnp.where(low, long_side, outs_v[c][rows, lanes]).astype(BF16).astype(F32)
            scaled = back * gain[:, cols]
            unit = (values[0, rows, cols].astype(F32) - mean) * inv
            grad_v[0, rows, cols] = (inv * (scaled - first - unit * second)).astype(BF16)
        return carry

    lax.fori_loop(0, ROWS // step, block, 0, unroll=2)


def exchanged(x, axis):
    return lax.all_to_all(x, axis, split_axis=0, concat_axis=0, tiled=True)


def compute(gated, values_in, upstream, gain, shift, mix_w, mix_bias):
    spot = lax.axis_index(Y) % QUAD
    place = jnp.stack([spot, lax.axis_index(X), lax.axis_index(CORE)]).astype(jnp.int32)
    gain_row, shift_row = gain.reshape(1, HALF), shift.reshape(1, HALF)
    n = len(CHUNKS)
    halves = [shape((ROWS, k * WIDTH), BF16) for k in CHUNKS]
    fulls = [shape((ROWS, k * WIDTH), F32) for k in CHUNKS]

    pre = call(
        pre_kernel,
        halves * 2 + [shape((2, ROWS, 128), F32)],
        (place, *map(far_memory, (values_in, gated, upstream, gain_row, shift_row))),
        scratch=[pltpu.VMEM((1, ROWS, HALF), BF16)] * 3
        + [pltpu.VMEM((1, HALF), F32)] * 2
        + [pltpu.SemaphoreType.DMA((3, 4)), pltpu.SemaphoreType.DMA((2,))],
        remote=range(1, 6),
    )
    us, vs, stats = pre[:n], pre[n : 2 * n], pre[2 * n]

    near, far, swap = [], [], []
    for i in range(n):
        near.append(lax.ppermute(vs[i], Y, NEAR))
        far.append(lax.ppermute(vs[i], Y, FAR))
        swap.append(lax.ppermute(vs[i], Y, SWAP))

    slab = call(slab_kernel, shape((4, GROUPS, SEG, 3 * ROWS), BF16), (place, mix_w))
    mine = exchanged(slab, X)
    theirs = lax.ppermute(mine, CORE, PARTNER)
    columns, bias_term = call(
        side_kernel,
        [shape((ROWS, ROWS), F32), shape((64, 128), F32)],
        (place, us[0], vs[0], us[1], vs[1], mix_bias),
    )
    weights = call(weight_kernel, shape((GROUPS, 2 * ROWS, 3 * ROWS), BF16), (place, mine, theirs))

    outs_u, outs_v, got, keeps, sends = [], [], [], [], []
    for i in range(n):
        operands = (us[i], vs[i], near[i], far[i], swap[i])
        part, out_u, out_v = call(
            functools.partial(product_kernel, i),
            [halves[i], fulls[i], fulls[i]],
            (*operands, weights),
            0,
        )
        got.append(lax.ppermute(part, Y, OUT))
        outs_u.append(out_u)
        outs_v.append(out_v)
        dims = (4, SEG, 2 * CHUNKS[i] * ROWS)
        keep, send = call(
            functools.partial(mix_grad_kernel, CHUNKS[i]),
            [shape(dims, F32), shape(dims, BF16)],
            (place, *operands),
        )
        keeps.append(keep)
        sends.append(send)

    folded = lax.ppermute(sends[0], CORE, PARTNER)
    keep, send = call(
        chip_kernel,
        [shape((2, SEG, 768), F32), shape((2, SEG, 768), BF16)],
        (place, keeps[0], folded),
    )
    own, send = call(
        chip_pair_kernel,
        [shape((SEG, 768), F32), shape((SEG, 768), BF16)],
        (place, keep, lax.ppermute(send, X, ACROSS)),
    )
    chip = (own, lax.ppermute(send, X, WITHIN))
    sums = call(
        functools.partial(sums_kernel, 0),
        shape((64, 128), F32),
        (place, values_in, stats, bias_term, outs_u[0], outs_v[0], got[0]),
    )
    small, last = call(
        last_sums_kernel,
        [shape((64, 128), F32), shape((5, SEG, 2 * ROWS), BF16)],
        (place, values_in, stats, sums, outs_u[1], outs_v[1], got[1], sends[1]),
    )
    last = call(
        last_chip_kernel,
        shape((4, SEG, 512), BF16),
        (keeps[1], small, lax.ppermute(last, CORE, PARTNER)),
        0,
    )
    dealt = call(deal_kernel, shape((8, 8, 1280), BF16), (*chip, exchanged(last, X)), 0)
    added = call(add_kernel, shape((8, 8, 1280), BF16), (exchanged(dealt, Z),), 0)
    placed = call(place_kernel, shape((8, 8, 2304), BF16), (exchanged(added, Y),), 0)
    grad_mix, grad_bias, grad_gain, grad_shift = call(
        final_kernel,
        [shape((SEG, GROUPS, 512), F32), shape((GROUPS, 512), F32)] + [shape((24, 128), F32)] * 2,
        (exchanged(placed, Z),),
        0,
    )

    grad_u, grad_v = call(
        post_kernel,
        [shape((1, ROWS, HALF), BF16)] * 2,
        (place, values_in, upstream, stats, columns, gain_row, *outs_u, *outs_v, *got),
    )
    return (grad_u, grad_v, grad_mix, grad_bias, grad_gain.reshape(HALF), grad_shift.reshape(HALF))


def solution(mesh):
    torus = Mesh(mesh.devices.reshape(8, 8, 4, 2), ("sp_0", "sp_1", "dp_0", "dp_1"))
    return jax.shard_map(
        compute,
        mesh=torus,
        in_specs=(
            P(DP, SP, None),
            P(DP, SP, None),
            P(DP, SP, None),
            P(),
            P(),
            P(DP, None, None),
            P(),
        ),
        out_specs=(P(DP, SP, None), P(DP, SP, None), P(DP, None, None), P(), P(), P()),
        check_vma=False,
    )
```

```python
import functools

import jax
import jax.numpy as jnp
from jax import lax
from jax.experimental import pallas as pl
from jax.experimental.pallas import tpu as pltpu
from jax.sharding import Mesh
from jax.sharding import PartitionSpec as P


SEG = 64
ROWS = 128
GROUPS = 4
WIDTH = 768
HALF = GROUPS * WIDTH
QUAD = 4
DP = ("dp_0", "dp_1")
SP = ("sp_0", "sp_1")
Y = "sp_1"
Z = "sp_0"
X = "dp_0"
CORE = "dp_1"
EPS = 1e-05

NEAR = [(0, 1), (3, 2), (4, 5), (7, 6)]
FAR = [(0, 2), (3, 1), (4, 6), (7, 5)]
SWAP = [(1, 2), (2, 1), (5, 6), (6, 5)]
OUT = [(1, 0), (2, 3), (5, 4), (6, 7)]
PARTNER = [(0, 1), (1, 0)]
CHIPS = [[(i, (i + k) % 4) for i in range(4)] for k in range(4)]
ACROSS = [(0, 3), (3, 0), (1, 2), (2, 1)]
WITHIN = [(0, 1), (1, 0), (2, 3), (3, 2)]

CHUNKS = (3, 1)
PLACES = [(i, k * WIDTH) for i, n in enumerate(CHUNKS) for k in range(n)]


VMEM = pl.BlockSpec(memory_space=pltpu.VMEM)
SMEM = pl.BlockSpec(memory_space=pltpu.SMEM)
HBM = pl.BlockSpec(memory_space=pltpu.HBM)
F32 = jnp.float32
BF16 = jnp.bfloat16


def far_memory(x):
    return pltpu.with_memory_space_constraint(x, pltpu.HBM)


def call(kernel, out_shape, inputs, scalars=1, scratch=(), vmem=16, remote=()):
    return pl.pallas_call(
        kernel,
        out_shape=out_shape,
        in_specs=[SMEM] * scalars + [HBM if i in remote else VMEM for i in range(scalars, len(inputs))],
        out_specs=jax.tree.map(lambda _: VMEM, out_shape),
        scratch_shapes=list(scratch),
        compiler_params=pltpu.CompilerParams(vmem_limit_bytes=vmem << 20),
    )(*inputs)


def shape(dims, dtype):
    return jax.ShapeDtypeStruct(dims, dtype)


def nt(a, b):
    return lax.dot_general(a, b, (((1,), (1,)), ((), ())), preferred_element_type=F32)


def tn(a, b):
    return lax.dot_general(a, b, (((0,), (0,)), ((), ())), preferred_element_type=F32)


def nn(a, b):
    return jnp.dot(a, b, preferred_element_type=F32)


def lanes_of(g, width=WIDTH):
    chunk, start = PLACES[g]
    start = start // WIDTH * width
    return chunk, slice(start, start + width)


def pre_kernel(place, values_in, gated_in, upstream_in, gain_in, shift_in, *outs):
    n = len(CHUNKS)
    us, vs, stats = outs[:n], outs[n : 2 * n], outs[2 * n]
    values, gated, upstream, gain, shift, sems, few = outs[2 * n + 1 :]
    low = place[0] < 2
    step = 16
    part = ROWS // 4
    pairs = ((values_in, values), (gated_in, gated), (upstream_in, upstream))

    def copy(k, i):
        rows = slice(i * part, (i + 1) * part)
        return pltpu.make_async_copy(pairs[k][0].at[0, rows], pairs[k][1].at[0, rows], sems.at[k, i])

    singles = [
        pltpu.make_async_copy(source, target, few.at[k])
        for k, (source, target) in enumerate(((gain_in, gain), (shift_in, shift)))
    ]
    copy(0, 0).start()
    for single in singles:
        single.start()
    copy(1, 0).start()
    copy(2, 0).start()
    for i in range(1, 4):
        for k in range(3):
            copy(k, i).start()
    for single in singles:
        single.wait()

    def block(i, carry):
        rows = pl.ds(pl.multiple_of(i * step, step), step)
        raw = values[0, rows, :].astype(F32)
        mean = jnp.sum(raw, axis=1, keepdims=True) * (1.0 / HALF)
        centred = raw - mean
        var = jnp.sum(centred * centred, axis=1, keepdims=True) * (1.0 / HALF)
        inv = lax.rsqrt(var + EPS)
        stats[0, rows, :] = jnp.broadcast_to(mean, (step, 128))
        stats[1, rows, :] = jnp.broadcast_to(inv, (step, 128))
        for g in range(GROUPS):
            cols = slice(g * WIDTH, (g + 1) * WIDTH)
            unit = (values[0, rows, cols].astype(F32) - mean) * inv
            normed = (unit * gain[:, cols] + shift[:, cols]).astype(BF16)
            sent = unit.astype(BF16)
            grad = (upstream[0, rows, cols].astype(F32) * gated[0, rows, cols].astype(F32)).astype(BF16)
            i, lanes = lanes_of(g)
            us[i][rows, lanes] = jnp.where(low, grad, normed)
            vs[i][rows, lanes] = jnp.where(low, sent, grad)
        return carry

    for i in range(4):
        for k in range(3):
            copy(k, i).wait()
        lax.fori_loop(i * part // step, (i + 1) * part // step, block, 0, unroll=True)


def side_kernel(place, u, v, u1, v1, mix_bias, columns, bias):
    p = place[0]
    low = p < 2
    own_bias = mix_bias[:, pl.ds(pl.multiple_of(p * ROWS, ROWS), ROWS)]
    columns[...] = jnp.concatenate([own_bias, jnp.zeros((ROWS - GROUPS, ROWS), F32)], axis=0).T
    bias[...] = jnp.zeros_like(bias)
    ones = jnp.ones((8, WIDTH), BF16)
    us, vs = (u, u1), (v, v1)
    for g in range(GROUPS):
        i, lanes = lanes_of(g)
        grad = jnp.where(low, us[i][:, lanes], vs[i][:, lanes])
        bias[pl.ds(g * QUAD + p, 1), :] = nt(ones, grad)[:1]


def slab_kernel(place, rows, out):
    p = place[0]

    @pl.when(p < 3)
    def _():
        for g in range(GROUPS):
            out[g] = rows[:, g, : 3 * ROWS]

    @pl.when(p == 3)
    def _():
        for g in range(GROUPS):
            out[g] = rows[:, g, ROWS:]


def join_kernel(place, *refs):
    for k in range(4):
        refs[4][(place[1] + 4 - k) % 4] = refs[k][...]


def weight_kernel(place, mine, theirs, out):
    p, core = place[0], place[2]
    low = p < 2
    first = core == 0
    start = jnp.where(p == 3, 1, 0)
    r = lax.broadcasted_iota(jnp.int32, (ROWS, ROWS), 0) // SEG
    c = lax.broadcasted_iota(jnp.int32, (ROWS, ROWS), 1) // SEG

    def piece(t, g, s):
        cols = pl.ds(pl.multiple_of((s - start) * ROWS, ROWS), ROWS)
        ours, others = mine[t, g, :, cols], theirs[t, g, :, cols]
        return jnp.concatenate([jnp.where(first, ours, others), jnp.where(first, others, ours)], axis=0)

    @pl.when(low)
    def _():
        for g in range(GROUPS):
            for i in range(2):
                for j in range(3):
                    got = piece(p + j, g, jnp.maximum(p - i, 0)).astype(F32)
                    if i == 0 and j == 0:
                        got = jnp.where(r >= c, got, 0.0)
                    out[g, i * ROWS : (i + 1) * ROWS, j * ROWS : (j + 1) * ROWS] = got.T.astype(BF16)

    @pl.when(jnp.logical_not(low))
    def _():
        for g in range(GROUPS):
            for i in range(2):
                for j in range(3):
                    got = piece(jnp.minimum(p + i, 3), g, p - j)
                    if i == 0 and j == 0:
                        got = jnp.where(r >= c, got.astype(F32), 0.0).astype(BF16)
                    out[g, i * ROWS : (i + 1) * ROWS, j * ROWS : (j + 1) * ROWS] = got


def product_kernel(chunk, place, u, v, near, far, swap, weights, gain, shift, part, out_u, out_v, *normed):
    p = place[0]
    for g in range(GROUPS):
        i, lanes = lanes_of(g)
        if i != chunk:
            continue
        cols = slice(g * WIDTH, (g + 1) * WIDTH)
        own, other = weights[g, :ROWS, :], weights[g, ROWS:, :]
        both = jnp.concatenate([own[:, :ROWS], other[:, :ROWS]], axis=0)

        def put(slot, ref, here):
            got = ref[:, lanes].astype(F32) * gain[:, cols] + shift[:, cols]
            if here is not None:
                got = jnp.where(here, got, 0.0)
            normed[slot][:, lanes] = got.astype(BF16)

        def products(long_side, short_side):
            long_side = jnp.concatenate([ref[:, lanes] for ref in long_side], axis=0)
            short_side = jnp.concatenate([ref[:, lanes] for ref in short_side], axis=0)
            part[:, lanes] = nn(other, long_side).astype(BF16)
            out_u[:, lanes] = nn(own, long_side)
            out_v[:, lanes] = tn(both, short_side)

        @pl.when(p < 2)
        def _():
            put(0, v, None)
            put(1, near, p == 1)
            products((u, swap, far), normed)

        @pl.when(p >= 2)
        def _():
            put(0, swap, p == 2)
            put(1, far, p == 2)
            products((u, *normed), (v, near))


def mix_grad_kernel(n, place, u, v, near, far, swap, one, two, keep, send):
    p, core = place[0], place[2]
    first = core == 0
    r = lax.broadcasted_iota(jnp.int32, (ROWS, ROWS), 0) // SEG
    c = lax.broadcasted_iota(jnp.int32, (ROWS, ROWS), 1) // SEG
    keep[...] = jnp.zeros_like(keep)
    send[...] = jnp.zeros_like(send)

    def put(target, slot, k, got):
        lanes = slice((slot * n + k) * ROWS, (slot * n + k + 1) * ROWS)
        keep[target, :, lanes] = jnp.where(first, got[:SEG], got[SEG:])
        send[target, :, lanes] = jnp.where(first, got[SEG:], got[:SEG]).astype(BF16)

    for k in range(n):
        at = slice(k * WIDTH, (k + 1) * WIDTH)

        @pl.when(p == 0)
        def _():
            put(0, 0, k, jnp.where(r >= c, nt(u[:, at], one[:, at]), 0.0))

        @pl.when(p == 1)
        def _():
            put(1, 0, k, nt(u[:, at], two[:, at]))
            put(1, 1, k, jnp.where(r >= c, nt(u[:, at], one[:, at]), 0.0))
            put(2, 0, k, nt(swap[:, at], two[:, at]))
            put(3, 0, k, nt(far[:, at], two[:, at]))

        @pl.when(p == 2)
        def _():
            put(2, 0, k, jnp.where(r >= c, nt(v[:, at], u[:, at]), 0.0))
            put(2, 1, k, nt(v[:, at], one[:, at]))
            put(3, 0, k, nt(near[:, at], u[:, at]))
            put(3, 1, k, nt(near[:, at], one[:, at]))

        @pl.when(p == 3)
        def _():
            put(3, 0, k, jnp.where(r >= c, nt(v[:, at], u[:, at]), 0.0))


def split(x):
    high = x.astype(BF16)
    return high, (x - high.astype(F32)).astype(BF16)


def sums_kernel(chunk, place, values, stats, before, out_u, out_v, part, near, small):
    p = place[0]
    small[...] = before[...]
    mean = stats[0, :, :1]
    inv = stats[1, :, :1]
    for g in range(GROUPS):
        i, lanes = lanes_of(g)
        if i != chunk:
            continue
        for k in range(WIDTH // 128):
            own = slice(lanes.start + k * 128, lanes.start + (k + 1) * 128)
            cols = slice(g * WIDTH + k * 128, g * WIDTH + (k + 1) * 128)
            back = jnp.where(p < 2, out_u[:, own], out_v[:, own])
            unit = (values[0, :, cols].astype(F32) - mean) * inv
            sent = jnp.where(p == 1, part[:, own].astype(F32), 0.0)
            row = 16 + g * 6 + k
            gain_rows = back * unit + sent * near[:, own].astype(F32)
            small[row : row + 1] = jnp.sum(gain_rows, axis=0, keepdims=True)
            small[row + 24 : row + 25] = jnp.sum(back + sent, axis=0, keepdims=True)


def last_sums_kernel(place, values, stats, before, out_u, out_v, part, near, last, small, send):
    sums_kernel(1, place, values, stats, before, out_u, out_v, part, near, small)
    send[:4] = last[...]
    high, low = split(small[...])
    send[4, :, :128] = high
    send[4, :, 128:] = low


def chip_kernel(place, keep, got, own, send):
    near = place[1] // 2 * 2
    for k in range(2):
        own[k] = keep[near + k] + got[near + k].astype(F32)
        other = 2 - near + k
        send[k] = (keep[other] + got[other].astype(F32)).astype(BF16)


def chip_pair_kernel(place, keep, got, own, send):
    b = place[1] % 2
    own[...] = keep[b] + got[b].astype(F32)
    send[...] = (keep[1 - b] + got[1 - b].astype(F32)).astype(BF16)


def last_chip_kernel(keep, small, got, out):
    extra = small[...] + (got[4, :, :128].astype(F32) + got[4, :, 128:].astype(F32))
    high, low = split(extra)
    for b in range(4):
        out[b, :, :256] = (keep[b] + got[b].astype(F32)).astype(BF16)
        out[b, :, 256:384] = high
        out[b, :, 384:512] = low


def deal_kernel(own, other, got1, out):
    def total_of(parts, lanes):
        total = parts[0][:, lanes].astype(F32)
        for part in parts[1:]:
            total = total + part[:, lanes].astype(F32)
        return total

    got0 = (own, other)
    got1 = [got1.at[k] for k in range(4)]

    def put(lane, block):
        for z in range(8):
            out[z, :, lane : lane + block.shape[1]] = block[z * 8 : (z + 1) * 8]

    for slot in range(2):
        put(slot * 512, total_of(got0, slice(slot * 384, (slot + 1) * 384)).astype(BF16))
        put(slot * 512 + 384, total_of(got1, slice(slot * 128, (slot + 1) * 128)).astype(BF16))
    high, low = split(total_of(got1, slice(256, 384)) + total_of(got1, slice(384, 512)))
    put(1024, high)
    put(1152, low)


def add_kernel(got, out):
    total = got[0].astype(F32)
    for z in range(1, 8):
        total = total + got[z].astype(F32)
    high, low = split(total[:, 1024:1152] + total[:, 1152:1280])
    total = total[:, :1024].astype(BF16)
    for y in range(8):
        out[y, :, :1024] = total
        out[y, :, 1024:1152] = high
        out[y, :, 1152:1280] = low


def place_kernel(got, out):
    def at(place, slot):
        lanes = slice(slot * 512, (slot + 1) * 512)
        return got[place, :, lanes].astype(F32) + got[place + QUAD, :, lanes].astype(F32)

    columns = (at(0, 0) + at(1, 0), at(1, 1) + at(2, 1), at(2, 0), at(3, 0))
    columns = [c.astype(BF16) for c in columns]
    extra = jnp.zeros((8, 128), F32)
    for y in range(8):
        extra = extra + got[y, :, 1024:1152].astype(F32) + got[y, :, 1152:1280].astype(F32)
    high, low = split(extra)
    for z in range(8):
        for s in range(4):
            for g in range(GROUPS):
                out[z, :, g * 512 + s * ROWS : g * 512 + (s + 1) * ROWS] = columns[s][
                    :, g * ROWS : (g + 1) * ROWS
                ]
        out[z, :, 2048:2176] = high
        out[z, :, 2176:2304] = low


def final_kernel(got, grad_mix, grad_bias, grad_gain, grad_shift):
    for z in range(8):
        rows = slice(z * 8, (z + 1) * 8)
        for g in range(GROUPS):
            grad_mix[rows, g, :] = got[z, :, g * 512 : (g + 1) * 512].astype(F32)
        small = got[z, :, 2048:2176].astype(F32) + got[z, :, 2176:2304].astype(F32)
        if z < 2:
            for i in range(8):
                g, p = 2 * z + i // QUAD, i % QUAD
                grad_bias[g : g + 1, p * ROWS : (p + 1) * ROWS] = small[i : i + 1]
        elif z < 5:
            grad_gain[(z - 2) * 8 : (z - 1) * 8] = small
        else:
            grad_shift[(z - 5) * 8 : (z - 4) * 8] = small


def post_kernel(place, values, upstream, stats, columns, gain, *refs):
    n = len(CHUNKS)
    outs_u, outs_v, got, grad_u, grad_v = refs[:n], refs[n : 2 * n], refs[2 * n : 3 * n], refs[3 * n], refs[3 * n + 1]
    low = place[0] < 2
    step = 16

    def block(i, carry):
        rows = pl.ds(pl.multiple_of(i * step, step), step)
        mean = stats[0, rows, :1]
        inv = stats[1, rows, :1]
        first = jnp.zeros((step, 1), F32)
        second = jnp.zeros((step, 1), F32)
        for g in range(GROUPS):
            cols = slice(g * WIDTH, (g + 1) * WIDTH)
            c, lanes = lanes_of(g)
            long_side = outs_u[c][rows, lanes] + got[c][rows, lanes].astype(F32)
            short_side = outs_v[c][rows, lanes]
            mixed = jnp.where(low, short_side, long_side) + columns[rows, g : g + 1]
            mixed = mixed.astype(BF16).astype(F32)
            grad_u[0, rows, cols] = (upstream[0, rows, cols].astype(F32) * mixed).astype(BF16)
            back = jnp.where(low, long_side, short_side).astype(BF16).astype(F32)
            scaled = back * gain[:, cols]
            unit = (values[0, rows, cols].astype(F32) - mean) * inv
            first = first + jnp.sum(scaled, axis=1, keepdims=True)
            second = second + jnp.sum(scaled * unit, axis=1, keepdims=True)
        first = first * (1.0 / HALF)
        second = second * (1.0 / HALF)
        for g in range(GROUPS):
            cols = slice(g * WIDTH, (g + 1) * WIDTH)
            c, lanes = lanes_of(g)
            long_side = outs_u[c][rows, lanes] + got[c][rows, lanes].astype(F32)
            back = jnp.where(low, long_side, outs_v[c][rows, lanes]).astype(BF16).astype(F32)
            scaled = back * gain[:, cols]
            unit = (values[0, rows, cols].astype(F32) - mean) * inv
            grad_v[0, rows, cols] = (inv * (scaled - first - unit * second)).astype(BF16)
        return carry

    lax.fori_loop(0, ROWS // step, block, 0, unroll=2)


def exchanged(x, axis):
    return lax.all_to_all(x, axis, split_axis=0, concat_axis=0, tiled=True)


def compute(gated, values_in, upstream, gain, shift, mix_w, mix_bias):
    spot = lax.axis_index(Y) % QUAD
    place = jnp.stack([spot, lax.axis_index(X), lax.axis_index(CORE)]).astype(jnp.int32)
    gain_row, shift_row = gain.reshape(1, HALF), shift.reshape(1, HALF)
    n = len(CHUNKS)
    halves = [shape((ROWS, k * WIDTH), BF16) for k in CHUNKS]
    fulls = [shape((ROWS, k * WIDTH), F32) for k in CHUNKS]

    pre = call(
        pre_kernel,
        halves * 2 + [shape((2, ROWS, 128), F32)],
        (place, *map(far_memory, (values_in, gated, upstream, gain_row, shift_row))),
        scratch=[pltpu.VMEM((1, ROWS, HALF), BF16)] * 3
        + [pltpu.VMEM((1, HALF), F32)] * 2
        + [pltpu.SemaphoreType.DMA((3, 4)), pltpu.SemaphoreType.DMA((2,))],
        remote=range(1, 6),
    )
    us, vs, stats = pre[:n], pre[n : 2 * n], pre[2 * n]

    near, far, swap = [], [], []
    for i in range(n):
        near.append(lax.ppermute(vs[i], Y, NEAR))
        far.append(lax.ppermute(vs[i], Y, FAR))
        swap.append(lax.ppermute(vs[i], Y, SWAP))

    slab = call(slab_kernel, shape((GROUPS, SEG, 3 * ROWS), BF16), (place, mix_w))
    slabs = [slab] + [lax.ppermute(slab, X, CHIPS[k]) for k in range(1, 4)]
    mine = call(join_kernel, shape((4, GROUPS, SEG, 3 * ROWS), BF16), (place, *slabs))
    theirs = lax.ppermute(mine, CORE, PARTNER)
    columns, bias_term = call(
        side_kernel,
        [shape((ROWS, ROWS), F32), shape((64, 128), F32)],
        (place, us[0], vs[0], us[1], vs[1], mix_bias),
    )
    weights = call(weight_kernel, shape((GROUPS, 2 * ROWS, 3 * ROWS), BF16), (place, mine, theirs))

    outs_u, outs_v, got, keeps, sends, parts = [], [], [], [], [], []
    for i in range(n):
        operands = (us[i], vs[i], near[i], far[i], swap[i])
        part, out_u, out_v, one, two = call(
            functools.partial(product_kernel, i),
            [halves[i], fulls[i], fulls[i], halves[i], halves[i]],
            (place, *operands, weights, gain_row, shift_row),
        )
        parts.append(part)
        got.append(lax.ppermute(part, Y, OUT))
        outs_u.append(out_u)
        outs_v.append(out_v)
        dims = (4, SEG, 2 * CHUNKS[i] * ROWS)
        keep, send = call(
            functools.partial(mix_grad_kernel, CHUNKS[i]),
            [shape(dims, F32), shape(dims, BF16)],
            (place, *operands, one, two),
        )
        keeps.append(keep)
        sends.append(send)

    folded = lax.ppermute(sends[0], CORE, PARTNER)
    keep, send = call(
        chip_kernel,
        [shape((2, SEG, 768), F32), shape((2, SEG, 768), BF16)],
        (place, keeps[0], folded),
    )
    own, send = call(
        chip_pair_kernel,
        [shape((SEG, 768), F32), shape((SEG, 768), BF16)],
        (place, keep, lax.ppermute(send, X, ACROSS)),
    )
    chip = (own, lax.ppermute(send, X, WITHIN))
    sums = call(
        functools.partial(sums_kernel, 0),
        shape((64, 128), F32),
        (place, values_in, stats, bias_term, outs_u[0], outs_v[0], parts[0], near[0]),
    )
    small, last = call(
        last_sums_kernel,
        [shape((64, 128), F32), shape((5, SEG, 2 * ROWS), BF16)],
        (place, values_in, stats, sums, outs_u[1], outs_v[1], parts[1], near[1], sends[1]),
    )
    last = call(
        last_chip_kernel,
        shape((4, SEG, 512), BF16),
        (keeps[1], small, lax.ppermute(last, CORE, PARTNER)),
        0,
    )
    dealt = call(deal_kernel, shape((8, 8, 1280), BF16), (*chip, exchanged(last, X)), 0)
    added = call(add_kernel, shape((8, 8, 1280), BF16), (exchanged(dealt, Z),), 0)
    placed = call(place_kernel, shape((8, 8, 2304), BF16), (exchanged(added, Y),), 0)
    grad_mix, grad_bias, grad_gain, grad_shift = call(
        final_kernel,
        [shape((SEG, GROUPS, 512), F32), shape((GROUPS, 512), F32)] + [shape((24, 128), F32)] * 2,
        (exchanged(placed, Z),),
        0,
    )

    grad_u, grad_v = call(
        post_kernel,
        [shape((1, ROWS, HALF), BF16)] * 2,
        (place, values_in, upstream, stats, columns, gain_row, *outs_u, *outs_v, *got),
    )
    return (grad_u, grad_v, grad_mix, grad_bias, grad_gain.reshape(HALF), grad_shift.reshape(HALF))


def solution(mesh):
    torus = Mesh(mesh.devices.reshape(8, 8, 4, 2), ("sp_0", "sp_1", "dp_0", "dp_1"))
    return jax.shard_map(
        compute,
        mesh=torus,
        in_specs=(
            P(DP, SP, None),
            P(DP, SP, None),
            P(DP, SP, None),
            P(),
            P(),
            P(DP, None, None),
            P(),
        ),
        out_specs=(P(DP, SP, None), P(DP, SP, None), P(DP, None, None), P(), P(), P()),
        check_vma=False,
    )
```

```python
import functools

import jax
import jax.numpy as jnp
from jax import lax
from jax.experimental import pallas as pl
from jax.experimental.pallas import tpu as pltpu
from jax.sharding import Mesh
from jax.sharding import PartitionSpec as P


SEG = 64
ROWS = 128
GROUPS = 4
WIDTH = 768
HALF = GROUPS * WIDTH
QUAD = 4
DP = ("dp_0", "dp_1")
SP = ("sp_0", "sp_1")
Y = "sp_1"
Z = "sp_0"
X = "dp_0"
CORE = "dp_1"
EPS = 1e-05

NEAR = [(0, 1), (3, 2), (4, 5), (7, 6)]
FAR = [(0, 2), (3, 1), (4, 6), (7, 5)]
SWAP = [(1, 2), (2, 1), (5, 6), (6, 5)]
OUT = [(1, 0), (2, 3), (5, 4), (6, 7)]
PARTNER = [(0, 1), (1, 0)]
CHIPS = [[(i, (i + k) % 4) for i in range(4)] for k in range(4)]
ACROSS = [(0, 3), (3, 0), (1, 2), (2, 1)]
WITHIN = [(0, 1), (1, 0), (2, 3), (3, 2)]

CHUNKS = (3, 1)
PLACES = [(i, k * WIDTH) for i, n in enumerate(CHUNKS) for k in range(n)]


VMEM = pl.BlockSpec(memory_space=pltpu.VMEM)
SMEM = pl.BlockSpec(memory_space=pltpu.SMEM)
HBM = pl.BlockSpec(memory_space=pltpu.HBM)
F32 = jnp.float32
BF16 = jnp.bfloat16


def far_memory(x):
    return pltpu.with_memory_space_constraint(x, pltpu.HBM)


def call(kernel, out_shape, inputs, scalars=1, scratch=(), vmem=16, remote=()):
    return pl.pallas_call(
        kernel,
        out_shape=out_shape,
        in_specs=[SMEM] * scalars + [HBM if i in remote else VMEM for i in range(scalars, len(inputs))],
        out_specs=jax.tree.map(lambda _: VMEM, out_shape),
        scratch_shapes=list(scratch),
        compiler_params=pltpu.CompilerParams(vmem_limit_bytes=vmem << 20),
    )(*inputs)


def shape(dims, dtype):
    return jax.ShapeDtypeStruct(dims, dtype)


def nt(a, b):
    return lax.dot_general(a, b, (((1,), (1,)), ((), ())), preferred_element_type=F32)


def tn(a, b):
    return lax.dot_general(a, b, (((0,), (0,)), ((), ())), preferred_element_type=F32)


def nn(a, b):
    return jnp.dot(a, b, preferred_element_type=F32)


def lanes_of(g, width=WIDTH):
    chunk, start = PLACES[g]
    start = start // WIDTH * width
    return chunk, slice(start, start + width)


def pre_kernel(place, values_in, gated_in, upstream_in, gain_in, shift_in, *outs):
    n = len(CHUNKS)
    us, vs, stats = outs[:n], outs[n : 2 * n], outs[2 * n]
    values, gated, upstream, gain, shift, sems, few = outs[2 * n + 1 :]
    low = place[0] < 2
    step = 16
    part = ROWS // 4
    pairs = ((values_in, values), (gated_in, gated), (upstream_in, upstream))

    def copy(k, i):
        rows = slice(i * part, (i + 1) * part)
        return pltpu.make_async_copy(pairs[k][0].at[0, rows], pairs[k][1].at[0, rows], sems.at[k, i])

    singles = [
        pltpu.make_async_copy(source, target, few.at[k])
        for k, (source, target) in enumerate(((gain_in, gain), (shift_in, shift)))
    ]
    copy(0, 0).start()
    for single in singles:
        single.start()
    copy(1, 0).start()
    copy(2, 0).start()
    for i in range(1, 4):
        for k in range(3):
            copy(k, i).start()
    for single in singles:
        single.wait()

    def block(i, carry):
        rows = pl.ds(pl.multiple_of(i * step, step), step)
        raw = values[0, rows, :].astype(F32)
        mean = jnp.sum(raw, axis=1, keepdims=True) * (1.0 / HALF)
        centred = raw - mean
        var = jnp.sum(centred * centred, axis=1, keepdims=True) * (1.0 / HALF)
        inv = lax.rsqrt(var + EPS)
        stats[0, rows, :] = jnp.broadcast_to(mean, (step, 128))
        stats[1, rows, :] = jnp.broadcast_to(inv, (step, 128))
        for g in range(GROUPS):
            cols = slice(g * WIDTH, (g + 1) * WIDTH)
            unit = (values[0, rows, cols].astype(F32) - mean) * inv
            normed = (unit * gain[:, cols] + shift[:, cols]).astype(BF16)
            sent = unit.astype(BF16)
            grad = (upstream[0, rows, cols].astype(F32) * gated[0, rows, cols].astype(F32)).astype(BF16)
            i, lanes = lanes_of(g)
            us[i][rows, lanes] = jnp.where(low, grad, normed)
            vs[i][rows, lanes] = jnp.where(low, sent, grad)
        return carry

    for i in range(4):
        for k in range(3):
            copy(k, i).wait()
        lax.fori_loop(i * part // step, (i + 1) * part // step, block, 0, unroll=True)


def side_kernel(place, u, v, u1, v1, mix_bias, columns, bias):
    p = place[0]
    low = p < 2
    own_bias = mix_bias[:, pl.ds(pl.multiple_of(p * ROWS, ROWS), ROWS)]
    columns[...] = jnp.concatenate([own_bias, jnp.zeros((ROWS - GROUPS, ROWS), F32)], axis=0).T
    bias[...] = jnp.zeros_like(bias)
    ones = jnp.ones((8, WIDTH), BF16)
    us, vs = (u, u1), (v, v1)
    for g in range(GROUPS):
        i, lanes = lanes_of(g)
        grad = jnp.where(low, us[i][:, lanes], vs[i][:, lanes])
        bias[pl.ds(g * QUAD + p, 1), :] = nt(ones, grad)[:1]


def slab_kernel(place, rows, out):
    p = place[0]

    @pl.when(p < 3)
    def _():
        for g in range(GROUPS):
            out[g] = rows[:, g, : 3 * ROWS]

    @pl.when(p == 3)
    def _():
        for g in range(GROUPS):
            out[g] = rows[:, g, ROWS:]


def join_kernel(place, *refs):
    for k in range(4):
        refs[4][(place[1] + 4 - k) % 4] = refs[k][...]


def weight_kernel(place, mine, theirs, out):
    p, core = place[0], place[2]
    low = p < 2
    first = core == 0
    start = jnp.where(p == 3, 1, 0)
    r = lax.broadcasted_iota(jnp.int32, (ROWS, ROWS), 0) // SEG
    c = lax.broadcasted_iota(jnp.int32, (ROWS, ROWS), 1) // SEG

    def piece(t, g, s):
        cols = pl.ds(pl.multiple_of((s - start) * ROWS, ROWS), ROWS)
        ours, others = mine[t, g, :, cols], theirs[t, g, :, cols]
        return jnp.concatenate([jnp.where(first, ours, others), jnp.where(first, others, ours)], axis=0)

    @pl.when(low)
    def _():
        for g in range(GROUPS):
            for i in range(2):
                for j in range(3):
                    got = piece(p + j, g, jnp.maximum(p - i, 0)).astype(F32)
                    if i == 0 and j == 0:
                        got = jnp.where(r >= c, got, 0.0)
                    out[g, i * ROWS : (i + 1) * ROWS, j * ROWS : (j + 1) * ROWS] = got.T.astype(BF16)

    @pl.when(jnp.logical_not(low))
    def _():
        for g in range(GROUPS):
            for i in range(2):
                for j in range(3):
                    got = piece(jnp.minimum(p + i, 3), g, p - j)
                    if i == 0 and j == 0:
                        got = jnp.where(r >= c, got.astype(F32), 0.0).astype(BF16)
                    out[g, i * ROWS : (i + 1) * ROWS, j * ROWS : (j + 1) * ROWS] = got


def product_kernel(chunk, place, u, v, near, far, swap, weights, gain, shift, part, out_u, out_v, *normed):
    p = place[0]
    for g in range(GROUPS):
        i, lanes = lanes_of(g)
        if i != chunk:
            continue
        cols = slice(g * WIDTH, (g + 1) * WIDTH)
        own, other = weights[g, :ROWS, :], weights[g, ROWS:, :]
        both = jnp.concatenate([own[:, :ROWS], other[:, :ROWS]], axis=0)

        def put(slot, ref, here):
            got = ref[:, lanes].astype(F32) * gain[:, cols] + shift[:, cols]
            if here is not None:
                got = jnp.where(here, got, 0.0)
            normed[slot][:, lanes] = got.astype(BF16)

        def products(long_side, short_side):
            long_side = jnp.concatenate([ref[:, lanes] for ref in long_side], axis=0)
            short_side = jnp.concatenate([ref[:, lanes] for ref in short_side], axis=0)
            part[:, lanes] = nn(other, long_side).astype(BF16)
            out_u[:, lanes] = nn(own, long_side)
            out_v[:, lanes] = tn(both, short_side)

        @pl.when(p < 2)
        def _():
            put(0, v, None)
            put(1, near, p == 1)
            products((u, swap, far), normed)

        @pl.when(p >= 2)
        def _():
            put(0, swap, p == 2)
            put(1, far, p == 2)
            products((u, *normed), (v, near))


def mix_grad_kernel(n, place, u, v, near, far, swap, one, two, keep, send):
    p, core = place[0], place[2]
    first = core == 0
    r = lax.broadcasted_iota(jnp.int32, (ROWS, ROWS), 0) // SEG
    c = lax.broadcasted_iota(jnp.int32, (ROWS, ROWS), 1) // SEG
    keep[...] = jnp.zeros_like(keep)
    send[...] = jnp.zeros_like(send)

    def put(target, slot, k, got):
        lanes = slice((slot * n + k) * ROWS, (slot * n + k + 1) * ROWS)
        keep[target, :, lanes] = jnp.where(first, got[:SEG], got[SEG:])
        send[target, :, lanes] = jnp.where(first, got[SEG:], got[:SEG]).astype(BF16)

    for k in range(n):
        at = slice(k * WIDTH, (k + 1) * WIDTH)

        @pl.when(p == 0)
        def _():
            put(0, 0, k, jnp.where(r >= c, nt(u[:, at], one[:, at]), 0.0))

        @pl.when(p == 1)
        def _():
            put(1, 0, k, nt(u[:, at], two[:, at]))
            put(1, 1, k, jnp.where(r >= c, nt(u[:, at], one[:, at]), 0.0))
            put(2, 0, k, nt(swap[:, at], two[:, at]))
            put(3, 0, k, nt(far[:, at], two[:, at]))

        @pl.when(p == 2)
        def _():
            put(2, 0, k, jnp.where(r >= c, nt(v[:, at], u[:, at]), 0.0))
            put(2, 1, k, nt(v[:, at], one[:, at]))
            put(3, 0, k, nt(near[:, at], u[:, at]))
            put(3, 1, k, nt(near[:, at], one[:, at]))

        @pl.when(p == 3)
        def _():
            put(3, 0, k, jnp.where(r >= c, nt(v[:, at], u[:, at]), 0.0))


def split(x):
    high = x.astype(BF16)
    return high, (x - high.astype(F32)).astype(BF16)


def sums_kernel(chunk, place, values, stats, before, out_u, out_v, part, near, small):
    p = place[0]
    small[...] = before[...]
    mean = stats[0, :, :1]
    inv = stats[1, :, :1]
    for g in range(GROUPS):
        i, lanes = lanes_of(g)
        if i != chunk:
            continue
        for k in range(WIDTH // 128):
            own = slice(lanes.start + k * 128, lanes.start + (k + 1) * 128)
            cols = slice(g * WIDTH + k * 128, g * WIDTH + (k + 1) * 128)
            back = jnp.where(p < 2, out_u[:, own], out_v[:, own])
            unit = (values[0, :, cols].astype(F32) - mean) * inv
            sent = jnp.where(p == 1, part[:, own].astype(F32), 0.0)
            row = 16 + g * 6 + k
            gain_rows = back * unit + sent * near[:, own].astype(F32)
            small[row : row + 1] = jnp.sum(gain_rows, axis=0, keepdims=True)
            small[row + 24 : row + 25] = jnp.sum(back + sent, axis=0, keepdims=True)


def last_sums_kernel(place, values, stats, before, out_u, out_v, part, near, last, small, send):
    sums_kernel(1, place, values, stats, before, out_u, out_v, part, near, small)
    send[:4] = last[...]
    high, low = split(small[...])
    send[4, :, :128] = high
    send[4, :, 128:] = low


def chip_kernel(place, keep, got, own, send):
    near = place[1] // 2 * 2
    for k in range(2):
        own[k] = keep[near + k] + got[near + k].astype(F32)
        other = 2 - near + k
        send[k] = (keep[other] + got[other].astype(F32)).astype(BF16)


def chip_pair_kernel(place, keep, got, own, send):
    b = place[1] % 2
    own[...] = keep[b] + got[b].astype(F32)
    send[...] = (keep[1 - b] + got[1 - b].astype(F32)).astype(BF16)


def last_chip_kernel(place, keep, small, got, own, total, send):
    extra = small[...] + (got[4, :, :128].astype(F32) + got[4, :, 128:].astype(F32))
    high, low = split(extra)
    total[...] = extra
    send[2, :, :128] = high
    send[2, :, 128:] = low
    near = place[1] // 2 * 2
    for k in range(2):
        own[k] = keep[near + k] + got[near + k].astype(F32)
        other = 2 - near + k
        send[k] = (keep[other] + got[other].astype(F32)).astype(BF16)


def last_pair_kernel(place, keep, small, got, own, total, send):
    extra = small[...] + (got[2, :, :128].astype(F32) + got[2, :, 128:].astype(F32))
    high, low = split(extra)
    total[...] = extra
    send[1, :, :128] = high
    send[1, :, 128:] = low
    b = place[1] % 2
    own[...] = keep[b] + got[b].astype(F32)
    send[0] = (keep[1 - b] + got[1 - b].astype(F32)).astype(BF16)


def deal_kernel(own0, got0, own1, small, got1, out):
    def put(lane, block):
        for z in range(8):
            out[z, :, lane : lane + block.shape[1]] = block[z * 8 : (z + 1) * 8]

    first = (own0[...] + got0[...].astype(F32)).astype(BF16)
    last = (own1[...] + got1[0].astype(F32)).astype(BF16)
    for slot in range(2):
        put(slot * 512, first[:, slot * 384 : (slot + 1) * 384])
        put(slot * 512 + 384, last[:, slot * 128 : (slot + 1) * 128])
    high, low = split(small[...] + (got1[1, :, :128].astype(F32) + got1[1, :, 128:].astype(F32)))
    put(1024, high)
    put(1152, low)


def add_kernel(got, out):
    total = got[0].astype(F32)
    for z in range(1, 8):
        total = total + got[z].astype(F32)
    high, low = split(total[:, 1024:1152] + total[:, 1152:1280])
    total = total[:, :1024].astype(BF16)
    for y in range(8):
        out[y, :, :1024] = total
        out[y, :, 1024:1152] = high
        out[y, :, 1152:1280] = low


def place_kernel(got, out):
    def at(place, slot):
        lanes = slice(slot * 512, (slot + 1) * 512)
        return got[place, :, lanes].astype(F32) + got[place + QUAD, :, lanes].astype(F32)

    columns = (at(0, 0) + at(1, 0), at(1, 1) + at(2, 1), at(2, 0), at(3, 0))
    columns = [c.astype(BF16) for c in columns]
    extra = jnp.zeros((8, 128), F32)
    for y in range(8):
        extra = extra + got[y, :, 1024:1152].astype(F32) + got[y, :, 1152:1280].astype(F32)
    high, low = split(extra)
    for z in range(8):
        for s in range(4):
            for g in range(GROUPS):
                out[z, :, g * 512 + s * ROWS : g * 512 + (s + 1) * ROWS] = columns[s][
                    :, g * ROWS : (g + 1) * ROWS
                ]
        out[z, :, 2048:2176] = high
        out[z, :, 2176:2304] = low


def final_kernel(got, grad_mix, grad_bias, grad_gain, grad_shift):
    for z in range(8):
        rows = slice(z * 8, (z + 1) * 8)
        for g in range(GROUPS):
            grad_mix[rows, g, :] = got[z, :, g * 512 : (g + 1) * 512].astype(F32)
        small = got[z, :, 2048:2176].astype(F32) + got[z, :, 2176:2304].astype(F32)
        if z < 2:
            for i in range(8):
                g, p = 2 * z + i // QUAD, i % QUAD
                grad_bias[g : g + 1, p * ROWS : (p + 1) * ROWS] = small[i : i + 1]
        elif z < 5:
            grad_gain[(z - 2) * 8 : (z - 1) * 8] = small
        else:
            grad_shift[(z - 5) * 8 : (z - 4) * 8] = small


def post_kernel(place, values, upstream, stats, columns, gain, *refs):
    n = len(CHUNKS)
    outs_u, outs_v, got, grad_u, grad_v = refs[:n], refs[n : 2 * n], refs[2 * n : 3 * n], refs[3 * n], refs[3 * n + 1]
    low = place[0] < 2
    step = 16

    def block(i, carry):
        rows = pl.ds(pl.multiple_of(i * step, step), step)
        mean = stats[0, rows, :1]
        inv = stats[1, rows, :1]
        first = jnp.zeros((step, 1), F32)
        second = jnp.zeros((step, 1), F32)
        for g in range(GROUPS):
            cols = slice(g * WIDTH, (g + 1) * WIDTH)
            c, lanes = lanes_of(g)
            long_side = outs_u[c][rows, lanes] + got[c][rows, lanes].astype(F32)
            short_side = outs_v[c][rows, lanes]
            mixed = jnp.where(low, short_side, long_side) + columns[rows, g : g + 1]
            mixed = mixed.astype(BF16).astype(F32)
            grad_u[0, rows, cols] = (upstream[0, rows, cols].astype(F32) * mixed).astype(BF16)
            back = jnp.where(low, long_side, short_side).astype(BF16).astype(F32)
            scaled = back * gain[:, cols]
            unit = (values[0, rows, cols].astype(F32) - mean) * inv
            first = first + jnp.sum(scaled, axis=1, keepdims=True)
            second = second + jnp.sum(scaled * unit, axis=1, keepdims=True)
        first = first * (1.0 / HALF)
        second = second * (1.0 / HALF)
        for g in range(GROUPS):
            cols = slice(g * WIDTH, (g + 1) * WIDTH)
            c, lanes = lanes_of(g)
            long_side = outs_u[c][rows, lanes] + got[c][rows, lanes].astype(F32)
            back = jnp.where(low, long_side, outs_v[c][rows, lanes]).astype(BF16).astype(F32)
            scaled = back * gain[:, cols]
            unit = (values[0, rows, cols].astype(F32) - mean) * inv
            grad_v[0, rows, cols] = (inv * (scaled - first - unit * second)).astype(BF16)
        return carry

    lax.fori_loop(0, ROWS // step, block, 0, unroll=2)


def exchanged(x, axis):
    return lax.all_to_all(x, axis, split_axis=0, concat_axis=0, tiled=True)


def compute(gated, values_in, upstream, gain, shift, mix_w, mix_bias):
    spot = lax.axis_index(Y) % QUAD
    place = jnp.stack([spot, lax.axis_index(X), lax.axis_index(CORE)]).astype(jnp.int32)
    gain_row, shift_row = gain.reshape(1, HALF), shift.reshape(1, HALF)
    n = len(CHUNKS)
    halves = [shape((ROWS, k * WIDTH), BF16) for k in CHUNKS]
    fulls = [shape((ROWS, k * WIDTH), F32) for k in CHUNKS]

    pre = call(
        pre_kernel,
        halves * 2 + [shape((2, ROWS, 128), F32)],
        (place, *map(far_memory, (values_in, gated, upstream, gain_row, shift_row))),
        scratch=[pltpu.VMEM((1, ROWS, HALF), BF16)] * 3
        + [pltpu.VMEM((1, HALF), F32)] * 2
        + [pltpu.SemaphoreType.DMA((3, 4)), pltpu.SemaphoreType.DMA((2,))],
        remote=range(1, 6),
    )
    us, vs, stats = pre[:n], pre[n : 2 * n], pre[2 * n]

    near, far, swap = [], [], []
    for i in range(n):
        near.append(lax.ppermute(vs[i], Y, NEAR))
        far.append(lax.ppermute(vs[i], Y, FAR))
        swap.append(lax.ppermute(vs[i], Y, SWAP))

    slab = call(slab_kernel, shape((GROUPS, SEG, 3 * ROWS), BF16), (place, mix_w))
    slabs = [slab] + [lax.ppermute(slab, X, CHIPS[k]) for k in range(1, 4)]
    mine = call(join_kernel, shape((4, GROUPS, SEG, 3 * ROWS), BF16), (place, *slabs))
    theirs = lax.ppermute(mine, CORE, PARTNER)
    columns, bias_term = call(
        side_kernel, [shape((ROWS, ROWS), F32), shape((64, 128), F32)], (place, us[0], vs[0], us[1], vs[1], mix_bias)
    )
    weights = call(weight_kernel, shape((GROUPS, 2 * ROWS, 3 * ROWS), BF16), (place, mine, theirs))

    outs_u, outs_v, got, keeps, sends, parts = [], [], [], [], [], []
    for i in range(n):
        operands = (us[i], vs[i], near[i], far[i], swap[i])
        part, out_u, out_v, one, two = call(
            functools.partial(product_kernel, i),
            [halves[i], fulls[i], fulls[i], halves[i], halves[i]],
            (place, *operands, weights, gain_row, shift_row),
        )
        parts.append(part)
        got.append(lax.ppermute(part, Y, OUT))
        outs_u.append(out_u)
        outs_v.append(out_v)
        dims = (4, SEG, 2 * CHUNKS[i] * ROWS)
        keep, send = call(
            functools.partial(mix_grad_kernel, CHUNKS[i]),
            [shape(dims, F32), shape(dims, BF16)],
            (place, *operands, one, two),
        )
        keeps.append(keep)
        sends.append(send)

    folded = lax.ppermute(sends[0], CORE, PARTNER)
    keep, send = call(chip_kernel, [shape((2, SEG, 768), F32), shape((2, SEG, 768), BF16)], (place, keeps[0], folded))
    own, send = call(
        chip_pair_kernel,
        [shape((SEG, 768), F32), shape((SEG, 768), BF16)],
        (place, keep, lax.ppermute(send, X, ACROSS)),
    )
    chip = (own, lax.ppermute(send, X, WITHIN))
    sums = call(
        functools.partial(sums_kernel, 0),
        shape((64, 128), F32),
        (place, values_in, stats, bias_term, outs_u[0], outs_v[0], parts[0], near[0]),
    )
    small, last = call(
        last_sums_kernel,
        [shape((64, 128), F32), shape((5, SEG, 2 * ROWS), BF16)],
        (place, values_in, stats, sums, outs_u[1], outs_v[1], parts[1], near[1], sends[1]),
    )
    half_terms = [shape((2, SEG, 256), F32), shape((64, 128), F32), shape((3, SEG, 256), BF16)]
    own, small, send = call(last_chip_kernel, half_terms, (place, keeps[1], small, lax.ppermute(last, CORE, PARTNER)))
    own, small, send = call(
        last_pair_kernel,
        [shape((SEG, 256), F32), shape((64, 128), F32), shape((2, SEG, 256), BF16)],
        (place, own, small, lax.ppermute(send, X, ACROSS)),
    )
    dealt = call(deal_kernel, shape((8, 8, 1280), BF16), (*chip, own, small, lax.ppermute(send, X, WITHIN)), 0)
    added = call(add_kernel, shape((8, 8, 1280), BF16), (exchanged(dealt, Z),), 0)
    placed = call(place_kernel, shape((8, 8, 2304), BF16), (exchanged(added, Y),), 0)
    grad_mix, grad_bias, grad_gain, grad_shift = call(
        final_kernel,
        [shape((SEG, GROUPS, 512), F32), shape((GROUPS, 512), F32)] + [shape((24, 128), F32)] * 2,
        (exchanged(placed, Z),),
        0,
    )

    grad_u, grad_v = call(
        post_kernel,
        [shape((1, ROWS, HALF), BF16)] * 2,
        (place, values_in, upstream, stats, columns, gain_row, *outs_u, *outs_v, *got),
    )
    return (grad_u, grad_v, grad_mix, grad_bias, grad_gain.reshape(HALF), grad_shift.reshape(HALF))


def solution(mesh):
    torus = Mesh(mesh.devices.reshape(8, 8, 4, 2), ("sp_0", "sp_1", "dp_0", "dp_1"))
    return jax.shard_map(
        compute,
        mesh=torus,
        in_specs=(
            P(DP, SP, None),
            P(DP, SP, None),
            P(DP, SP, None),
            P(),
            P(),
            P(DP, None, None),
            P(),
        ),
        out_specs=(P(DP, SP, None), P(DP, SP, None), P(DP, None, None), P(), P(), P()),
        check_vma=False,
    )
```

```python
import functools

import jax
import jax.numpy as jnp
from jax import lax
from jax.experimental import pallas as pl
from jax.experimental.pallas import tpu as pltpu
from jax.sharding import Mesh
from jax.sharding import PartitionSpec as P


SEG = 64
ROWS = 128
GROUPS = 4
WIDTH = 768
HALF = GROUPS * WIDTH
QUAD = 4
DP = ("dp_0", "dp_1")
SP = ("sp_0", "sp_1")
Y = "sp_1"
Z = "sp_0"
X = "dp_0"
CORE = "dp_1"
EPS = 1e-05

NEAR = [(0, 1), (3, 2), (4, 5), (7, 6)]
FAR = [(0, 2), (3, 1), (4, 6), (7, 5)]
SWAP = [(1, 2), (2, 1), (5, 6), (6, 5)]
OUT = [(1, 0), (2, 3), (5, 4), (6, 7)]
PARTNER = [(0, 1), (1, 0)]
CHIPS = [[(i, (i + k) % 4) for i in range(4)] for k in range(4)]
ACROSS = [(0, 3), (3, 0), (1, 2), (2, 1)]
WITHIN = [(0, 1), (1, 0), (2, 3), (3, 2)]

CHUNKS = (3, 1)
PLACES = [(i, k * WIDTH) for i, n in enumerate(CHUNKS) for k in range(n)]


VMEM = pl.BlockSpec(memory_space=pltpu.VMEM)
SMEM = pl.BlockSpec(memory_space=pltpu.SMEM)
HBM = pl.BlockSpec(memory_space=pltpu.HBM)
F32 = jnp.float32
BF16 = jnp.bfloat16


def far_memory(x):
    return pltpu.with_memory_space_constraint(x, pltpu.HBM)


def call(kernel, out_shape, inputs, scalars=1, scratch=(), vmem=16, remote=(), out=VMEM):
    return pl.pallas_call(
        kernel,
        out_shape=out_shape,
        in_specs=[SMEM] * scalars + [HBM if i in remote else VMEM for i in range(scalars, len(inputs))],
        out_specs=jax.tree.map(lambda _: out, out_shape),
        scratch_shapes=list(scratch),
        compiler_params=pltpu.CompilerParams(vmem_limit_bytes=vmem << 20),
    )(*inputs)


def shape(dims, dtype):
    return jax.ShapeDtypeStruct(dims, dtype)


def nt(a, b):
    return lax.dot_general(a, b, (((1,), (1,)), ((), ())), preferred_element_type=F32)


def tn(a, b):
    return lax.dot_general(a, b, (((0,), (0,)), ((), ())), preferred_element_type=F32)


def nn(a, b):
    return jnp.dot(a, b, preferred_element_type=F32)


def lanes_of(g, width=WIDTH):
    chunk, start = PLACES[g]
    start = start // WIDTH * width
    return chunk, slice(start, start + width)


def pre_kernel(place, values_in, gated_in, upstream_in, gain_in, shift_in, *outs):
    n = len(CHUNKS)
    us, vs, stats = outs[:n], outs[n : 2 * n], outs[2 * n]
    values, gated, upstream, gain, shift, sems, few = outs[2 * n + 1 :]
    low = place[0] < 2
    step = 16
    part = ROWS // 4
    pairs = ((values_in, values), (gated_in, gated), (upstream_in, upstream))

    def copy(k, i):
        rows = slice(i * part, (i + 1) * part)
        return pltpu.make_async_copy(pairs[k][0].at[0, rows], pairs[k][1].at[0, rows], sems.at[k, i])

    singles = [
        pltpu.make_async_copy(source, target, few.at[k])
        for k, (source, target) in enumerate(((gain_in, gain), (shift_in, shift)))
    ]
    copy(0, 0).start()
    for single in singles:
        single.start()
    copy(1, 0).start()
    copy(2, 0).start()
    for i in range(1, 4):
        for k in range(3):
            copy(k, i).start()
    for single in singles:
        single.wait()

    def block(i, carry):
        rows = pl.ds(pl.multiple_of(i * step, step), step)
        raw = values[0, rows, :].astype(F32)
        mean = jnp.sum(raw, axis=1, keepdims=True) * (1.0 / HALF)
        centred = raw - mean
        var = jnp.sum(centred * centred, axis=1, keepdims=True) * (1.0 / HALF)
        inv = lax.rsqrt(var + EPS)
        stats[0, rows, :] = jnp.broadcast_to(mean, (step, 128))
        stats[1, rows, :] = jnp.broadcast_to(inv, (step, 128))
        for g in range(GROUPS):
            cols = slice(g * WIDTH, (g + 1) * WIDTH)
            unit = (values[0, rows, cols].astype(F32) - mean) * inv
            normed = (unit * gain[:, cols] + shift[:, cols]).astype(BF16)
            sent = unit.astype(BF16)
            grad = (upstream[0, rows, cols].astype(F32) * gated[0, rows, cols].astype(F32)).astype(BF16)
            i, lanes = lanes_of(g)
            us[i][rows, lanes] = jnp.where(low, grad, normed)
            vs[i][rows, lanes] = jnp.where(low, sent, grad)
        return carry

    for i in range(4):
        for k in range(3):
            copy(k, i).wait()
        lax.fori_loop(i * part // step, (i + 1) * part // step, block, 0, unroll=True)


def side_kernel(place, u, v, u1, v1, mix_bias, columns, bias):
    p = place[0]
    low = p < 2
    own_bias = mix_bias[:, pl.ds(pl.multiple_of(p * ROWS, ROWS), ROWS)]
    columns[...] = jnp.concatenate([own_bias, jnp.zeros((ROWS - GROUPS, ROWS), F32)], axis=0).T
    bias[...] = jnp.zeros_like(bias)
    ones = jnp.ones((8, WIDTH), BF16)
    us, vs = (u, u1), (v, v1)
    for g in range(GROUPS):
        i, lanes = lanes_of(g)
        grad = jnp.where(low, us[i][:, lanes], vs[i][:, lanes])
        bias[pl.ds(g * QUAD + p, 1), :] = nt(ones, grad)[:1]


def slab_kernel(place, rows, out):
    p = place[0]

    @pl.when(p < 3)
    def _():
        for g in range(GROUPS):
            out[g] = rows[:, g, : 3 * ROWS]

    @pl.when(p == 3)
    def _():
        for g in range(GROUPS):
            out[g] = rows[:, g, ROWS:]


def join_kernel(place, *refs):
    for k in range(4):
        refs[4][(place[1] + 4 - k) % 4] = refs[k][...]


def weight_kernel(place, mine, theirs, out):
    p, core = place[0], place[2]
    low = p < 2
    first = core == 0
    start = jnp.where(p == 3, 1, 0)
    r = lax.broadcasted_iota(jnp.int32, (ROWS, ROWS), 0) // SEG
    c = lax.broadcasted_iota(jnp.int32, (ROWS, ROWS), 1) // SEG

    def piece(t, g, s):
        cols = pl.ds(pl.multiple_of((s - start) * ROWS, ROWS), ROWS)
        ours, others = mine[t, g, :, cols], theirs[t, g, :, cols]
        return jnp.concatenate([jnp.where(first, ours, others), jnp.where(first, others, ours)], axis=0)

    @pl.when(low)
    def _():
        for g in range(GROUPS):
            for i in range(2):
                for j in range(3):
                    got = piece(p + j, g, jnp.maximum(p - i, 0)).astype(F32)
                    if i == 0 and j == 0:
                        got = jnp.where(r >= c, got, 0.0)
                    out[g, i * ROWS : (i + 1) * ROWS, j * ROWS : (j + 1) * ROWS] = got.T.astype(BF16)

    @pl.when(jnp.logical_not(low))
    def _():
        for g in range(GROUPS):
            for i in range(2):
                for j in range(3):
                    got = piece(jnp.minimum(p + i, 3), g, p - j)
                    if i == 0 and j == 0:
                        got = jnp.where(r >= c, got.astype(F32), 0.0).astype(BF16)
                    out[g, i * ROWS : (i + 1) * ROWS, j * ROWS : (j + 1) * ROWS] = got


def product_kernel(chunk, place, u, v, near, far, swap, weights, gain, shift, part, out_u, out_v, *normed):
    p = place[0]
    for g in range(GROUPS):
        i, lanes = lanes_of(g)
        if i != chunk:
            continue
        cols = slice(g * WIDTH, (g + 1) * WIDTH)
        own, other = weights[g, :ROWS, :], weights[g, ROWS:, :]
        both = jnp.concatenate([own[:, :ROWS], other[:, :ROWS]], axis=0)

        def put(slot, ref, here):
            got = ref[:, lanes].astype(F32) * gain[:, cols] + shift[:, cols]
            if here is not None:
                got = jnp.where(here, got, 0.0)
            normed[slot][:, lanes] = got.astype(BF16)

        def products(long_side, short_side):
            long_side = jnp.concatenate([ref[:, lanes] for ref in long_side], axis=0)
            short_side = jnp.concatenate([ref[:, lanes] for ref in short_side], axis=0)
            part[:, lanes] = nn(other, long_side).astype(BF16)
            out_u[:, lanes] = nn(own, long_side)
            out_v[:, lanes] = tn(both, short_side)

        @pl.when(p < 2)
        def _():
            put(0, v, None)
            put(1, near, p == 1)
            products((u, swap, far), normed)

        @pl.when(p >= 2)
        def _():
            put(0, swap, p == 2)
            put(1, far, p == 2)
            products((u, *normed), (v, near))


def mix_grad_kernel(n, place, u, v, near, far, swap, one, two, keep, send):
    p, core = place[0], place[2]
    first = core == 0
    r = lax.broadcasted_iota(jnp.int32, (ROWS, ROWS), 0) // SEG
    c = lax.broadcasted_iota(jnp.int32, (ROWS, ROWS), 1) // SEG
    keep[...] = jnp.zeros_like(keep)
    send[...] = jnp.zeros_like(send)

    def put(target, slot, k, got):
        lanes = slice((slot * n + k) * ROWS, (slot * n + k + 1) * ROWS)
        keep[target, :, lanes] = jnp.where(first, got[:SEG], got[SEG:])
        send[target, :, lanes] = jnp.where(first, got[SEG:], got[:SEG]).astype(BF16)

    for k in range(n):
        at = slice(k * WIDTH, (k + 1) * WIDTH)

        @pl.when(p == 0)
        def _():
            put(0, 0, k, jnp.where(r >= c, nt(u[:, at], one[:, at]), 0.0))

        @pl.when(p == 1)
        def _():
            put(1, 0, k, nt(u[:, at], two[:, at]))
            put(1, 1, k, jnp.where(r >= c, nt(u[:, at], one[:, at]), 0.0))
            put(2, 0, k, nt(swap[:, at], two[:, at]))
            put(3, 0, k, nt(far[:, at], two[:, at]))

        @pl.when(p == 2)
        def _():
            put(2, 0, k, jnp.where(r >= c, nt(v[:, at], u[:, at]), 0.0))
            put(2, 1, k, nt(v[:, at], one[:, at]))
            put(3, 0, k, nt(near[:, at], u[:, at]))
            put(3, 1, k, nt(near[:, at], one[:, at]))

        @pl.when(p == 3)
        def _():
            put(3, 0, k, jnp.where(r >= c, nt(v[:, at], u[:, at]), 0.0))


def split(x):
    high = x.astype(BF16)
    return high, (x - high.astype(F32)).astype(BF16)


def sums_kernel(chunk, place, values, stats, before, out_u, out_v, part, near, small):
    p = place[0]
    small[...] = before[...]
    mean = stats[0, :, :1]
    inv = stats[1, :, :1]
    for g in range(GROUPS):
        i, lanes = lanes_of(g)
        if i != chunk:
            continue
        for k in range(WIDTH // 128):
            own = slice(lanes.start + k * 128, lanes.start + (k + 1) * 128)
            cols = slice(g * WIDTH + k * 128, g * WIDTH + (k + 1) * 128)
            back = jnp.where(p < 2, out_u[:, own], out_v[:, own])
            unit = (values[0, :, cols].astype(F32) - mean) * inv
            sent = jnp.where(p == 1, part[:, own].astype(F32), 0.0)
            row = 16 + g * 6 + k
            gain_rows = back * unit + sent * near[:, own].astype(F32)
            small[row : row + 1] = jnp.sum(gain_rows, axis=0, keepdims=True)
            small[row + 24 : row + 25] = jnp.sum(back + sent, axis=0, keepdims=True)


def last_sums_kernel(place, values, stats, before, out_u, out_v, part, near, last, small, send):
    sums_kernel(1, place, values, stats, before, out_u, out_v, part, near, small)
    send[:4] = last[...]
    high, low = split(small[...])
    send[4, :, :128] = high
    send[4, :, 128:] = low


def last_kernel(place, u, v, near, far, swap, weights, gain, shift, values, stats, before, *refs):
    part, out_u, out_v, keep, small, send, one, two, terms = refs
    product_kernel(1, place, u, v, near, far, swap, weights, gain, shift, part, out_u, out_v, one, two)
    mix_grad_kernel(CHUNKS[1], place, u, v, near, far, swap, one, two, keep, terms)
    last_sums_kernel(place, values, stats, before, out_u, out_v, part, near, terms, small, send)


def chip_kernel(place, keep, got, own, send):
    near = place[1] // 2 * 2
    for k in range(2):
        own[k] = keep[near + k] + got[near + k].astype(F32)
        other = 2 - near + k
        send[k] = (keep[other] + got[other].astype(F32)).astype(BF16)


def last_chip_kernel(place, keep, small, got, own, total, send):
    extra = small[...] + (got[4, :, :128].astype(F32) + got[4, :, 128:].astype(F32))
    high, low = split(extra)
    total[...] = extra
    send[2, :, :128] = high
    send[2, :, 128:] = low
    near = place[1] // 2 * 2
    for k in range(2):
        own[k] = keep[near + k] + got[near + k].astype(F32)
        other = 2 - near + k
        send[k] = (keep[other] + got[other].astype(F32)).astype(BF16)


def last_pair_kernel(place, keep0, got0, keep1, small, got1, own, total, send):
    extra = small[...] + (got1[2, :, :128].astype(F32) + got1[2, :, 128:].astype(F32))
    high, low = split(extra)
    total[...] = extra
    send[:, 1024:1152] = high
    send[:, 1152:1280] = low
    b = place[1] % 2
    for keep, got, first, width in ((keep0, got0, 0, 384), (keep1, got1, 384, 128)):
        mine = keep[b] + got[b].astype(F32)
        theirs = (keep[1 - b] + got[1 - b].astype(F32)).astype(BF16)
        for slot in range(2):
            lanes = slice(slot * 512 + first, slot * 512 + first + width)
            own[:, lanes] = mine[:, slot * width : (slot + 1) * width]
            send[:, lanes] = theirs[:, slot * width : (slot + 1) * width]


def deal_kernel(own, small, got, out):
    total = (own[...] + got[:, :1024].astype(F32)).astype(BF16)
    high, low = split(small[...] + (got[:, 1024:1152].astype(F32) + got[:, 1152:1280].astype(F32)))
    for z in range(8):
        rows = slice(z * 8, (z + 1) * 8)
        out[z, :, :1024] = total[rows]
        out[z, :, 1024:1152] = high[rows]
        out[z, :, 1152:1280] = low[rows]


def add_kernel(got, out):
    total = got[0].astype(F32)
    for z in range(1, 8):
        total = total + got[z].astype(F32)
    high, low = split(total[:, 1024:1152] + total[:, 1152:1280])
    total = total[:, :1024].astype(BF16)
    for y in range(8):
        out[y, :, :1024] = total
        out[y, :, 1024:1152] = high
        out[y, :, 1152:1280] = low


def place_kernel(got, out):
    def at(place, slot):
        lanes = slice(slot * 512, (slot + 1) * 512)
        return got[place, :, lanes].astype(F32) + got[place + QUAD, :, lanes].astype(F32)

    columns = (at(0, 0) + at(1, 0), at(1, 1) + at(2, 1), at(2, 0), at(3, 0))
    columns = [c.astype(BF16) for c in columns]
    extra = jnp.zeros((8, 128), F32)
    for y in range(8):
        extra = extra + got[y, :, 1024:1152].astype(F32) + got[y, :, 1152:1280].astype(F32)
    high, low = split(extra)
    for z in range(8):
        for s in range(4):
            for g in range(GROUPS):
                out[z, :, g * 512 + s * ROWS : g * 512 + (s + 1) * ROWS] = columns[s][
                    :, g * ROWS : (g + 1) * ROWS
                ]
        out[z, :, 2048:2176] = high
        out[z, :, 2176:2304] = low


def final_kernel(got, grad_mix, grad_bias, grad_gain, grad_shift):
    for z in range(8):
        rows = slice(z * 8, (z + 1) * 8)
        for g in range(GROUPS):
            grad_mix[rows, g, :] = got[z, :, g * 512 : (g + 1) * 512].astype(F32)
        small = got[z, :, 2048:2176].astype(F32) + got[z, :, 2176:2304].astype(F32)
        if z < 2:
            for i in range(8):
                g, p = 2 * z + i // QUAD, i % QUAD
                grad_bias[g : g + 1, p * ROWS : (p + 1) * ROWS] = small[i : i + 1]
        elif z < 5:
            grad_gain[(z - 2) * 8 : (z - 1) * 8] = small
        else:
            grad_shift[(z - 5) * 8 : (z - 4) * 8] = small


def post_kernel(place, values, upstream, stats, columns, gain, *refs):
    n = len(CHUNKS)
    outs_u, outs_v, got, to_u, to_v = refs[:n], refs[n : 2 * n], refs[2 * n : 3 * n], refs[3 * n], refs[3 * n + 1]
    grad_u, grad_v, backs, sems = refs[3 * n + 2 :]
    low = place[0] < 2
    step = 16
    part = ROWS // 4

    def copy(k, i):
        rows = slice(i * part, (i + 1) * part)
        source, target = ((grad_u, to_u), (grad_v, to_v))[k]
        return pltpu.make_async_copy(source.at[0, rows], target.at[0, rows], sems.at[k, i])

    def block(i, carry):
        rows = pl.ds(pl.multiple_of(i * step, step), step)
        mean = stats[0, rows, :1]
        inv = stats[1, rows, :1]
        first = jnp.zeros((step, 1), F32)
        second = jnp.zeros((step, 1), F32)
        for g in range(GROUPS):
            cols = slice(g * WIDTH, (g + 1) * WIDTH)
            c, lanes = lanes_of(g)
            long_side = outs_u[c][rows, lanes] + got[c][rows, lanes].astype(F32)
            short_side = outs_v[c][rows, lanes]
            mixed = jnp.where(low, short_side, long_side) + columns[rows, g : g + 1]
            mixed = mixed.astype(BF16).astype(F32)
            grad_u[0, rows, cols] = (upstream[0, rows, cols].astype(F32) * mixed).astype(BF16)
            back = jnp.where(low, long_side, short_side).astype(BF16)
            backs[rows, cols] = back
            scaled = back.astype(F32) * gain[:, cols]
            unit = (values[0, rows, cols].astype(F32) - mean) * inv
            first = first + jnp.sum(scaled, axis=1, keepdims=True)
            second = second + jnp.sum(scaled * unit, axis=1, keepdims=True)
        first = first * (1.0 / HALF)
        second = second * (1.0 / HALF)
        for g in range(GROUPS):
            cols = slice(g * WIDTH, (g + 1) * WIDTH)
            scaled = backs[rows, cols].astype(F32) * gain[:, cols]
            unit = (values[0, rows, cols].astype(F32) - mean) * inv
            grad_v[0, rows, cols] = (inv * (scaled - first - unit * second)).astype(BF16)
        return carry

    for i in range(4):
        lax.fori_loop(i * part // step, (i + 1) * part // step, block, 0, unroll=True)
        copy(0, i).start()
        copy(1, i).start()
    for i in range(4):
        copy(0, i).wait()
        copy(1, i).wait()


def exchanged(x, axis):
    return lax.all_to_all(x, axis, split_axis=0, concat_axis=0, tiled=True)


def compute(gated, values_in, upstream, gain, shift, mix_w, mix_bias):
    spot = lax.axis_index(Y) % QUAD
    place = jnp.stack([spot, lax.axis_index(X), lax.axis_index(CORE)]).astype(jnp.int32)
    gain_row, shift_row = gain.reshape(1, HALF), shift.reshape(1, HALF)
    n = len(CHUNKS)
    halves = [shape((ROWS, k * WIDTH), BF16) for k in CHUNKS]
    fulls = [shape((ROWS, k * WIDTH), F32) for k in CHUNKS]

    pre = call(
        pre_kernel,
        halves * 2 + [shape((2, ROWS, 128), F32)],
        (place, *map(far_memory, (values_in, gated, upstream, gain_row, shift_row))),
        scratch=[pltpu.VMEM((1, ROWS, HALF), BF16)] * 3
        + [pltpu.VMEM((1, HALF), F32)] * 2
        + [pltpu.SemaphoreType.DMA((3, 4)), pltpu.SemaphoreType.DMA((2,))],
        remote=range(1, 6),
    )
    us, vs, stats = pre[:n], pre[n : 2 * n], pre[2 * n]

    near, far, swap = [], [], []
    for i in range(n):
        near.append(lax.ppermute(vs[i], Y, NEAR))
        far.append(lax.ppermute(vs[i], Y, FAR))
        swap.append(lax.ppermute(vs[i], Y, SWAP))

    slab = call(slab_kernel, shape((GROUPS, SEG, 3 * ROWS), BF16), (place, mix_w))
    slabs = [slab] + [lax.ppermute(slab, X, CHIPS[k]) for k in range(1, 4)]
    mine = call(join_kernel, shape((4, GROUPS, SEG, 3 * ROWS), BF16), (place, *slabs))
    theirs = lax.ppermute(mine, CORE, PARTNER)
    columns, bias_term = call(
        side_kernel, [shape((ROWS, ROWS), F32), shape((64, 128), F32)], (place, us[0], vs[0], us[1], vs[1], mix_bias)
    )
    weights = call(weight_kernel, shape((GROUPS, 2 * ROWS, 3 * ROWS), BF16), (place, mine, theirs))

    operands = [(us[i], vs[i], near[i], far[i], swap[i]) for i in range(n)]
    part, out_u, out_v, one, two = call(
        functools.partial(product_kernel, 0),
        [halves[0], fulls[0], fulls[0], halves[0], halves[0]],
        (place, *operands[0], weights, gain_row, shift_row),
    )
    first_got = lax.ppermute(part, Y, OUT)
    dims = (4, SEG, 2 * CHUNKS[0] * ROWS)
    keep, send = call(
        functools.partial(mix_grad_kernel, CHUNKS[0]),
        [shape(dims, F32), shape(dims, BF16)],
        (place, *operands[0], one, two),
    )
    sums = call(
        functools.partial(sums_kernel, 0),
        shape((64, 128), F32),
        (place, values_in, stats, bias_term, out_u, out_v, part, near[0]),
    )
    keep, send = call(
        chip_kernel,
        [shape((2, SEG, 768), F32), shape((2, SEG, 768), BF16)],
        (place, keep, lax.ppermute(send, CORE, PARTNER)),
    )
    chip = (keep, lax.ppermute(send, X, ACROSS))

    part, last_u, last_v, keep, small, last = call(
        last_kernel,
        [
            halves[1],
            fulls[1],
            fulls[1],
            shape((4, SEG, 256), F32),
            shape((64, 128), F32),
            shape((5, SEG, 256), BF16),
        ],
        (place, *operands[1], weights, gain_row, shift_row, values_in, stats, sums),
        scratch=[pltpu.VMEM((ROWS, WIDTH), BF16)] * 2 + [pltpu.VMEM((4, SEG, 256), BF16)],
    )
    outs_u, outs_v, got = (out_u, last_u), (out_v, last_v), (first_got, lax.ppermute(part, Y, OUT))
    half_terms = [shape((2, SEG, 256), F32), shape((64, 128), F32), shape((3, SEG, 256), BF16)]
    own, small, send = call(last_chip_kernel, half_terms, (place, keep, small, lax.ppermute(last, CORE, PARTNER)))
    own, small, send = call(
        last_pair_kernel,
        [shape((SEG, 1024), F32), shape((64, 128), F32), shape((SEG, 1280), BF16)],
        (place, *chip, own, small, lax.ppermute(send, X, ACROSS)),
    )
    dealt = call(deal_kernel, shape((8, 8, 1280), BF16), (own, small, lax.ppermute(send, X, WITHIN)), 0)
    added = call(add_kernel, shape((8, 8, 1280), BF16), (exchanged(dealt, Z),), 0)
    placed = call(place_kernel, shape((8, 8, 2304), BF16), (exchanged(added, Y),), 0)
    grad_mix, grad_bias, grad_gain, grad_shift = call(
        final_kernel,
        [shape((SEG, GROUPS, 512), F32), shape((GROUPS, 512), F32)] + [shape((24, 128), F32)] * 2,
        (exchanged(placed, Z),),
        0,
    )

    grad_u, grad_v = call(
        post_kernel,
        [shape((1, ROWS, HALF), BF16)] * 2,
        (place, values_in, upstream, stats, columns, gain_row, *outs_u, *outs_v, *got),
        scratch=[pltpu.VMEM((1, ROWS, HALF), BF16)] * 2
        + [pltpu.VMEM((ROWS, HALF), BF16), pltpu.SemaphoreType.DMA((2, 4))],
        out=HBM,
    )
    return (grad_u, grad_v, grad_mix, grad_bias, grad_gain.reshape(HALF), grad_shift.reshape(HALF))


def solution(mesh):
    torus = Mesh(mesh.devices.reshape(8, 8, 4, 2), ("sp_0", "sp_1", "dp_0", "dp_1"))
    return jax.shard_map(
        compute,
        mesh=torus,
        in_specs=(
            P(DP, SP, None),
            P(DP, SP, None),
            P(DP, SP, None),
            P(),
            P(),
            P(DP, None, None),
            P(),
        ),
        out_specs=(P(DP, SP, None), P(DP, SP, None), P(DP, None, None), P(), P(), P()),
        check_vma=False,
    )
```

```python
import functools

import jax
import jax.numpy as jnp
from jax import lax
from jax.experimental import pallas as pl
from jax.experimental.pallas import tpu as pltpu
from jax.sharding import Mesh
from jax.sharding import PartitionSpec as P


SEG = 64
ROWS = 128
GROUPS = 4
WIDTH = 768
HALF = GROUPS * WIDTH
QUAD = 4
DP = ("dp_0", "dp_1")
SP = ("sp_0", "sp_1")
Y = "sp_1"
Z = "sp_0"
X = "dp_0"
CORE = "dp_1"
EPS = 1e-05

NEAR = [(0, 1), (3, 2), (4, 5), (7, 6)]
FAR = [(0, 2), (3, 1), (4, 6), (7, 5)]
SWAP = [(1, 2), (2, 1), (5, 6), (6, 5)]
OUT = [(1, 0), (2, 3), (5, 4), (6, 7)]
PARTNER = [(0, 1), (1, 0)]
CHIPS = [[(i, (i + k) % 4) for i in range(4)] for k in range(4)]
ACROSS = [(0, 3), (3, 0), (1, 2), (2, 1)]
WITHIN = [(0, 1), (1, 0), (2, 3), (3, 2)]

CHUNKS = (3, 1)
PLACES = [(i, k * WIDTH) for i, n in enumerate(CHUNKS) for k in range(n)]


VMEM = pl.BlockSpec(memory_space=pltpu.VMEM)
SMEM = pl.BlockSpec(memory_space=pltpu.SMEM)
HBM = pl.BlockSpec(memory_space=pltpu.HBM)
F32 = jnp.float32
BF16 = jnp.bfloat16


def far_memory(x):
    return pltpu.with_memory_space_constraint(x, pltpu.HBM)


def call(kernel, out_shape, inputs, scalars=1, scratch=(), vmem=16, remote=(), out=VMEM):
    return pl.pallas_call(
        kernel,
        out_shape=out_shape,
        in_specs=[SMEM] * scalars + [HBM if i in remote else VMEM for i in range(scalars, len(inputs))],
        out_specs=jax.tree.map(lambda _: out, out_shape),
        scratch_shapes=list(scratch),
        compiler_params=pltpu.CompilerParams(vmem_limit_bytes=vmem << 20),
    )(*inputs)


def shape(dims, dtype):
    return jax.ShapeDtypeStruct(dims, dtype)


def nt(a, b):
    return lax.dot_general(a, b, (((1,), (1,)), ((), ())), preferred_element_type=F32)


def tn(a, b):
    return lax.dot_general(a, b, (((0,), (0,)), ((), ())), preferred_element_type=F32)


def nn(a, b):
    return jnp.dot(a, b, preferred_element_type=F32)


def lanes_of(g, width=WIDTH):
    chunk, start = PLACES[g]
    start = start // WIDTH * width
    return chunk, slice(start, start + width)


def pre_kernel(place, values_in, gated_in, upstream_in, gain_in, shift_in, *outs):
    n = len(CHUNKS)
    us, vs, stats = outs[:n], outs[n : 2 * n], outs[2 * n]
    values, gated, upstream, gain, shift, sems, few = outs[2 * n + 1 :]
    low = place[0] < 2
    step = 16
    part = ROWS // 4
    pairs = ((values_in, values), (gated_in, gated), (upstream_in, upstream))

    def copy(k, i):
        rows = slice(i * part, (i + 1) * part)
        return pltpu.make_async_copy(pairs[k][0].at[0, rows], pairs[k][1].at[0, rows], sems.at[k, i])

    singles = [
        pltpu.make_async_copy(source, target, few.at[k])
        for k, (source, target) in enumerate(((gain_in, gain), (shift_in, shift)))
    ]
    copy(0, 0).start()
    for single in singles:
        single.start()
    copy(1, 0).start()
    copy(2, 0).start()
    for i in range(1, 4):
        for k in range(3):
            copy(k, i).start()
    for single in singles:
        single.wait()

    def block(i, carry):
        rows = pl.ds(pl.multiple_of(i * step, step), step)
        raw = values[0, rows, :].astype(F32)
        mean = jnp.sum(raw, axis=1, keepdims=True) * (1.0 / HALF)
        centred = raw - mean
        var = jnp.sum(centred * centred, axis=1, keepdims=True) * (1.0 / HALF)
        inv = lax.rsqrt(var + EPS)
        stats[0, rows, :] = jnp.broadcast_to(mean, (step, 128))
        stats[1, rows, :] = jnp.broadcast_to(inv, (step, 128))
        for g in range(GROUPS):
            cols = slice(g * WIDTH, (g + 1) * WIDTH)
            unit = (values[0, rows, cols].astype(F32) - mean) * inv
            normed = (unit * gain[:, cols] + shift[:, cols]).astype(BF16)
            sent = unit.astype(BF16)
            grad = (upstream[0, rows, cols].astype(F32) * gated[0, rows, cols].astype(F32)).astype(BF16)
            i, lanes = lanes_of(g)
            us[i][rows, lanes] = jnp.where(low, grad, normed)
            vs[i][rows, lanes] = jnp.where(low, sent, grad)
        return carry

    for i in range(4):
        for k in range(3):
            copy(k, i).wait()
        lax.fori_loop(i * part // step, (i + 1) * part // step, block, 0, unroll=True)


def side_kernel(place, u, v, u1, v1, mix_bias, columns, bias):
    p = place[0]
    low = p < 2
    own_bias = mix_bias[:, pl.ds(pl.multiple_of(p * ROWS, ROWS), ROWS)]
    columns[...] = jnp.concatenate([own_bias, jnp.zeros((ROWS - GROUPS, ROWS), F32)], axis=0).T
    bias[...] = jnp.zeros_like(bias)
    ones = jnp.ones((8, WIDTH), BF16)
    us, vs = (u, u1), (v, v1)
    for g in range(GROUPS):
        i, lanes = lanes_of(g)
        grad = jnp.where(low, us[i][:, lanes], vs[i][:, lanes])
        bias[pl.ds(g * QUAD + p, 1), :] = nt(ones, grad)[:1]


def slab_kernel(place, rows, out):
    p = place[0]

    @pl.when(p < 3)
    def _():
        for g in range(GROUPS):
            out[g] = rows[:, g, : 3 * ROWS]

    @pl.when(p == 3)
    def _():
        for g in range(GROUPS):
            out[g] = rows[:, g, ROWS:]


def join_kernel(place, *refs):
    for k in range(4):
        refs[4][(place[1] + 4 - k) % 4] = refs[k][...]


def weight_kernel(place, mine, theirs, out):
    p, core = place[0], place[2]
    low = p < 2
    first = core == 0
    start = jnp.where(p == 3, 1, 0)
    r = lax.broadcasted_iota(jnp.int32, (ROWS, ROWS), 0) // SEG
    c = lax.broadcasted_iota(jnp.int32, (ROWS, ROWS), 1) // SEG

    def piece(t, g, s):
        cols = pl.ds(pl.multiple_of((s - start) * ROWS, ROWS), ROWS)
        ours, others = mine[t, g, :, cols], theirs[t, g, :, cols]
        return jnp.concatenate([jnp.where(first, ours, others), jnp.where(first, others, ours)], axis=0)

    @pl.when(low)
    def _():
        for g in range(GROUPS):
            for i in range(2):
                for j in range(3):
                    got = piece(p + j, g, jnp.maximum(p - i, 0)).astype(F32)
                    if i == 0 and j == 0:
                        got = jnp.where(r >= c, got, 0.0)
                    out[g, i * ROWS : (i + 1) * ROWS, j * ROWS : (j + 1) * ROWS] = got.T.astype(BF16)

    @pl.when(jnp.logical_not(low))
    def _():
        for g in range(GROUPS):
            for i in range(2):
                for j in range(3):
                    got = piece(jnp.minimum(p + i, 3), g, p - j)
                    if i == 0 and j == 0:
                        got = jnp.where(r >= c, got.astype(F32), 0.0).astype(BF16)
                    out[g, i * ROWS : (i + 1) * ROWS, j * ROWS : (j + 1) * ROWS] = got


def product_kernel(chunk, place, u, v, near, far, swap, weights, gain, shift, part, out_u, out_v, *normed):
    p = place[0]
    for g in range(GROUPS):
        i, lanes = lanes_of(g)
        if i != chunk:
            continue
        cols = slice(g * WIDTH, (g + 1) * WIDTH)
        own, other = weights[g, :ROWS, :], weights[g, ROWS:, :]
        both = jnp.concatenate([own[:, :ROWS], other[:, :ROWS]], axis=0)

        def put(slot, ref, here):
            got = ref[:, lanes].astype(F32) * gain[:, cols] + shift[:, cols]
            if here is not None:
                got = jnp.where(here, got, 0.0)
            normed[slot][:, lanes] = got.astype(BF16)

        def products(long_side, short_side):
            long_side = jnp.concatenate([ref[:, lanes] for ref in long_side], axis=0)
            short_side = jnp.concatenate([ref[:, lanes] for ref in short_side], axis=0)
            part[:, lanes] = nn(other, long_side).astype(BF16)
            out_u[:, lanes] = nn(own, long_side)
            out_v[:, lanes] = tn(both, short_side)

        @pl.when(p < 2)
        def _():
            put(0, v, None)
            put(1, near, p == 1)
            products((u, swap, far), normed)

        @pl.when(p >= 2)
        def _():
            put(0, swap, p == 2)
            put(1, far, p == 2)
            products((u, *normed), (v, near))


def mix_grad_kernel(n, place, u, v, near, far, swap, one, two, keep, send):
    p, core = place[0], place[2]
    first = core == 0
    r = lax.broadcasted_iota(jnp.int32, (ROWS, ROWS), 0) // SEG
    c = lax.broadcasted_iota(jnp.int32, (ROWS, ROWS), 1) // SEG
    keep[...] = jnp.zeros_like(keep)
    send[...] = jnp.zeros_like(send)

    def put(target, slot, k, got):
        lanes = slice((slot * n + k) * ROWS, (slot * n + k + 1) * ROWS)
        keep[target, :, lanes] = jnp.where(first, got[:SEG], got[SEG:])
        send[target, :, lanes] = jnp.where(first, got[SEG:], got[:SEG]).astype(BF16)

    for k in range(n):
        at = slice(k * WIDTH, (k + 1) * WIDTH)

        @pl.when(p == 0)
        def _():
            put(0, 0, k, jnp.where(r >= c, nt(u[:, at], one[:, at]), 0.0))

        @pl.when(p == 1)
        def _():
            put(1, 0, k, nt(u[:, at], two[:, at]))
            put(1, 1, k, jnp.where(r >= c, nt(u[:, at], one[:, at]), 0.0))
            put(2, 0, k, nt(swap[:, at], two[:, at]))
            put(3, 0, k, nt(far[:, at], two[:, at]))

        @pl.when(p == 2)
        def _():
            put(2, 0, k, jnp.where(r >= c, nt(v[:, at], u[:, at]), 0.0))
            put(2, 1, k, nt(v[:, at], one[:, at]))
            put(3, 0, k, nt(near[:, at], u[:, at]))
            put(3, 1, k, nt(near[:, at], one[:, at]))

        @pl.when(p == 3)
        def _():
            put(3, 0, k, jnp.where(r >= c, nt(v[:, at], u[:, at]), 0.0))


def split(x):
    high = x.astype(BF16)
    return high, (x - high.astype(F32)).astype(BF16)


def sums_kernel(chunk, place, values, stats, before, out_u, out_v, part, near, small):
    p = place[0]
    small[...] = before[...]
    mean = stats[0, :, :1]
    inv = stats[1, :, :1]
    for g in range(GROUPS):
        i, lanes = lanes_of(g)
        if i != chunk:
            continue
        for k in range(WIDTH // 128):
            own = slice(lanes.start + k * 128, lanes.start + (k + 1) * 128)
            cols = slice(g * WIDTH + k * 128, g * WIDTH + (k + 1) * 128)
            back = jnp.where(p < 2, out_u[:, own], out_v[:, own])
            unit = (values[0, :, cols].astype(F32) - mean) * inv
            sent = jnp.where(p == 1, part[:, own].astype(F32), 0.0)
            row = 16 + g * 6 + k
            gain_rows = back * unit + sent * near[:, own].astype(F32)
            small[row : row + 1] = jnp.sum(gain_rows, axis=0, keepdims=True)
            small[row + 24 : row + 25] = jnp.sum(back + sent, axis=0, keepdims=True)


def last_sums_kernel(place, values, stats, before, out_u, out_v, part, near, last, small, send):
    sums_kernel(1, place, values, stats, before, out_u, out_v, part, near, small)
    send[:4] = last[...]
    high, low = split(small[...])
    send[4, :, :128] = high
    send[4, :, 128:] = low


def last_kernel(place, u, v, near, far, swap, weights, gain, shift, values, stats, before, *refs):
    part, out_u, out_v, keep, small, send, one, two, terms = refs
    product_kernel(1, place, u, v, near, far, swap, weights, gain, shift, part, out_u, out_v, one, two)
    mix_grad_kernel(CHUNKS[1], place, u, v, near, far, swap, one, two, keep, terms)
    last_sums_kernel(place, values, stats, before, out_u, out_v, part, near, terms, small, send)


def chip_kernel(place, keep0, got0, keep1, small, got1, own, total, send):
    extra = small[...] + (got1[4, :, :128].astype(F32) + got1[4, :, 128:].astype(F32))
    high, low = split(extra)
    total[...] = extra
    send[0, :, 1024:] = high
    send[1, :, 1024:] = low
    near = place[1] // 2 * 2
    for k in range(2):
        other = 2 - near + k
        for keep, got, first, width in ((keep0, got0, 0, 384), (keep1, got1, 384, 128)):
            for slot in range(2):
                at = slice(slot * width, (slot + 1) * width)
                lanes = slice(slot * 512 + first, slot * 512 + first + width)
                own[k, :, lanes] = keep[near + k, :, at] + got[near + k, :, at].astype(F32)
                send[k, :, lanes] = (keep[other, :, at] + got[other, :, at].astype(F32)).astype(BF16)


def pair_kernel(place, keep, small, got, own, total, send):
    extra = small[...] + (got[0, :, 1024:].astype(F32) + got[1, :, 1024:].astype(F32))
    high, low = split(extra)
    total[...] = extra
    send[:, 1024:1152] = high
    send[:, 1152:1280] = low
    b = place[1] % 2
    own[...] = keep[b] + got[b, :, :1024].astype(F32)
    send[:, :1024] = (keep[1 - b] + got[1 - b, :, :1024].astype(F32)).astype(BF16)


def deal_kernel(own, small, got, out):
    total = (own[...] + got[:, :1024].astype(F32)).astype(BF16)
    high, low = split(small[...] + (got[:, 1024:1152].astype(F32) + got[:, 1152:1280].astype(F32)))
    for z in range(8):
        rows = slice(z * 8, (z + 1) * 8)
        out[z, :, :1024] = total[rows]
        out[z, :, 1024:1152] = high[rows]
        out[z, :, 1152:1280] = low[rows]


def add_kernel(got, out):
    total = got[0].astype(F32)
    for z in range(1, 8):
        total = total + got[z].astype(F32)
    high, low = split(total[:, 1024:1152] + total[:, 1152:1280])
    total = total[:, :1024].astype(BF16)
    for y in range(8):
        out[y, :, :1024] = total
        out[y, :, 1024:1152] = high
        out[y, :, 1152:1280] = low


def place_kernel(got, out):
    def at(place, slot):
        lanes = slice(slot * 512, (slot + 1) * 512)
        return got[place, :, lanes].astype(F32) + got[place + QUAD, :, lanes].astype(F32)

    columns = (at(0, 0) + at(1, 0), at(1, 1) + at(2, 1), at(2, 0), at(3, 0))
    columns = [c.astype(BF16) for c in columns]
    extra = jnp.zeros((8, 128), F32)
    for y in range(8):
        extra = extra + got[y, :, 1024:1152].astype(F32) + got[y, :, 1152:1280].astype(F32)
    high, low = split(extra)
    for z in range(8):
        for s in range(4):
            for g in range(GROUPS):
                out[z, :, g * 512 + s * ROWS : g * 512 + (s + 1) * ROWS] = columns[s][
                    :, g * ROWS : (g + 1) * ROWS
                ]
        out[z, :, 2048:2176] = high
        out[z, :, 2176:2304] = low


def final_kernel(got, grad_mix, grad_bias, grad_gain, grad_shift):
    for z in range(8):
        rows = slice(z * 8, (z + 1) * 8)
        for g in range(GROUPS):
            grad_mix[rows, g, :] = got[z, :, g * 512 : (g + 1) * 512].astype(F32)
        small = got[z, :, 2048:2176].astype(F32) + got[z, :, 2176:2304].astype(F32)
        if z < 2:
            for i in range(8):
                g, p = 2 * z + i // QUAD, i % QUAD
                grad_bias[g : g + 1, p * ROWS : (p + 1) * ROWS] = small[i : i + 1]
        elif z < 5:
            grad_gain[(z - 2) * 8 : (z - 1) * 8] = small
        else:
            grad_shift[(z - 5) * 8 : (z - 4) * 8] = small


def post_kernel(place, values, upstream, stats, columns, gain, *refs):
    n = len(CHUNKS)
    outs_u, outs_v, got, to_u, to_v = refs[:n], refs[n : 2 * n], refs[2 * n : 3 * n], refs[3 * n], refs[3 * n + 1]
    grad_u, grad_v, backs, sems = refs[3 * n + 2 :]
    low = place[0] < 2
    step = 16
    part = ROWS // 4

    def copy(k, i):
        rows = slice(i * part, (i + 1) * part)
        source, target = ((grad_u, to_u), (grad_v, to_v))[k]
        return pltpu.make_async_copy(source.at[0, rows], target.at[0, rows], sems.at[k, i])

    def block(i, carry):
        rows = pl.ds(pl.multiple_of(i * step, step), step)
        mean = stats[0, rows, :1]
        inv = stats[1, rows, :1]
        first = jnp.zeros((step, 1), F32)
        second = jnp.zeros((step, 1), F32)
        for g in range(GROUPS):
            cols = slice(g * WIDTH, (g + 1) * WIDTH)
            c, lanes = lanes_of(g)
            long_side = outs_u[c][rows, lanes] + got[c][rows, lanes].astype(F32)
            short_side = outs_v[c][rows, lanes]
            mixed = jnp.where(low, short_side, long_side) + columns[rows, g : g + 1]
            mixed = mixed.astype(BF16).astype(F32)
            grad_u[0, rows, cols] = (upstream[0, rows, cols].astype(F32) * mixed).astype(BF16)
            back = jnp.where(low, long_side, short_side).astype(BF16)
            backs[rows, cols] = back
            scaled = back.astype(F32) * gain[:, cols]
            unit = (values[0, rows, cols].astype(F32) - mean) * inv
            first = first + jnp.sum(scaled, axis=1, keepdims=True)
            second = second + jnp.sum(scaled * unit, axis=1, keepdims=True)
        first = first * (1.0 / HALF)
        second = second * (1.0 / HALF)
        for g in range(GROUPS):
            cols = slice(g * WIDTH, (g + 1) * WIDTH)
            scaled = backs[rows, cols].astype(F32) * gain[:, cols]
            unit = (values[0, rows, cols].astype(F32) - mean) * inv
            grad_v[0, rows, cols] = (inv * (scaled - first - unit * second)).astype(BF16)
        return carry

    for i in range(4):
        lax.fori_loop(i * part // step, (i + 1) * part // step, block, 0, unroll=True)
        copy(0, i).start()
        copy(1, i).start()
    for i in range(4):
        copy(0, i).wait()
        copy(1, i).wait()


def exchanged(x, axis):
    return lax.all_to_all(x, axis, split_axis=0, concat_axis=0, tiled=True)


def compute(gated, values_in, upstream, gain, shift, mix_w, mix_bias):
    spot = lax.axis_index(Y) % QUAD
    place = jnp.stack([spot, lax.axis_index(X), lax.axis_index(CORE)]).astype(jnp.int32)
    gain_row, shift_row = gain.reshape(1, HALF), shift.reshape(1, HALF)
    n = len(CHUNKS)
    halves = [shape((ROWS, k * WIDTH), BF16) for k in CHUNKS]
    fulls = [shape((ROWS, k * WIDTH), F32) for k in CHUNKS]

    pre = call(
        pre_kernel,
        halves * 2 + [shape((2, ROWS, 128), F32)],
        (place, *map(far_memory, (values_in, gated, upstream, gain_row, shift_row))),
        scratch=[pltpu.VMEM((1, ROWS, HALF), BF16)] * 3
        + [pltpu.VMEM((1, HALF), F32)] * 2
        + [pltpu.SemaphoreType.DMA((3, 4)), pltpu.SemaphoreType.DMA((2,))],
        remote=range(1, 6),
    )
    us, vs, stats = pre[:n], pre[n : 2 * n], pre[2 * n]

    near, far, swap = [], [], []
    for i in range(n):
        near.append(lax.ppermute(vs[i], Y, NEAR))
        far.append(lax.ppermute(vs[i], Y, FAR))
        swap.append(lax.ppermute(vs[i], Y, SWAP))

    slab = call(slab_kernel, shape((GROUPS, SEG, 3 * ROWS), BF16), (place, mix_w))
    slabs = [slab] + [lax.ppermute(slab, X, CHIPS[k]) for k in range(1, 4)]
    mine = call(join_kernel, shape((4, GROUPS, SEG, 3 * ROWS), BF16), (place, *slabs))
    theirs = lax.ppermute(mine, CORE, PARTNER)
    columns, bias_term = call(
        side_kernel, [shape((ROWS, ROWS), F32), shape((64, 128), F32)], (place, us[0], vs[0], us[1], vs[1], mix_bias)
    )
    weights = call(weight_kernel, shape((GROUPS, 2 * ROWS, 3 * ROWS), BF16), (place, mine, theirs))

    operands = [(us[i], vs[i], near[i], far[i], swap[i]) for i in range(n)]
    part, out_u, out_v, one, two = call(
        functools.partial(product_kernel, 0),
        [halves[0], fulls[0], fulls[0], halves[0], halves[0]],
        (place, *operands[0], weights, gain_row, shift_row),
    )
    first_got = lax.ppermute(part, Y, OUT)
    dims = (4, SEG, 2 * CHUNKS[0] * ROWS)
    keep, send = call(
        functools.partial(mix_grad_kernel, CHUNKS[0]),
        [shape(dims, F32), shape(dims, BF16)],
        (place, *operands[0], one, two),
    )
    sums = call(
        functools.partial(sums_kernel, 0),
        shape((64, 128), F32),
        (place, values_in, stats, bias_term, out_u, out_v, part, near[0]),
    )
    folded = (keep, lax.ppermute(send, CORE, PARTNER))

    part, last_u, last_v, keep, small, last = call(
        last_kernel,
        [
            halves[1],
            fulls[1],
            fulls[1],
            shape((4, SEG, 256), F32),
            shape((64, 128), F32),
            shape((5, SEG, 256), BF16),
        ],
        (place, *operands[1], weights, gain_row, shift_row, values_in, stats, sums),
        scratch=[pltpu.VMEM((ROWS, WIDTH), BF16)] * 2 + [pltpu.VMEM((4, SEG, 256), BF16)],
    )
    outs_u, outs_v, got = (out_u, last_u), (out_v, last_v), (first_got, lax.ppermute(part, Y, OUT))
    own, small, send = call(
        chip_kernel,
        [shape((2, SEG, 1024), F32), shape((64, 128), F32), shape((2, SEG, 1152), BF16)],
        (place, *folded, keep, small, lax.ppermute(last, CORE, PARTNER)),
    )
    own, small, send = call(
        pair_kernel,
        [shape((SEG, 1024), F32), shape((64, 128), F32), shape((SEG, 1280), BF16)],
        (place, own, small, lax.ppermute(send, X, ACROSS)),
    )
    dealt = call(deal_kernel, shape((8, 8, 1280), BF16), (own, small, lax.ppermute(send, X, WITHIN)), 0)
    added = call(add_kernel, shape((8, 8, 1280), BF16), (exchanged(dealt, Z),), 0)
    placed = call(place_kernel, shape((8, 8, 2304), BF16), (exchanged(added, Y),), 0)
    grad_mix, grad_bias, grad_gain, grad_shift = call(
        final_kernel,
        [shape((SEG, GROUPS, 512), F32), shape((GROUPS, 512), F32)] + [shape((24, 128), F32)] * 2,
        (exchanged(placed, Z),),
        0,
    )

    grad_u, grad_v = call(
        post_kernel,
        [shape((1, ROWS, HALF), BF16)] * 2,
        (place, values_in, upstream, stats, columns, gain_row, *outs_u, *outs_v, *got),
        scratch=[pltpu.VMEM((1, ROWS, HALF), BF16)] * 2
        + [pltpu.VMEM((ROWS, HALF), BF16), pltpu.SemaphoreType.DMA((2, 4))],
        out=HBM,
    )
    return (grad_u, grad_v, grad_mix, grad_bias, grad_gain.reshape(HALF), grad_shift.reshape(HALF))


def solution(mesh):
    torus = Mesh(mesh.devices.reshape(8, 8, 4, 2), ("sp_0", "sp_1", "dp_0", "dp_1"))
    return jax.shard_map(
        compute,
        mesh=torus,
        in_specs=(
            P(DP, SP, None),
            P(DP, SP, None),
            P(DP, SP, None),
            P(),
            P(),
            P(DP, None, None),
            P(),
        ),
        out_specs=(P(DP, SP, None), P(DP, SP, None), P(DP, None, None), P(), P(), P()),
        check_vma=False,
    )
```

```python
import functools

import jax
import jax.numpy as jnp
from jax import lax
from jax.experimental import pallas as pl
from jax.experimental.pallas import tpu as pltpu
from jax.sharding import Mesh
from jax.sharding import PartitionSpec as P


SEG = 64
ROWS = 128
GROUPS = 4
WIDTH = 768
HALF = GROUPS * WIDTH
QUAD = 4
DP = ("dp_0", "dp_1")
SP = ("sp_0", "sp_1")
Y = "sp_1"
Z = "sp_0"
X = "dp_0"
CORE = "dp_1"
EPS = 1e-05

NEAR = [(0, 1), (3, 2), (4, 5), (7, 6)]
FAR = [(0, 2), (3, 1), (4, 6), (7, 5)]
SWAP = [(1, 2), (2, 1), (5, 6), (6, 5)]
OUT = [(1, 0), (2, 3), (5, 4), (6, 7)]
PARTNER = [(0, 1), (1, 0)]
CHIPS = [[(i, (i + k) % 4) for i in range(4)] for k in range(4)]
ACROSS = [(0, 3), (3, 0), (1, 2), (2, 1)]
WITHIN = [(0, 1), (1, 0), (2, 3), (3, 2)]

CHUNKS = (3, 1)
PLACES = [(i, k * WIDTH) for i, n in enumerate(CHUNKS) for k in range(n)]


VMEM = pl.BlockSpec(memory_space=pltpu.VMEM)
SMEM = pl.BlockSpec(memory_space=pltpu.SMEM)
HBM = pl.BlockSpec(memory_space=pltpu.HBM)
F32 = jnp.float32
BF16 = jnp.bfloat16


def far_memory(x):
    return pltpu.with_memory_space_constraint(x, pltpu.HBM)


def call(kernel, out_shape, inputs, scalars=1, scratch=(), vmem=16, remote=(), out=VMEM):
    return pl.pallas_call(
        kernel,
        out_shape=out_shape,
        in_specs=[SMEM] * scalars + [HBM if i in remote else VMEM for i in range(scalars, len(inputs))],
        out_specs=jax.tree.map(lambda _: out, out_shape),
        scratch_shapes=list(scratch),
        compiler_params=pltpu.CompilerParams(vmem_limit_bytes=vmem << 20),
    )(*inputs)


def shape(dims, dtype):
    return jax.ShapeDtypeStruct(dims, dtype)


def nt(a, b):
    return lax.dot_general(a, b, (((1,), (1,)), ((), ())), preferred_element_type=F32)


def tn(a, b):
    return lax.dot_general(a, b, (((0,), (0,)), ((), ())), preferred_element_type=F32)


def nn(a, b):
    return jnp.dot(a, b, preferred_element_type=F32)


def lanes_of(g, width=WIDTH):
    chunk, start = PLACES[g]
    start = start // WIDTH * width
    return chunk, slice(start, start + width)


TILES = [slice(k * 128, (k + 1) * 128) for k in range(HALF // 128)]


def tile_of(k):
    chunk, start = PLACES[k * 128 // WIDTH]
    start += k * 128 % WIDTH
    return chunk, slice(start, start + 128)


def row_mean(terms):
    totals = [None] * 4
    for k, term in enumerate(terms):
        totals[k % 4] = term if totals[k % 4] is None else totals[k % 4] + term
    total = (totals[0] + totals[1]) + (totals[2] + totals[3])
    return jnp.sum(total, axis=1, keepdims=True) * (1.0 / HALF)


def add_term(totals, term):
    return totals + [term] if len(totals) < 4 else totals[1:] + [totals[0] + term]


def pre_kernel(place, values_in, gated_in, upstream_in, gain_in, shift_in, *outs):
    n = len(CHUNKS)
    us, vs, stats = outs[:n], outs[n : 2 * n], outs[2 * n]
    values, gated, upstream, gain, shift, sems, few = outs[2 * n + 1 :]
    low = place[0] < 2
    step = 16
    part = ROWS // 4
    pairs = ((values_in, values), (gated_in, gated), (upstream_in, upstream))

    def copy(k, i):
        rows = slice(i * part, (i + 1) * part)
        return pltpu.make_async_copy(pairs[k][0].at[0, rows], pairs[k][1].at[0, rows], sems.at[k, i])

    singles = [
        pltpu.make_async_copy(source, target, few.at[k])
        for k, (source, target) in enumerate(((gain_in, gain), (shift_in, shift)))
    ]
    copy(0, 0).start()
    for single in singles:
        single.start()
    copy(1, 0).start()
    copy(2, 0).start()
    for i in range(1, 4):
        for k in range(3):
            copy(k, i).start()
    for single in singles:
        single.wait()

    def measure(i, carry):
        rows = pl.ds(pl.multiple_of(i * step, step), step)
        mean = row_mean(values[0, rows, at].astype(F32) for at in TILES)
        centred = (values[0, rows, at].astype(F32) - mean for at in TILES)
        inv = lax.rsqrt(row_mean(c * c for c in centred) + EPS)
        stats[0, rows, :] = jnp.broadcast_to(mean, (step, 128))
        stats[1, rows, :] = jnp.broadcast_to(inv, (step, 128))
        return carry

    def block(low, i, carry):
        rows = pl.ds(pl.multiple_of(i * step, step), step)
        mean, inv = stats[0, rows, :], stats[1, rows, :]
        for k, at in enumerate(TILES):
            chunk, lanes = tile_of(k)
            unit = (values[0, rows, at].astype(F32) - mean) * inv
            grad = (upstream[0, rows, at].astype(F32) * gated[0, rows, at].astype(F32)).astype(BF16)
            if low:
                us[chunk][rows, lanes] = grad
                vs[chunk][rows, lanes] = unit.astype(BF16)
            else:
                us[chunk][rows, lanes] = (unit * gain[:, at] + shift[:, at]).astype(BF16)
                vs[chunk][rows, lanes] = grad
        return carry

    for i in range(4):
        copy(0, i).wait()
        lax.fori_loop(i * part // step, (i + 1) * part // step, measure, 0, unroll=True)
    for k in range(1, 3):
        for i in range(4):
            copy(k, i).wait()

    @pl.when(low)
    def _():
        lax.fori_loop(0, ROWS // step, functools.partial(block, True), 0, unroll=2)

    @pl.when(jnp.logical_not(low))
    def _():
        lax.fori_loop(0, ROWS // step, functools.partial(block, False), 0, unroll=2)


def side_kernel(place, u, v, u1, v1, mix_bias, columns, bias):
    p = place[0]
    low = p < 2
    own_bias = mix_bias[:, pl.ds(pl.multiple_of(p * ROWS, ROWS), ROWS)]
    columns[...] = jnp.concatenate([own_bias, jnp.zeros((ROWS - GROUPS, ROWS), F32)], axis=0).T
    bias[...] = jnp.zeros_like(bias)
    ones = jnp.ones((8, WIDTH), BF16)
    us, vs = (u, u1), (v, v1)
    for g in range(GROUPS):
        i, lanes = lanes_of(g)
        grad = jnp.where(low, us[i][:, lanes], vs[i][:, lanes])
        bias[pl.ds(g * QUAD + p, 1), :] = nt(ones, grad)[:1]


def slab_kernel(place, rows, out):
    p = place[0]

    @pl.when(p < 3)
    def _():
        for g in range(GROUPS):
            out[g] = rows[:, g, : 3 * ROWS]

    @pl.when(p == 3)
    def _():
        for g in range(GROUPS):
            out[g] = rows[:, g, ROWS:]


def join_kernel(place, *refs):
    for k in range(4):
        refs[4][(place[1] + 4 - k) % 4] = refs[k][...]


def weight_kernel(place, mine, theirs, out):
    p, core = place[0], place[2]
    low = p < 2
    first = core == 0
    start = jnp.where(p == 3, 1, 0)
    r = lax.broadcasted_iota(jnp.int32, (ROWS, ROWS), 0) // SEG
    c = lax.broadcasted_iota(jnp.int32, (ROWS, ROWS), 1) // SEG

    def piece(t, g, s):
        cols = pl.ds(pl.multiple_of((s - start) * ROWS, ROWS), ROWS)
        ours, others = mine[t, g, :, cols], theirs[t, g, :, cols]
        return jnp.concatenate([jnp.where(first, ours, others), jnp.where(first, others, ours)], axis=0)

    @pl.when(low)
    def _():
        for g in range(GROUPS):
            for i in range(2):
                for j in range(3):
                    got = piece(p + j, g, jnp.maximum(p - i, 0)).astype(F32)
                    if i == 0 and j == 0:
                        got = jnp.where(r >= c, got, 0.0)
                    out[g, i * ROWS : (i + 1) * ROWS, j * ROWS : (j + 1) * ROWS] = got.T.astype(BF16)

    @pl.when(jnp.logical_not(low))
    def _():
        for g in range(GROUPS):
            for i in range(2):
                for j in range(3):
                    got = piece(jnp.minimum(p + i, 3), g, p - j)
                    if i == 0 and j == 0:
                        got = jnp.where(r >= c, got.astype(F32), 0.0).astype(BF16)
                    out[g, i * ROWS : (i + 1) * ROWS, j * ROWS : (j + 1) * ROWS] = got


def product_kernel(chunk, place, u, v, near, far, swap, weights, gain, shift, part, out_u, out_v, *normed):
    p = place[0]
    for g in range(GROUPS):
        i, lanes = lanes_of(g)
        if i != chunk:
            continue
        cols = slice(g * WIDTH, (g + 1) * WIDTH)
        own, other = weights[g, :ROWS, :], weights[g, ROWS:, :]
        both = jnp.concatenate([own[:, :ROWS], other[:, :ROWS]], axis=0)

        def put(slot, ref, here):
            got = ref[:, lanes].astype(F32) * gain[:, cols] + shift[:, cols]
            if here is not None:
                got = jnp.where(here, got, 0.0)
            normed[slot][:, lanes] = got.astype(BF16)

        def products(long_side, short_side):
            long_side = jnp.concatenate([ref[:, lanes] for ref in long_side], axis=0)
            short_side = jnp.concatenate([ref[:, lanes] for ref in short_side], axis=0)
            part[:, lanes] = nn(other, long_side).astype(BF16)
            out_u[:, lanes] = nn(own, long_side)
            out_v[:, lanes] = tn(both, short_side)

        @pl.when(p < 2)
        def _():
            put(0, v, None)
            put(1, near, p == 1)
            products((u, swap, far), normed)

        @pl.when(p >= 2)
        def _():
            put(0, swap, p == 2)
            put(1, far, p == 2)
            products((u, *normed), (v, near))


def mix_grad_kernel(n, place, u, v, near, far, swap, one, two, keep, send):
    p, core = place[0], place[2]
    first = core == 0
    r = lax.broadcasted_iota(jnp.int32, (ROWS, ROWS), 0) // SEG
    c = lax.broadcasted_iota(jnp.int32, (ROWS, ROWS), 1) // SEG
    keep[...] = jnp.zeros_like(keep)
    send[...] = jnp.zeros_like(send)

    def put(target, slot, k, got):
        lanes = slice((slot * n + k) * ROWS, (slot * n + k + 1) * ROWS)
        keep[target, :, lanes] = jnp.where(first, got[:SEG], got[SEG:])
        send[target, :, lanes] = jnp.where(first, got[SEG:], got[:SEG]).astype(BF16)

    for k in range(n):
        at = slice(k * WIDTH, (k + 1) * WIDTH)

        @pl.when(p == 0)
        def _():
            put(0, 0, k, jnp.where(r >= c, nt(u[:, at], one[:, at]), 0.0))

        @pl.when(p == 1)
        def _():
            put(1, 0, k, nt(u[:, at], two[:, at]))
            put(1, 1, k, jnp.where(r >= c, nt(u[:, at], one[:, at]), 0.0))
            put(2, 0, k, nt(swap[:, at], two[:, at]))
            put(3, 0, k, nt(far[:, at], two[:, at]))

        @pl.when(p == 2)
        def _():
            put(2, 0, k, jnp.where(r >= c, nt(v[:, at], u[:, at]), 0.0))
            put(2, 1, k, nt(v[:, at], one[:, at]))
            put(3, 0, k, nt(near[:, at], u[:, at]))
            put(3, 1, k, nt(near[:, at], one[:, at]))

        @pl.when(p == 3)
        def _():
            put(3, 0, k, jnp.where(r >= c, nt(v[:, at], u[:, at]), 0.0))


def split(x):
    high = x.astype(BF16)
    return high, (x - high.astype(F32)).astype(BF16)


def sums_kernel(chunk, place, values, stats, before, out_u, out_v, part, near, small):
    p = place[0]
    small[...] = before[...]
    mean = stats[0, :, :1]
    inv = stats[1, :, :1]
    for g in range(GROUPS):
        i, lanes = lanes_of(g)
        if i != chunk:
            continue
        for k in range(WIDTH // 128):
            own = slice(lanes.start + k * 128, lanes.start + (k + 1) * 128)
            cols = slice(g * WIDTH + k * 128, g * WIDTH + (k + 1) * 128)
            back = jnp.where(p < 2, out_u[:, own], out_v[:, own])
            unit = (values[0, :, cols].astype(F32) - mean) * inv
            sent = jnp.where(p == 1, part[:, own].astype(F32), 0.0)
            row = 16 + g * 6 + k
            gain_rows = back * unit + sent * near[:, own].astype(F32)
            small[row : row + 1] = jnp.sum(gain_rows, axis=0, keepdims=True)
            small[row + 24 : row + 25] = jnp.sum(back + sent, axis=0, keepdims=True)


def last_sums_kernel(place, values, stats, before, out_u, out_v, part, near, last, small, send):
    sums_kernel(1, place, values, stats, before, out_u, out_v, part, near, small)
    send[:4] = last[...]
    high, low = split(small[...])
    send[4, :, :128] = high
    send[4, :, 128:] = low


def last_kernel(place, u, v, near, far, swap, weights, gain, shift, values, stats, before, *refs):
    part, out_u, out_v, keep, small, send, one, two, terms = refs
    product_kernel(1, place, u, v, near, far, swap, weights, gain, shift, part, out_u, out_v, one, two)
    mix_grad_kernel(CHUNKS[1], place, u, v, near, far, swap, one, two, keep, terms)
    last_sums_kernel(place, values, stats, before, out_u, out_v, part, near, terms, small, send)


def chip_kernel(place, keep0, got0, keep1, small, got1, own, total, send):
    extra = small[...] + (got1[4, :, :128].astype(F32) + got1[4, :, 128:].astype(F32))
    high, low = split(extra)
    total[...] = extra
    send[0, :, 1024:] = high
    send[1, :, 1024:] = low
    near = place[1] // 2 * 2
    for k in range(2):
        other = 2 - near + k
        for keep, got, first, width in ((keep0, got0, 0, 384), (keep1, got1, 384, 128)):
            for slot in range(2):
                at = slice(slot * width, (slot + 1) * width)
                lanes = slice(slot * 512 + first, slot * 512 + first + width)
                own[k, :, lanes] = keep[near + k, :, at] + got[near + k, :, at].astype(F32)
                send[k, :, lanes] = (keep[other, :, at] + got[other, :, at].astype(F32)).astype(BF16)


def pair_kernel(place, keep, small, got, own, total, send):
    extra = small[...] + (got[0, :, 1024:].astype(F32) + got[1, :, 1024:].astype(F32))
    high, low = split(extra)
    total[...] = extra
    send[:, 1024:1152] = high
    send[:, 1152:1280] = low
    b = place[1] % 2
    own[...] = keep[b] + got[b, :, :1024].astype(F32)
    send[:, :1024] = (keep[1 - b] + got[1 - b, :, :1024].astype(F32)).astype(BF16)


def deal_kernel(own, small, got, out):
    total = (own[...] + got[:, :1024].astype(F32)).astype(BF16)
    high, low = split(small[...] + (got[:, 1024:1152].astype(F32) + got[:, 1152:1280].astype(F32)))
    for z in range(8):
        rows = slice(z * 8, (z + 1) * 8)
        out[z, :, :1024] = total[rows]
        out[z, :, 1024:1152] = high[rows]
        out[z, :, 1152:1280] = low[rows]


def add_kernel(got, out):
    total = got[0].astype(F32)
    for z in range(1, 8):
        total = total + got[z].astype(F32)
    high, low = split(total[:, 1024:1152] + total[:, 1152:1280])
    total = total[:, :1024].astype(BF16)
    for y in range(8):
        out[y, :, :1024] = total
        out[y, :, 1024:1152] = high
        out[y, :, 1152:1280] = low


def place_kernel(got, out):
    def at(place, slot):
        lanes = slice(slot * 512, (slot + 1) * 512)
        return got[place, :, lanes].astype(F32) + got[place + QUAD, :, lanes].astype(F32)

    columns = (at(0, 0) + at(1, 0), at(1, 1) + at(2, 1), at(2, 0), at(3, 0))
    columns = [c.astype(BF16) for c in columns]
    extra = jnp.zeros((8, 128), F32)
    for y in range(8):
        extra = extra + got[y, :, 1024:1152].astype(F32) + got[y, :, 1152:1280].astype(F32)
    high, low = split(extra)
    for z in range(8):
        for s in range(4):
            for g in range(GROUPS):
                out[z, :, g * 512 + s * ROWS : g * 512 + (s + 1) * ROWS] = columns[s][
                    :, g * ROWS : (g + 1) * ROWS
                ]
        out[z, :, 2048:2176] = high
        out[z, :, 2176:2304] = low


def final_kernel(got, grad_mix, grad_bias, grad_gain, grad_shift):
    for z in range(8):
        rows = slice(z * 8, (z + 1) * 8)
        for g in range(GROUPS):
            grad_mix[rows, g, :] = got[z, :, g * 512 : (g + 1) * 512].astype(F32)
        small = got[z, :, 2048:2176].astype(F32) + got[z, :, 2176:2304].astype(F32)
        if z < 2:
            for i in range(8):
                g, p = 2 * z + i // QUAD, i % QUAD
                grad_bias[g : g + 1, p * ROWS : (p + 1) * ROWS] = small[i : i + 1]
        elif z < 5:
            grad_gain[(z - 2) * 8 : (z - 1) * 8] = small
        else:
            grad_shift[(z - 5) * 8 : (z - 4) * 8] = small


def post_kernel(place, values, upstream, stats, columns, gain, *refs):
    n = len(CHUNKS)
    outs_u, outs_v, got, to_u, to_v = refs[:n], refs[n : 2 * n], refs[2 * n : 3 * n], refs[3 * n], refs[3 * n + 1]
    grad_u, grad_v, backs, sems = refs[3 * n + 2 :]
    low = place[0] < 2
    step = 16
    part = ROWS // 4

    def copy(k, i):
        rows = slice(i * part, (i + 1) * part)
        source, target = ((grad_u, to_u), (grad_v, to_v))[k]
        return pltpu.make_async_copy(source.at[0, rows], target.at[0, rows], sems.at[k, i])

    def block(i, carry):
        rows = pl.ds(pl.multiple_of(i * step, step), step)
        mean, inv = stats[0, rows, :], stats[1, rows, :]
        firsts, seconds = [], []
        for k, at in enumerate(TILES):
            chunk, lanes = tile_of(k)
            g = k * 128 // WIDTH
            long_side = outs_u[chunk][rows, lanes] + got[chunk][rows, lanes].astype(F32)
            short_side = outs_v[chunk][rows, lanes]
            mixed = jnp.where(low, short_side, long_side) + columns[rows, g : g + 1]
            mixed = mixed.astype(BF16).astype(F32)
            grad_u[0, rows, at] = (upstream[0, rows, at].astype(F32) * mixed).astype(BF16)
            back = jnp.where(low, long_side, short_side).astype(BF16)
            backs[rows, at] = back
            scaled = back.astype(F32) * gain[:, at]
            unit = (values[0, rows, at].astype(F32) - mean) * inv
            firsts, seconds = add_term(firsts, scaled), add_term(seconds, scaled * unit)
        first, second = row_mean(firsts), row_mean(seconds)
        for at in TILES:
            scaled = backs[rows, at].astype(F32) * gain[:, at]
            unit = (values[0, rows, at].astype(F32) - mean) * inv
            grad_v[0, rows, at] = (inv * (scaled - first - unit * second)).astype(BF16)
        return carry

    for i in range(4):
        lax.fori_loop(i * part // step, (i + 1) * part // step, block, 0, unroll=True)
        copy(0, i).start()
        copy(1, i).start()
    for i in range(4):
        copy(0, i).wait()
        copy(1, i).wait()


def exchanged(x, axis):
    return lax.all_to_all(x, axis, split_axis=0, concat_axis=0, tiled=True)


def compute(gated, values_in, upstream, gain, shift, mix_w, mix_bias):
    spot = lax.axis_index(Y) % QUAD
    place = jnp.stack([spot, lax.axis_index(X), lax.axis_index(CORE)]).astype(jnp.int32)
    gain_row, shift_row = gain.reshape(1, HALF), shift.reshape(1, HALF)
    n = len(CHUNKS)
    halves = [shape((ROWS, k * WIDTH), BF16) for k in CHUNKS]
    fulls = [shape((ROWS, k * WIDTH), F32) for k in CHUNKS]

    pre = call(
        pre_kernel,
        halves * 2 + [shape((2, ROWS, 128), F32)],
        (place, *map(far_memory, (values_in, gated, upstream, gain_row, shift_row))),
        scratch=[pltpu.VMEM((1, ROWS, HALF), BF16)] * 3
        + [pltpu.VMEM((1, HALF), F32)] * 2
        + [pltpu.SemaphoreType.DMA((3, 4)), pltpu.SemaphoreType.DMA((2,))],
        remote=range(1, 6),
    )
    us, vs, stats = pre[:n], pre[n : 2 * n], pre[2 * n]

    near, far, swap = [], [], []
    for i in range(n):
        near.append(lax.ppermute(vs[i], Y, NEAR))
        far.append(lax.ppermute(vs[i], Y, FAR))
        swap.append(lax.ppermute(vs[i], Y, SWAP))

    slab = call(slab_kernel, shape((GROUPS, SEG, 3 * ROWS), BF16), (place, mix_w))
    slabs = [slab] + [lax.ppermute(slab, X, CHIPS[k]) for k in range(1, 4)]
    mine = call(join_kernel, shape((4, GROUPS, SEG, 3 * ROWS), BF16), (place, *slabs))
    theirs = lax.ppermute(mine, CORE, PARTNER)
    columns, bias_term = call(
        side_kernel, [shape((ROWS, ROWS), F32), shape((64, 128), F32)], (place, us[0], vs[0], us[1], vs[1], mix_bias)
    )
    weights = call(weight_kernel, shape((GROUPS, 2 * ROWS, 3 * ROWS), BF16), (place, mine, theirs))

    operands = [(us[i], vs[i], near[i], far[i], swap[i]) for i in range(n)]
    part, out_u, out_v, one, two = call(
        functools.partial(product_kernel, 0),
        [halves[0], fulls[0], fulls[0], halves[0], halves[0]],
        (place, *operands[0], weights, gain_row, shift_row),
    )
    first_got = lax.ppermute(part, Y, OUT)
    dims = (4, SEG, 2 * CHUNKS[0] * ROWS)
    keep, send = call(
        functools.partial(mix_grad_kernel, CHUNKS[0]),
        [shape(dims, F32), shape(dims, BF16)],
        (place, *operands[0], one, two),
    )
    sums = call(
        functools.partial(sums_kernel, 0),
        shape((64, 128), F32),
        (place, values_in, stats, bias_term, out_u, out_v, part, near[0]),
    )
    folded = (keep, lax.ppermute(send, CORE, PARTNER))

    part, last_u, last_v, keep, small, last = call(
        last_kernel,
        [
            halves[1],
            fulls[1],
            fulls[1],
            shape((4, SEG, 256), F32),
            shape((64, 128), F32),
            shape((5, SEG, 256), BF16),
        ],
        (place, *operands[1], weights, gain_row, shift_row, values_in, stats, sums),
        scratch=[pltpu.VMEM((ROWS, WIDTH), BF16)] * 2 + [pltpu.VMEM((4, SEG, 256), BF16)],
    )
    outs_u, outs_v, got = (out_u, last_u), (out_v, last_v), (first_got, lax.ppermute(part, Y, OUT))
    own, small, send = call(
        chip_kernel,
        [shape((2, SEG, 1024), F32), shape((64, 128), F32), shape((2, SEG, 1152), BF16)],
        (place, *folded, keep, small, lax.ppermute(last, CORE, PARTNER)),
    )
    own, small, send = call(
        pair_kernel,
        [shape((SEG, 1024), F32), shape((64, 128), F32), shape((SEG, 1280), BF16)],
        (place, own, small, lax.ppermute(send, X, ACROSS)),
    )
    dealt = call(deal_kernel, shape((8, 8, 1280), BF16), (own, small, lax.ppermute(send, X, WITHIN)), 0)
    added = call(add_kernel, shape((8, 8, 1280), BF16), (exchanged(dealt, Z),), 0)
    placed = call(place_kernel, shape((8, 8, 2304), BF16), (exchanged(added, Y),), 0)
    grad_mix, grad_bias, grad_gain, grad_shift = call(
        final_kernel,
        [shape((SEG, GROUPS, 512), F32), shape((GROUPS, 512), F32)] + [shape((24, 128), F32)] * 2,
        (exchanged(placed, Z),),
        0,
    )

    grad_u, grad_v = call(
        post_kernel,
        [shape((1, ROWS, HALF), BF16)] * 2,
        (place, values_in, upstream, stats, columns, gain_row, *outs_u, *outs_v, *got),
        scratch=[pltpu.VMEM((1, ROWS, HALF), BF16)] * 2
        + [pltpu.VMEM((ROWS, HALF), BF16), pltpu.SemaphoreType.DMA((2, 4))],
        out=HBM,
    )
    return (grad_u, grad_v, grad_mix, grad_bias, grad_gain.reshape(HALF), grad_shift.reshape(HALF))


def solution(mesh):
    torus = Mesh(mesh.devices.reshape(8, 8, 4, 2), ("sp_0", "sp_1", "dp_0", "dp_1"))
    return jax.shard_map(
        compute,
        mesh=torus,
        in_specs=(
            P(DP, SP, None),
            P(DP, SP, None),
            P(DP, SP, None),
            P(),
            P(),
            P(DP, None, None),
            P(),
        ),
        out_specs=(P(DP, SP, None), P(DP, SP, None), P(DP, None, None), P(), P(), P()),
        check_vma=False,
    )
```

```python
import functools

import jax
import jax.numpy as jnp
from jax import lax
from jax.experimental import pallas as pl
from jax.experimental.pallas import tpu as pltpu
from jax.sharding import Mesh
from jax.sharding import PartitionSpec as P


SEG = 64
ROWS = 128
GROUPS = 4
WIDTH = 768
HALF = GROUPS * WIDTH
QUAD = 4
DP = ("dp_0", "dp_1")
SP = ("sp_0", "sp_1")
Y = "sp_1"
Z = "sp_0"
X = "dp_0"
CORE = "dp_1"
EPS = 1e-05

NEAR = [(0, 1), (3, 2), (4, 5), (7, 6)]
FAR = [(0, 2), (3, 1), (4, 6), (7, 5)]
SWAP = [(1, 2), (2, 1), (5, 6), (6, 5)]
OUT = [(1, 0), (2, 3), (5, 4), (6, 7)]
PARTNER = [(0, 1), (1, 0)]
CHIPS = [[(i, (i + k) % 4) for i in range(4)] for k in range(4)]
ACROSS = [(0, 3), (3, 0), (1, 2), (2, 1)]
WITHIN = [(0, 1), (1, 0), (2, 3), (3, 2)]

CHUNKS = (2, 2)
WIDE = CHUNKS[0] * ROWS
PLACES = [(i, k * WIDTH) for i, n in enumerate(CHUNKS) for k in range(n)]


VMEM = pl.BlockSpec(memory_space=pltpu.VMEM)
SMEM = pl.BlockSpec(memory_space=pltpu.SMEM)
HBM = pl.BlockSpec(memory_space=pltpu.HBM)
F32 = jnp.float32
BF16 = jnp.bfloat16


def far_memory(x):
    return pltpu.with_memory_space_constraint(x, pltpu.HBM)


def call(kernel, out_shape, inputs, scalars=1, scratch=(), vmem=16, remote=(), out=VMEM):
    return pl.pallas_call(
        kernel,
        out_shape=out_shape,
        in_specs=[SMEM] * scalars + [HBM if i in remote else VMEM for i in range(scalars, len(inputs))],
        out_specs=jax.tree.map(lambda _: out, out_shape),
        scratch_shapes=list(scratch),
        compiler_params=pltpu.CompilerParams(vmem_limit_bytes=vmem << 20),
    )(*inputs)


def shape(dims, dtype):
    return jax.ShapeDtypeStruct(dims, dtype)


def nt(a, b):
    return lax.dot_general(a, b, (((1,), (1,)), ((), ())), preferred_element_type=F32)


def tn(a, b):
    return lax.dot_general(a, b, (((0,), (0,)), ((), ())), preferred_element_type=F32)


def nn(a, b):
    return jnp.dot(a, b, preferred_element_type=F32)


def lanes_of(g, width=WIDTH):
    chunk, start = PLACES[g]
    start = start // WIDTH * width
    return chunk, slice(start, start + width)


TILES = [slice(k * 128, (k + 1) * 128) for k in range(HALF // 128)]


def tile_of(k):
    chunk, start = PLACES[k * 128 // WIDTH]
    start += k * 128 % WIDTH
    return chunk, slice(start, start + 128)


def row_mean(terms):
    totals = [None] * 4
    for k, term in enumerate(terms):
        totals[k % 4] = term if totals[k % 4] is None else totals[k % 4] + term
    total = (totals[0] + totals[1]) + (totals[2] + totals[3])
    return jnp.sum(total, axis=1, keepdims=True) * (1.0 / HALF)


def add_term(totals, term):
    return totals + [term] if len(totals) < 4 else totals[1:] + [totals[0] + term]


def pre_kernel(place, values_in, gated_in, upstream_in, gain_in, shift_in, *outs):
    n = len(CHUNKS)
    us, vs, stats = outs[:n], outs[n : 2 * n], outs[2 * n]
    values, gated, upstream, gain, shift, sems, few = outs[2 * n + 1 :]
    low = place[0] < 2
    step = 16
    part = ROWS // 4
    pairs = ((values_in, values), (gated_in, gated), (upstream_in, upstream))

    def copy(k, i):
        rows = slice(i * part, (i + 1) * part)
        return pltpu.make_async_copy(pairs[k][0].at[0, rows], pairs[k][1].at[0, rows], sems.at[k, i])

    singles = [
        pltpu.make_async_copy(source, target, few.at[k])
        for k, (source, target) in enumerate(((gain_in, gain), (shift_in, shift)))
    ]
    copy(0, 0).start()
    for single in singles:
        single.start()
    copy(1, 0).start()
    copy(2, 0).start()
    for i in range(1, 4):
        for k in range(3):
            copy(k, i).start()
    for single in singles:
        single.wait()

    def measure(i, carry):
        rows = pl.ds(pl.multiple_of(i * step, step), step)
        mean = row_mean(values[0, rows, at].astype(F32) for at in TILES)
        centred = (values[0, rows, at].astype(F32) - mean for at in TILES)
        inv = lax.rsqrt(row_mean(c * c for c in centred) + EPS)
        stats[0, rows, :] = jnp.broadcast_to(mean, (step, 128))
        stats[1, rows, :] = jnp.broadcast_to(inv, (step, 128))
        return carry

    def block(low, i, carry):
        rows = pl.ds(pl.multiple_of(i * step, step), step)
        mean, inv = stats[0, rows, :], stats[1, rows, :]
        for k, at in enumerate(TILES):
            chunk, lanes = tile_of(k)
            unit = (values[0, rows, at].astype(F32) - mean) * inv
            grad = (upstream[0, rows, at].astype(F32) * gated[0, rows, at].astype(F32)).astype(BF16)
            if low:
                us[chunk][rows, lanes] = grad
                vs[chunk][rows, lanes] = unit.astype(BF16)
            else:
                us[chunk][rows, lanes] = (unit * gain[:, at] + shift[:, at]).astype(BF16)
                vs[chunk][rows, lanes] = grad
        return carry

    for i in range(4):
        copy(0, i).wait()
        lax.fori_loop(i * part // step, (i + 1) * part // step, measure, 0, unroll=True)
    for k in range(1, 3):
        for i in range(4):
            copy(k, i).wait()

    @pl.when(low)
    def _():
        lax.fori_loop(0, ROWS // step, functools.partial(block, True), 0, unroll=2)

    @pl.when(jnp.logical_not(low))
    def _():
        lax.fori_loop(0, ROWS // step, functools.partial(block, False), 0, unroll=2)


def side_kernel(place, u, v, u1, v1, mix_bias, columns, bias):
    p = place[0]
    low = p < 2
    own_bias = mix_bias[:, pl.ds(pl.multiple_of(p * ROWS, ROWS), ROWS)]
    columns[...] = jnp.concatenate([own_bias, jnp.zeros((ROWS - GROUPS, ROWS), F32)], axis=0).T
    bias[...] = jnp.zeros_like(bias)
    ones = jnp.ones((8, WIDTH), BF16)
    us, vs = (u, u1), (v, v1)
    for g in range(GROUPS):
        i, lanes = lanes_of(g)
        grad = jnp.where(low, us[i][:, lanes], vs[i][:, lanes])
        bias[pl.ds(g * QUAD + p, 1), :] = nt(ones, grad)[:1]


def slab_kernel(place, rows, out):
    p = place[0]

    @pl.when(p < 3)
    def _():
        for g in range(GROUPS):
            out[g] = rows[:, g, : 3 * ROWS]

    @pl.when(p == 3)
    def _():
        for g in range(GROUPS):
            out[g] = rows[:, g, ROWS:]


def join_kernel(place, *refs):
    for k in range(4):
        refs[4][(place[1] + 4 - k) % 4] = refs[k][...]


def weight_kernel(place, mine, theirs, out):
    p, core = place[0], place[2]
    low = p < 2
    first = core == 0
    start = jnp.where(p == 3, 1, 0)
    r = lax.broadcasted_iota(jnp.int32, (ROWS, ROWS), 0) // SEG
    c = lax.broadcasted_iota(jnp.int32, (ROWS, ROWS), 1) // SEG

    def piece(t, g, s):
        cols = pl.ds(pl.multiple_of((s - start) * ROWS, ROWS), ROWS)
        ours, others = mine[t, g, :, cols], theirs[t, g, :, cols]
        return jnp.concatenate([jnp.where(first, ours, others), jnp.where(first, others, ours)], axis=0)

    @pl.when(low)
    def _():
        for g in range(GROUPS):
            for i in range(2):
                for j in range(3):
                    got = piece(p + j, g, jnp.maximum(p - i, 0)).astype(F32)
                    if i == 0 and j == 0:
                        got = jnp.where(r >= c, got, 0.0)
                    out[g, i * ROWS : (i + 1) * ROWS, j * ROWS : (j + 1) * ROWS] = got.T.astype(BF16)

    @pl.when(jnp.logical_not(low))
    def _():
        for g in range(GROUPS):
            for i in range(2):
                for j in range(3):
                    got = piece(jnp.minimum(p + i, 3), g, p - j)
                    if i == 0 and j == 0:
                        got = jnp.where(r >= c, got.astype(F32), 0.0).astype(BF16)
                    out[g, i * ROWS : (i + 1) * ROWS, j * ROWS : (j + 1) * ROWS] = got


def product_kernel(chunk, place, u, v, near, far, swap, weights, gain, shift, part, out_u, out_v, *normed):
    p = place[0]
    for g in range(GROUPS):
        i, lanes = lanes_of(g)
        if i != chunk:
            continue
        cols = slice(g * WIDTH, (g + 1) * WIDTH)
        own, other = weights[g, :ROWS, :], weights[g, ROWS:, :]
        both = jnp.concatenate([own[:, :ROWS], other[:, :ROWS]], axis=0)

        def put(slot, ref, here):
            got = ref[:, lanes].astype(F32) * gain[:, cols] + shift[:, cols]
            if here is not None:
                got = jnp.where(here, got, 0.0)
            normed[slot][:, lanes] = got.astype(BF16)

        def products(long_side, short_side):
            long_side = jnp.concatenate([ref[:, lanes] for ref in long_side], axis=0)
            short_side = jnp.concatenate([ref[:, lanes] for ref in short_side], axis=0)
            part[:, lanes] = nn(other, long_side).astype(BF16)
            out_u[:, lanes] = nn(own, long_side)
            out_v[:, lanes] = tn(both, short_side)

        @pl.when(p < 2)
        def _():
            put(0, v, None)
            put(1, near, p == 1)
            products((u, swap, far), normed)

        @pl.when(p >= 2)
        def _():
            put(0, swap, p == 2)
            put(1, far, p == 2)
            products((u, *normed), (v, near))


def mix_grad_kernel(n, place, u, v, near, far, swap, one, two, keep, send):
    p, core = place[0], place[2]
    first = core == 0
    r = lax.broadcasted_iota(jnp.int32, (ROWS, ROWS), 0) // SEG
    c = lax.broadcasted_iota(jnp.int32, (ROWS, ROWS), 1) // SEG
    keep[...] = jnp.zeros_like(keep)
    send[...] = jnp.zeros_like(send)

    def put(target, slot, k, got):
        lanes = slice((slot * n + k) * ROWS, (slot * n + k + 1) * ROWS)
        keep[target, :, lanes] = jnp.where(first, got[:SEG], got[SEG:])
        send[target, :, lanes] = jnp.where(first, got[SEG:], got[:SEG]).astype(BF16)

    for k in range(n):
        at = slice(k * WIDTH, (k + 1) * WIDTH)

        @pl.when(p == 0)
        def _():
            put(0, 0, k, jnp.where(r >= c, nt(u[:, at], one[:, at]), 0.0))

        @pl.when(p == 1)
        def _():
            put(1, 0, k, nt(u[:, at], two[:, at]))
            put(1, 1, k, jnp.where(r >= c, nt(u[:, at], one[:, at]), 0.0))
            put(2, 0, k, nt(swap[:, at], two[:, at]))
            put(3, 0, k, nt(far[:, at], two[:, at]))

        @pl.when(p == 2)
        def _():
            put(2, 0, k, jnp.where(r >= c, nt(v[:, at], u[:, at]), 0.0))
            put(2, 1, k, nt(v[:, at], one[:, at]))
            put(3, 0, k, nt(near[:, at], u[:, at]))
            put(3, 1, k, nt(near[:, at], one[:, at]))

        @pl.when(p == 3)
        def _():
            put(3, 0, k, jnp.where(r >= c, nt(v[:, at], u[:, at]), 0.0))


def split(x):
    high = x.astype(BF16)
    return high, (x - high.astype(F32)).astype(BF16)


def sums_kernel(chunk, place, values, stats, before, out_u, out_v, part, near, small):
    p = place[0]
    small[...] = before[...]
    mean = stats[0, :, :1]
    inv = stats[1, :, :1]
    for g in range(GROUPS):
        i, lanes = lanes_of(g)
        if i != chunk:
            continue
        for k in range(WIDTH // 128):
            own = slice(lanes.start + k * 128, lanes.start + (k + 1) * 128)
            cols = slice(g * WIDTH + k * 128, g * WIDTH + (k + 1) * 128)
            back = jnp.where(p < 2, out_u[:, own], out_v[:, own])
            unit = (values[0, :, cols].astype(F32) - mean) * inv
            sent = jnp.where(p == 1, part[:, own].astype(F32), 0.0)
            row = 16 + g * 6 + k
            gain_rows = back * unit + sent * near[:, own].astype(F32)
            small[row : row + 1] = jnp.sum(gain_rows, axis=0, keepdims=True)
            small[row + 24 : row + 25] = jnp.sum(back + sent, axis=0, keepdims=True)


def last_sums_kernel(place, values, stats, before, out_u, out_v, part, near, last, small, send):
    sums_kernel(1, place, values, stats, before, out_u, out_v, part, near, small)
    send[:4] = last[...]
    send[4] = jnp.zeros_like(send[4])
    high, low = split(small[...])
    send[4, :, :128] = high
    send[4, :, 128:256] = low


def last_kernel(place, u, v, near, far, swap, weights, gain, shift, values, stats, before, *refs):
    part, out_u, out_v, keep, small, send, one, two, terms = refs
    product_kernel(1, place, u, v, near, far, swap, weights, gain, shift, part, out_u, out_v, one, two)
    mix_grad_kernel(CHUNKS[1], place, u, v, near, far, swap, one, two, keep, terms)
    last_sums_kernel(place, values, stats, before, out_u, out_v, part, near, terms, small, send)


def chip_kernel(place, keep0, got0, keep1, small, got1, own, total, send):
    extra = small[...] + (got1[4, :, :128].astype(F32) + got1[4, :, 128:256].astype(F32))
    high, low = split(extra)
    total[...] = extra
    send[0, :, 1024:] = high
    send[1, :, 1024:] = low
    near = place[1] // 2 * 2
    for k in range(2):
        other = 2 - near + k
        for keep, got, first, width in ((keep0, got0, 0, WIDE), (keep1, got1, WIDE, 512 - WIDE)):
            for slot in range(2):
                at = slice(slot * width, (slot + 1) * width)
                lanes = slice(slot * 512 + first, slot * 512 + first + width)
                own[k, :, lanes] = keep[near + k, :, at] + got[near + k, :, at].astype(F32)
                send[k, :, lanes] = (keep[other, :, at] + got[other, :, at].astype(F32)).astype(BF16)


def pair_kernel(place, keep, small, got, own, total, send):
    extra = small[...] + (got[0, :, 1024:].astype(F32) + got[1, :, 1024:].astype(F32))
    high, low = split(extra)
    total[...] = extra
    send[:, 1024:1152] = high
    send[:, 1152:1280] = low
    b = place[1] % 2
    own[...] = keep[b] + got[b, :, :1024].astype(F32)
    send[:, :1024] = (keep[1 - b] + got[1 - b, :, :1024].astype(F32)).astype(BF16)


def deal_kernel(own, small, got, out):
    total = (own[...] + got[:, :1024].astype(F32)).astype(BF16)
    high, low = split(small[...] + (got[:, 1024:1152].astype(F32) + got[:, 1152:1280].astype(F32)))
    for z in range(8):
        rows = slice(z * 8, (z + 1) * 8)
        out[z, :, :1024] = total[rows]
        out[z, :, 1024:1152] = high[rows]
        out[z, :, 1152:1280] = low[rows]


def add_kernel(got, out):
    total = got[0].astype(F32)
    for z in range(1, 8):
        total = total + got[z].astype(F32)
    high, low = split(total[:, 1024:1152] + total[:, 1152:1280])
    total = total[:, :1024].astype(BF16)
    for y in range(8):
        out[y, :, :1024] = total
        out[y, :, 1024:1152] = high
        out[y, :, 1152:1280] = low


def place_kernel(got, out):
    def at(place, slot):
        lanes = slice(slot * 512, (slot + 1) * 512)
        return got[place, :, lanes].astype(F32) + got[place + QUAD, :, lanes].astype(F32)

    columns = (at(0, 0) + at(1, 0), at(1, 1) + at(2, 1), at(2, 0), at(3, 0))
    columns = [c.astype(BF16) for c in columns]
    extra = jnp.zeros((8, 128), F32)
    for y in range(8):
        extra = extra + got[y, :, 1024:1152].astype(F32) + got[y, :, 1152:1280].astype(F32)
    high, low = split(extra)
    for z in range(8):
        for s in range(4):
            for g in range(GROUPS):
                out[z, :, g * 512 + s * ROWS : g * 512 + (s + 1) * ROWS] = columns[s][
                    :, g * ROWS : (g + 1) * ROWS
                ]
        out[z, :, 2048:2176] = high
        out[z, :, 2176:2304] = low


def final_kernel(got, grad_mix, grad_bias, grad_gain, grad_shift):
    for z in range(8):
        rows = slice(z * 8, (z + 1) * 8)
        for g in range(GROUPS):
            grad_mix[rows, g, :] = got[z, :, g * 512 : (g + 1) * 512].astype(F32)
        small = got[z, :, 2048:2176].astype(F32) + got[z, :, 2176:2304].astype(F32)
        if z < 2:
            for i in range(8):
                g, p = 2 * z + i // QUAD, i % QUAD
                grad_bias[g : g + 1, p * ROWS : (p + 1) * ROWS] = small[i : i + 1]
        elif z < 5:
            grad_gain[(z - 2) * 8 : (z - 1) * 8] = small
        else:
            grad_shift[(z - 5) * 8 : (z - 4) * 8] = small


def post_kernel(place, values, upstream, stats, columns, gain, *refs):
    n = len(CHUNKS)
    outs_u, outs_v, got, to_u, to_v = refs[:n], refs[n : 2 * n], refs[2 * n : 3 * n], refs[3 * n], refs[3 * n + 1]
    grad_u, grad_v, backs, sems = refs[3 * n + 2 :]
    low = place[0] < 2
    step = 16
    part = ROWS // 4

    def copy(k, i):
        rows = slice(i * part, (i + 1) * part)
        source, target = ((grad_u, to_u), (grad_v, to_v))[k]
        return pltpu.make_async_copy(source.at[0, rows], target.at[0, rows], sems.at[k, i])

    def block(i, carry):
        rows = pl.ds(pl.multiple_of(i * step, step), step)
        mean, inv = stats[0, rows, :], stats[1, rows, :]
        firsts, seconds = [], []
        for k, at in enumerate(TILES):
            chunk, lanes = tile_of(k)
            g = k * 128 // WIDTH
            long_side = outs_u[chunk][rows, lanes] + got[chunk][rows, lanes].astype(F32)
            short_side = outs_v[chunk][rows, lanes]
            mixed = jnp.where(low, short_side, long_side) + columns[rows, g : g + 1]
            mixed = mixed.astype(BF16).astype(F32)
            grad_u[0, rows, at] = (upstream[0, rows, at].astype(F32) * mixed).astype(BF16)
            back = jnp.where(low, long_side, short_side).astype(BF16)
            backs[rows, at] = back
            scaled = back.astype(F32) * gain[:, at]
            unit = (values[0, rows, at].astype(F32) - mean) * inv
            firsts, seconds = add_term(firsts, scaled), add_term(seconds, scaled * unit)
        first, second = row_mean(firsts), row_mean(seconds)
        for at in TILES:
            scaled = backs[rows, at].astype(F32) * gain[:, at]
            unit = (values[0, rows, at].astype(F32) - mean) * inv
            grad_v[0, rows, at] = (inv * (scaled - first - unit * second)).astype(BF16)
        return carry

    for i in range(4):
        lax.fori_loop(i * part // step, (i + 1) * part // step, block, 0, unroll=True)
        copy(0, i).start()
        copy(1, i).start()
    for i in range(4):
        copy(0, i).wait()
        copy(1, i).wait()


def exchanged(x, axis):
    return lax.all_to_all(x, axis, split_axis=0, concat_axis=0, tiled=True)


def compute(gated, values_in, upstream, gain, shift, mix_w, mix_bias):
    spot = lax.axis_index(Y) % QUAD
    place = jnp.stack([spot, lax.axis_index(X), lax.axis_index(CORE)]).astype(jnp.int32)
    gain_row, shift_row = gain.reshape(1, HALF), shift.reshape(1, HALF)
    n = len(CHUNKS)
    halves = [shape((ROWS, k * WIDTH), BF16) for k in CHUNKS]
    fulls = [shape((ROWS, k * WIDTH), F32) for k in CHUNKS]

    pre = call(
        pre_kernel,
        halves * 2 + [shape((2, ROWS, 128), F32)],
        (place, *map(far_memory, (values_in, gated, upstream, gain_row, shift_row))),
        scratch=[pltpu.VMEM((1, ROWS, HALF), BF16)] * 3
        + [pltpu.VMEM((1, HALF), F32)] * 2
        + [pltpu.SemaphoreType.DMA((3, 4)), pltpu.SemaphoreType.DMA((2,))],
        remote=range(1, 6),
    )
    us, vs, stats = pre[:n], pre[n : 2 * n], pre[2 * n]

    near, far, swap = [], [], []
    for i in range(n):
        near.append(lax.ppermute(vs[i], Y, NEAR))
        far.append(lax.ppermute(vs[i], Y, FAR))
        swap.append(lax.ppermute(vs[i], Y, SWAP))

    slab = call(slab_kernel, shape((GROUPS, SEG, 3 * ROWS), BF16), (place, mix_w))
    slabs = [slab] + [lax.ppermute(slab, X, CHIPS[k]) for k in range(1, 4)]
    mine = call(join_kernel, shape((4, GROUPS, SEG, 3 * ROWS), BF16), (place, *slabs))
    theirs = lax.ppermute(mine, CORE, PARTNER)
    columns, bias_term = call(
        side_kernel,
        [shape((ROWS, ROWS), F32), shape((64, 128), F32)],
        (place, us[0], vs[0], us[1], vs[1], mix_bias),
    )
    weights = call(weight_kernel, shape((GROUPS, 2 * ROWS, 3 * ROWS), BF16), (place, mine, theirs))

    operands = [(us[i], vs[i], near[i], far[i], swap[i]) for i in range(n)]
    part, out_u, out_v, one, two = call(
        functools.partial(product_kernel, 0),
        [halves[0], fulls[0], fulls[0], halves[0], halves[0]],
        (place, *operands[0], weights, gain_row, shift_row),
    )
    first_got = lax.ppermute(part, Y, OUT)
    dims = (4, SEG, 2 * CHUNKS[0] * ROWS)
    keep, send = call(
        functools.partial(mix_grad_kernel, CHUNKS[0]),
        [shape(dims, F32), shape(dims, BF16)],
        (place, *operands[0], one, two),
    )
    sums = call(
        functools.partial(sums_kernel, 0),
        shape((64, 128), F32),
        (place, values_in, stats, bias_term, out_u, out_v, part, near[0]),
    )
    folded = (keep, lax.ppermute(send, CORE, PARTNER))

    last_dims = (4, SEG, 2 * CHUNKS[1] * ROWS)
    part, last_u, last_v, keep, small, last = call(
        last_kernel,
        [
            halves[1],
            fulls[1],
            fulls[1],
            shape(last_dims, F32),
            shape((64, 128), F32),
            shape((5, *last_dims[1:]), BF16),
        ],
        (place, *operands[1], weights, gain_row, shift_row, values_in, stats, sums),
        scratch=[pltpu.VMEM(halves[1].shape, BF16)] * 2 + [pltpu.VMEM(last_dims, BF16)],
    )
    outs_u, outs_v, got = (out_u, last_u), (out_v, last_v), (first_got, lax.ppermute(part, Y, OUT))
    own, small, send = call(
        chip_kernel,
        [shape((2, SEG, 1024), F32), shape((64, 128), F32), shape((2, SEG, 1152), BF16)],
        (place, *folded, keep, small, lax.ppermute(last, CORE, PARTNER)),
    )
    own, small, send = call(
        pair_kernel,
        [shape((SEG, 1024), F32), shape((64, 128), F32), shape((SEG, 1280), BF16)],
        (place, own, small, lax.ppermute(send, X, ACROSS)),
    )
    dealt = call(
        deal_kernel, shape((8, 8, 1280), BF16), (own, small, lax.ppermute(send, X, WITHIN)), 0
    )
    added = call(add_kernel, shape((8, 8, 1280), BF16), (exchanged(dealt, Z),), 0)
    placed = call(place_kernel, shape((8, 8, 2304), BF16), (exchanged(added, Y),), 0)
    grad_mix, grad_bias, grad_gain, grad_shift = call(
        final_kernel,
        [shape((SEG, GROUPS, 512), F32), shape((GROUPS, 512), F32)] + [shape((24, 128), F32)] * 2,
        (exchanged(placed, Z),),
        0,
    )

    grad_u, grad_v = call(
        post_kernel,
        [shape((1, ROWS, HALF), BF16)] * 2,
        (place, values_in, upstream, stats, columns, gain_row, *outs_u, *outs_v, *got),
        scratch=[pltpu.VMEM((1, ROWS, HALF), BF16)] * 2
        + [pltpu.VMEM((ROWS, HALF), BF16), pltpu.SemaphoreType.DMA((2, 4))],
        out=HBM,
    )
    return (grad_u, grad_v, grad_mix, grad_bias, grad_gain.reshape(HALF), grad_shift.reshape(HALF))


def solution(mesh):
    torus = Mesh(mesh.devices.reshape(8, 8, 4, 2), ("sp_0", "sp_1", "dp_0", "dp_1"))
    return jax.shard_map(
        compute,
        mesh=torus,
        in_specs=(
            P(DP, SP, None),
            P(DP, SP, None),
            P(DP, SP, None),
            P(),
            P(),
            P(DP, None, None),
            P(),
        ),
        out_specs=(P(DP, SP, None), P(DP, SP, None), P(DP, None, None), P(), P(), P()),
        check_vma=False,
    )
```
